32 devices in a mesh: ep: 8 (over z, x), tp: 4 (over y, core).
Axes of the slice: x: 2, y: 2, z: 4, core: 2. Of those that a mesh axis runs over, the one named last changes fastest.
Arguments:
- mixer_input: bfloat16 [2048, 2048], P('ep', 'tp'), may hold values from -80 to 80
- mixer_gain: float32 [2048], P('tp'), may hold values from 0.1 to 1.9
- time_step: float32 [2048, 128], P('ep', 'tp'), may hold values from 0.25 to 4
- pole_real: float32 [128, 32], P('tp'), may hold values from -0.1 to 0, as said below
- pole_imag: float32 [128, 32], P('tp'), may hold values from 0.25 to 3
- input_real: float32 [128, 32, 16], P('tp'), may hold values from -1 to 1
- input_imag: float32 [128, 32, 16], P('tp'), may hold values from -1 to 1
- read_real: float32 [128, 16, 32], P('tp'), may hold values from -1 to 1
- read_imag: float32 [128, 16, 32], P('tp'), may hold values from -1 to 1
- out_value: bfloat16 [2048, 2048], P(None, 'tp'), may hold values from -0.125 to 0.125
- out_gate: bfloat16 [2048, 2048], P(None, 'tp'), may hold values from -0.125 to 0.125
- expert_input: bfloat16 [1024, 2048], P('ep', 'tp'), may hold values from -80 to 80
- expert_gain: float32 [2048], P('tp'), may hold values from 0.1 to 1.9
- routes: int32 [1024, 2], P('ep'), may hold values from 0 to 7, all different within a row; in each aligned block of 128 rows (0 to 127, 128 to 255, ...) at most 64 rows name the same one
- route_weight: float32 [1024, 2], P('ep'), may hold values from 0.2 to 1
- expert_gate: bfloat16 [8, 2048, 4096], P('ep', None, 'tp'), may hold values from -0.125 to 0.125
- expert_up: bfloat16 [8, 2048, 4096], P('ep', None, 'tp'), may hold values from -0.125 to 0.125
- expert_down: bfloat16 [8, 4096, 2048], P('ep', 'tp'), may hold values from -0.125 to 0.125
Outputs:
- mixer_output: bfloat16 [2048, 2048], P('ep', 'tp')
- expert_output: bfloat16 [1024, 2048], P('ep', 'tp')
The draws below stay inside these ranges and needn't reach their ends.
Inputs may be any that keep to these rules, and one draw needn't show every extreme that they name: `routes`: each row names 2 different experts. Among the 128 rows of one index of ep, no expert is named more than 64 times, a bound that some block reaches in some of them. `pole_real`: every rate is negative.
All inputs are finite; a program needn't handle non-finite values.
Results may differ from the reference program's by a relative error of at most 0.02.
Values may be sent and summed in bfloat16 or wider, within the bound.
A program may use at most 128 MiB of HBM per device.

```python
import math
import jax
import jax.numpy as jnp
import numpy as np
from jax import lax

D = 2048
GROUP_CH = 16
GROUPS = 128
STATE = 32
FFE = 4096
EXPERTS = 8
TOP = 2
TOK_A = 256
TOK_B = 128
BLOCK = 128
SEQ_A = 2048
SEQ_B = 1024
CAP = 64
N_EP = 8
N_TP = 4


def scaled_rows(key, length):
    first, second, third = jax.random.split(key, 3)
    base = jnp.clip(jax.random.normal(first, (length, D), jnp.float32), -6.0, 6.0)
    levels = jnp.exp(jax.random.uniform(second, (16,), jnp.float32, -1.1, 1.1))
    column_scale = jnp.repeat(levels, D // 16)
    return base * column_scale[None, :]


def draw_mixer_input(key, part):
    return scaled_rows(jax.random.fold_in(key, 7), SEQ_A).astype(jnp.bfloat16)


def draw_expert_input(key, part):
    return scaled_rows(jax.random.fold_in(key, 8), SEQ_B).astype(jnp.bfloat16)


def draw_time_step(key, part):
    first, second = jax.random.split(jax.random.fold_in(key, 9))
    spans = SEQ_A // TOK_A
    fine = jax.random.uniform(first, (SEQ_A, GROUPS), jnp.float32, -0.5, 0.5)
    coarse = jax.random.uniform(second, (spans, 1, GROUPS), jnp.float32, -0.8, 0.8)
    coarse = jnp.broadcast_to(coarse, (spans, TOK_A, GROUPS)).reshape(SEQ_A, GROUPS)
    return jnp.exp(fine + coarse)


def rate_table(key):
    first, second, third = jax.random.split(jax.random.fold_in(key, 101), 3)
    share = 0.5
    slow = jax.random.uniform(first, (GROUPS, STATE), jnp.float32) < share
    slow_rate = jnp.exp(jax.random.uniform(second, (GROUPS, STATE), jnp.float32, math.log(0.1), math.log(0.6))) / SEQ_A
    fast_rate = jnp.exp(jax.random.uniform(third, (GROUPS, STATE), jnp.float32, math.log(0.03), math.log(0.1)))
    return jnp.where(slow, slow_rate, fast_rate)


def draw_pole_real(key, part):
    return -rate_table(key)


def read_table(key, salt):
    rates = rate_table(key)
    scale = jnp.sqrt(2.4 * rates / STATE) * 1.4
    noise = jnp.clip(jax.random.normal(jax.random.fold_in(key, salt), (GROUPS, GROUP_CH, STATE), jnp.float32), -4.0, 4.0)
    return noise * scale[:, None, :]


def draw_read_real(key, part):
    return read_table(key, 202)


def draw_read_imag(key, part):
    return read_table(key, 203)


def spiked(values, rng, source, target, parts, factor):
    owner, partner = [(jnp.arange(values.shape[dim]) // (values.shape[dim] // parts)).reshape([-1 if axis == dim else 1 for axis in range(values.ndim)]) for dim in (source, target)]
    chosen = jax.random.permutation(rng, parts)[partner]
    strong = (owner == chosen) | (owner == (partner + parts // 2) % parts)
    return jnp.where(strong, factor * values, values)


def block_scale(own_key, dims, cuts, low, top_value):
    level, own = 1.0, jax.random.fold_in(own_key, 6)
    for position, shards_of in cuts:
        steps = jnp.exp(jax.random.uniform(jax.random.fold_in(own, position), (shards_of,), jnp.float32, low / len(cuts), top_value / len(cuts)))
        level = level * jnp.repeat(steps, dims[position] // shards_of).reshape([-1 if axis == position else 1 for axis in range(len(dims))])
    return level


def deal_out(stream_key, own, number, rows, number_of, top, reach, skew):
    ranking = jax.random.permutation(stream_key, number_of)
    heavy_load, common = portions_of(number_of, rows * top, reach, skew, True), portions_of(number_of, rows * top, reach, skew, False)
    places = jnp.arange(number_of)

    def named(sizes, offset_by):
        used = int((sizes > 0).sum())
        fixed = max(1, used // 4)
        moved = fixed + (places - fixed + offset_by * (used - fixed)) % max(1, number_of - fixed)
        return jnp.zeros((number_of,), jnp.int32).at[ranking[jnp.where(places < fixed, places, moved)]].set(jnp.asarray(sizes, jnp.int32))

    sizes = jnp.where(number % 4 == 0, named(heavy_load, number // 4), named(common, number - number // 4 - 1))
    mixed = jax.random.permutation(jax.random.fold_in(own, 3), number_of)
    source_of, taker = mixed[0:number_of // 2 * 2:2], mixed[1:number_of // 2 * 2:2]
    margin = jnp.minimum(sizes[source_of] - 1, reach - sizes[taker]) // 2
    margin = jnp.where((source_of == ranking[0]) | (taker == ranking[0]) | (sizes[taker] == 0), 0, jnp.maximum(margin, 0))
    moved = jax.random.randint(jax.random.fold_in(own, 4), (number_of // 2,), 0, 1 << 20) % (margin + 1)
    sizes = sizes.at[source_of].add(-moved).at[taker].add(moved)
    items = jnp.searchsorted(jnp.cumsum(sizes), jnp.arange(rows * top), side="right").astype(jnp.int32)
    table = items.reshape(top, rows).T
    table = table[jax.random.permutation(jax.random.fold_in(own, 1), rows)]
    offset_by = jax.random.randint(jax.random.fold_in(own, 2), (rows, 1), 0, top)
    return jnp.take_along_axis(table, (jnp.arange(top)[None, :] + offset_by) % top, axis=1)


def portions_of(amount, total, most, slope, full):
    weights = [(1 << 20) // math.isqrt(rank ** slope) + 1 for rank in range(1, amount + 1)]
    largest = most if full else min(most, max(-(-total // amount), total * weights[0] // sum(weights)))
    least = 1 if total - largest >= amount - 1 else 0
    counts, rest = [largest] + [least] * (amount - 1), total - largest - least * (amount - 1)
    while rest > 0:
        movable = [i for i in range(1, amount) if counts[i] < largest] or [i for i in range(1, amount) if counts[i] < most]
        pool, budget = sum([weights[i] for i in movable]), rest
        for i in movable:
            more = min(most - counts[i], max(1, budget * weights[i] // pool), rest)
            counts[i] = counts[i] + more
            rest = rest - more
    return np.array(counts)


def scatter_about(key, shape, width, bound, shards=(), held_as=jnp.bfloat16):
    values = width * jax.random.normal(key, shape, jnp.float32)
    if shards:
        values = values * block_scale(key, shape, shards, -0.22, 0.18)
    return jnp.clip(values, -bound, bound).astype(held_as)


def bell_draw_with(rng, extent, spread, reach, shards, heavy, kind=jnp.bfloat16):
    array = spread * jax.random.normal(rng, extent, jnp.float32)
    if shards:
        array = array * block_scale(rng, extent, shards, -0.22, 0.18)
    return jnp.clip(spiked(array, jax.random.fold_in(rng, 3), *heavy), -reach, reach).astype(kind)


def setup_inputs(seed: int = 0) -> dict:
    keys = jax.random.split(jax.random.key(seed), 19)
    mixer_input = draw_mixer_input(jax.random.fold_in(keys[18], 71), 0)
    mixer_gain = jnp.clip(1.0 + 0.18 * jax.random.normal(keys[1], (D,), jnp.float32), 0.1, 1.9)
    time_step = draw_time_step(jax.random.fold_in(keys[18], 71), 0)
    pole_real = draw_pole_real(jax.random.fold_in(keys[18], 71), 0)
    pole_imag = jnp.clip(0.25 + 2.75 * jax.random.uniform(keys[4], (GROUPS, STATE), jnp.float32) ** block_scale(keys[4], (GROUPS, STATE), ((0, 4),), -0.2, 0.2), 0.25, 3.0)
    input_real = scatter_about(keys[5], (GROUPS, STATE, GROUP_CH), (2 * GROUP_CH) ** -0.5, 1.0, ((0, 4),), jnp.float32)
    input_imag = scatter_about(keys[6], (GROUPS, STATE, GROUP_CH), (2 * GROUP_CH) ** -0.5, 1.0, ((0, 4),), jnp.float32)
    read_real = draw_read_real(jax.random.fold_in(keys[18], 71), 0)
    read_imag = draw_read_imag(jax.random.fold_in(keys[18], 71), 0)
    out_value = scatter_about(keys[9], (D, D), D ** -0.5, 0.125, ((1, 4),))
    out_gate = scatter_about(keys[10], (D, D), D ** -0.5, 0.125, ((1, 4),))
    expert_input = draw_expert_input(jax.random.fold_in(keys[18], 71), 0)
    expert_gain = jnp.clip(1.0 + 0.18 * jax.random.normal(keys[12], (D,), jnp.float32), 0.1, 1.9)
    routes_keys = jax.random.split(jax.random.fold_in(keys[13], 1), SEQ_B // TOK_B)
    routes_turns = jax.random.permutation(jax.random.fold_in(keys[13], 3), SEQ_B // TOK_B)
    routes = jax.vmap(lambda own, number: deal_out(jax.random.fold_in(keys[13], 2), own, number, TOK_B, EXPERTS, TOP, CAP, 1))(routes_keys, routes_turns).reshape((SEQ_B, TOP))
    route_weight = jnp.clip(0.2 + 0.8 * jax.random.uniform(keys[14], (SEQ_B, TOP), jnp.float32) ** block_scale(keys[14], (SEQ_B, TOP), ((0, 8),), -0.2, 0.2), 0.2, 1.0)
    expert_gate = scatter_about(keys[15], (EXPERTS, D, FFE), D ** -0.5, 0.125, ((0, 8), (2, 4)))
    expert_up = scatter_about(keys[16], (EXPERTS, D, FFE), D ** -0.5, 0.125, ((0, 8), (2, 4)))
    expert_down = bell_draw_with(keys[17], (EXPERTS, FFE, D), FFE ** -0.5, 0.125, ((0, 8), (1, 4)), (1, 2, 4, 2.0))
    return dict(mixer_input=mixer_input, mixer_gain=mixer_gain, time_step=time_step, pole_real=pole_real, pole_imag=pole_imag, input_real=input_real, input_imag=input_imag, read_real=read_real, read_imag=read_imag, out_value=out_value, out_gate=out_gate, expert_input=expert_input, expert_gain=expert_gain, routes=routes, route_weight=route_weight, expert_gate=expert_gate, expert_up=expert_up, expert_down=expert_down)


def layer_norm(rows, gain):
    wide = rows.astype(jnp.float32)
    average = lax.optimization_barrier(jnp.mean(wide, axis=1, keepdims=True))
    variance = lax.optimization_barrier(jnp.mean(wide * wide, axis=1, keepdims=True)) - average * average
    return (wide - average) * lax.rsqrt(variance + 1e-05) * gain[None, :]

def compose(earlier, later):
    a1r, a1i, b1r, b1i = earlier
    a2r, a2i, b2r, b2i = later
    return (a2r * a1r - a2i * a1i, a2r * a1i + a2i * a1r, a2r * b1r - a2i * b1i + b2r, a2r * b1i + a2i * b1r + b2i)

def mixer_part(mixer_input, mixer_gain, time_step, pole_real, pole_imag, input_real, input_imag, read_real, read_imag, out_value, out_gate):
    normed = layer_norm(mixer_input, mixer_gain)
    blocks = SEQ_A // BLOCK
    rows_in = normed.reshape(blocks, BLOCK, GROUPS, GROUP_CH)
    steps_in = time_step.reshape(blocks, BLOCK, GROUPS)
    denom = pole_real * pole_real + pole_imag * pole_imag
    highest = lax.Precision.HIGHEST

    def advance(carried, inputs):
        state_re, state_im = carried
        rows_blk, step_blk = inputs
        drive_re = jnp.einsum('tgm,gpm->tgp', rows_blk, input_real, precision=highest)
        drive_im = jnp.einsum('tgm,gpm->tgp', rows_blk, input_imag, precision=highest)
        delta = step_blk[:, :, None]
        magnitude = jnp.exp(pole_real[None] * delta)
        angle = pole_imag[None] * delta
        abar_re = magnitude * jnp.cos(angle)
        abar_im = magnitude * jnp.sin(angle)
        numer_re = abar_re - 1.0
        coef_re = (numer_re * pole_real[None] + abar_im * pole_imag[None]) / denom[None]
        coef_im = (abar_im * pole_real[None] - numer_re * pole_imag[None]) / denom[None]
        push_re = coef_re * drive_re - coef_im * drive_im
        push_im = coef_re * drive_im + coef_im * drive_re
        cum_re, cum_im, acc_re, acc_im = lax.associative_scan(compose, (abar_re, abar_im, push_re, push_im), axis=0)
        new_re = cum_re * state_re[None] - cum_im * state_im[None] + acc_re
        new_im = cum_re * state_im[None] + cum_im * state_re[None] + acc_im
        response = jnp.einsum('gmp,tgp->tgm', read_real, new_re, precision=highest) - jnp.einsum('gmp,tgp->tgm', read_imag, new_im, precision=highest)
        mixed_blk = jax.nn.gelu(response.reshape(BLOCK, D)).astype(jnp.bfloat16)
        return ((new_re[-1], new_im[-1]), mixed_blk)
    zeros_state = jnp.zeros((GROUPS, STATE), jnp.float32)
    unused, mixed = lax.scan(advance, (zeros_state, zeros_state), (rows_in, steps_in))
    mixed = mixed.reshape(SEQ_A, D)
    value_sum = jnp.dot(mixed, out_value, preferred_element_type=jnp.float32)
    gate_sum = jnp.dot(mixed, out_gate, preferred_element_type=jnp.float32)
    return (value_sum * jax.nn.sigmoid(gate_sum)).astype(jnp.bfloat16)

def expert_part(expert_input, expert_gain, routes, route_weight, expert_gate, expert_up, expert_down):
    normed = layer_norm(expert_input, expert_gain).astype(jnp.bfloat16)
    tokens = normed.shape[0]
    flat_routes = routes.reshape(-1)
    flat_weights = route_weight.reshape(-1)
    owners = jnp.arange(flat_routes.shape[0], dtype=jnp.int32) // TOP
    padded = jnp.concatenate([normed, jnp.zeros((1, D), jnp.bfloat16)], axis=0)
    limit = N_EP * CAP
    blocks = FFE // N_TP

    def one_expert(totals, index):
        hits = flat_routes == index
        where_to = jnp.cumsum(hits.astype(jnp.int32)) - 1
        target = jnp.where(hits, where_to, limit).astype(jnp.int32)
        holder = jnp.full((limit,), tokens, jnp.int32).at[target].set(owners, mode='drop')
        share = jnp.zeros((limit,), jnp.float32).at[target].set(flat_weights, mode='drop')
        rows = padded[holder]
        gate_w = lax.dynamic_index_in_dim(expert_gate, index, 0, keepdims=False)
        up_w = lax.dynamic_index_in_dim(expert_up, index, 0, keepdims=False)
        down_w = lax.dynamic_index_in_dim(expert_down, index, 0, keepdims=False)
        gate_val = jnp.dot(rows, gate_w, preferred_element_type=jnp.float32)
        up_val = jnp.dot(rows, up_w, preferred_element_type=jnp.float32)
        hidden = (jax.nn.silu(gate_val) * up_val).astype(jnp.bfloat16)
        pieces = hidden.reshape(limit, N_TP, blocks).astype(jnp.float32)
        down_pieces = down_w.reshape(N_TP, blocks, D).astype(jnp.float32)
        partial_value = jnp.einsum('snk,nkd->nsd', pieces, down_pieces).astype(jnp.bfloat16)
        result = lax.optimization_barrier(jnp.sum(partial_value.astype(jnp.float32), axis=0)).astype(jnp.bfloat16)
        contrib = result.astype(jnp.float32) * share[:, None]
        return (totals.at[holder].add(contrib), None)
    totals, unused = lax.scan(one_expert, jnp.zeros((tokens + 1, D), jnp.float32), jnp.arange(EXPERTS, dtype=jnp.int32))
    return totals[:tokens].astype(jnp.bfloat16)

def reference(mixer_input, mixer_gain, time_step, pole_real, pole_imag, input_real, input_imag, read_real, read_imag, out_value, out_gate, expert_input, expert_gain, routes, route_weight, expert_gate, expert_up, expert_down):
    mixer_output = mixer_part(mixer_input, mixer_gain, time_step, pole_real, pole_imag, input_real, input_imag, read_real, read_imag, out_value, out_gate)
    expert_output = expert_part(expert_input, expert_gain, routes, route_weight, expert_gate, expert_up, expert_down)
    return (mixer_output, expert_output)
```

```python
import functools
import jax
import jax.numpy as jnp
from jax import lax
from jax.experimental import pallas as pl
from jax.experimental.pallas import tpu as pltpu
from jax.sharding import PartitionSpec as P

norm_eps = 1e-05
CHUNKS = 8
CORES = 2
f32 = jnp.float32
bf16 = jnp.bfloat16


def sin_cos(angle):
    turns = jnp.round(angle * 0.6366197723675814)
    left = angle - turns * 1.5703125
    left = left - turns * 4.83751296997e-4
    left = left - turns * 7.549789948768648e-8
    sq = left * left
    sine = ((-1.9515295891e-4 * sq + 8.3321608736e-3) * sq - 1.6666654611e-1) * sq * left + left
    cosine = (
        ((2.443315711809948e-5 * sq - 1.388731625493765e-3) * sq + 4.166664568298827e-2) * sq * sq
        - 0.5 * sq
        + 1.0
    )
    quadrant = turns.astype(jnp.int32)
    odd = (quadrant & 1) == 1
    sin_out = jnp.where(odd, cosine, sine)
    cos_out = jnp.where(odd, sine, cosine)
    sin_out = jnp.where((quadrant & 2) == 2, -sin_out, sin_out)
    cos_out = jnp.where(((quadrant + 1) & 2) == 2, -cos_out, cos_out)
    return sin_out, cos_out


def iota(shape, dim):
    return lax.broadcasted_iota(jnp.int32, shape, dim)


def nn(left, right):
    return jnp.dot(left, right, preferred_element_type=f32)


def nt(left, right):
    return lax.dot_general(left, right, (((1,), (1,)), ((), ())), preferred_element_type=f32)


def tn(left, right):
    return lax.dot_general(left, right, (((0,), (0,)), ((), ())), preferred_element_type=f32)


def partner(me, k):
    other, bit = me, 1
    while bit <= k:
        if k & bit:
            other = other + bit * (1 - 2 * ((me // bit) % 2))
        bit *= 2
    return other


def spread(table, row_div, lanes, lane_div):
    rows, width = table.shape
    pick = (iota((width, lanes), 0) == iota((width, lanes), 1) % width).astype(bf16)
    wide = nn(table.astype(bf16), pick)
    same = iota((rows, lanes), 0) // row_div == iota((rows, lanes), 1) // lane_div
    return jnp.where(same, wide, 0.0).astype(bf16)


def row_sums(rows):
    ones = jnp.ones((16, rows.shape[1]), bf16)
    wide = rows.astype(f32)
    square = wide * wide
    high = square.astype(bf16)
    low = (square - high.astype(f32)).astype(bf16)
    sums = nt(ones, rows)
    squares = nt(ones, high) + nt(ones, low)
    return jnp.where(iota((8, 1), 0) == 0, sums[:8], squares[:8])


def normalize(rows, stats, gain, width):
    average = stats[:, 0:1] / width
    variance = stats[:, 1:2] / width - average * average
    return (rows.astype(f32) - average) * lax.rsqrt(variance + norm_eps) * gain


def kernel(dims, *refs):
    count_ep, count_tp, groups_y, halves, state_size = dims
    hbm, refs = refs[:17], refs[17:]
    (out_a, out_b), refs = refs[:2], refs[2:]
    vm, refs = refs[:17], refs[17:]
    (
        mine_stats, slot_stats, outgoing, rows_x, share_hi, share_lo, a_re, a_im, u_re, u_im,
        sums, enter, mine_state, slot_state, n_re, n_im, mixed, mixed_all, hidden, own,
        sib_send, sib_recv, y_send, y_recv, final, returned,
        sem_in, st_s, st_r, aa_s, aa_r, dy_s, dy_r, ds_s, ds_r, hs_s, hs_r,
        my_s, my_r, ms_s, ms_r, rs_s, rs_r, ry_s, ry_r, ra_s, ra_r,
    ) = refs
    (
        a_in, step_in, gain_a, pole_in, in_re, in_im, rd_re, rd_im, w_value, w_gate_out,
        b_in, gain_b, routes_in, weight_in, w_gate, w_up, w_down,
    ) = vm

    me = lax.axis_index("ep")
    tp = lax.axis_index("tp")
    count_y = count_tp // CORES
    my_y = tp // CORES
    my_core = tp % CORES
    sibling = my_y * CORES + 1 - my_core

    barrier = pltpu.get_barrier_semaphore()
    for k in range(1, count_ep):
        pl.semaphore_signal(
            barrier, inc=1, device_id={"ep": partner(me, k)}, device_id_type=pl.DeviceIdType.MESH
        )
    for k in range(1, count_tp):
        pl.semaphore_signal(
            barrier, inc=1, device_id={"tp": lax.rem(tp + k, count_tp)},
            device_id_type=pl.DeviceIdType.MESH,
        )

    loads = [
        pltpu.make_async_copy(source, target, sem_in.at[i])
        for i, (source, target) in enumerate(zip(hbm, vm))
    ]
    for i in (10, 0, 12, 13, 11, 1, 3, 2, 4, 5, 6, 7, 14, 15, 16, 8, 9):
        loads[i].start()

    pending = []

    def send(source, target, send_sem, recv_sem, **where):
        copy = pltpu.make_async_remote_copy(
            src_ref=source, dst_ref=target, send_sem=send_sem, recv_sem=recv_sem,
            device_id=where, device_id_type=pl.DeviceIdType.MESH,
        )
        copy.start()
        pending.append(copy)
        return copy

    positions, channels = a_in.shape
    tokens, feats = b_in.shape
    width = feats * count_tp
    flat = a_re.shape[1]
    states = state_size
    group_ch = in_re.shape[0] * states // flat
    slots = rows_x.shape[0]
    cap = slots // count_ep
    tile = min(256, flat)
    tiles = flat // tile
    tile_ch = tile // states * group_ch
    steps = positions // CHUNKS
    hid = w_gate.shape[1]
    expert_rows = max(16, count_ep)
    my_cols = pl.ds(pl.multiple_of(tp * feats, 128), feats)

    loads[10].wait()
    loads[0].wait()
    mine_stats[:, :tokens] = row_sums(b_in[...])
    mine_stats[:, tokens:] = row_sums(a_in[...])
    pl.semaphore_wait(barrier, count_ep + count_tp - 2)
    stat_copies = [
        send(mine_stats, slot_stats.at[k], st_s.at[k], st_r.at[k], tp=lax.rem(tp + k, count_tp))
        for k in range(1, count_tp)
    ]

    loads[12].wait()
    loads[13].wait()
    expert_of = iota((expert_rows, tokens), 0)
    hit = jnp.zeros((expert_rows, tokens), jnp.bool_)
    weight = jnp.zeros((expert_rows, tokens), f32)
    for k in range(routes_in.shape[0]):
        this = routes_in[k : k + 1, :] == expert_of
        hit = jnp.logical_or(hit, this)
        weight = jnp.where(this, weight_in[k : k + 1, :], weight)
    before = (iota((tokens, tokens), 0) < iota((tokens, tokens), 1)).astype(bf16)
    place = nn(hit.astype(f32).astype(bf16), before)
    place = jnp.where(hit, place, -1.0).astype(bf16)
    owner = jnp.concatenate(
        [
            (iota((cap, expert_rows), 1) == partner(me, k)).astype(f32)
            for k in range(count_ep)
        ],
        axis=0,
    ).astype(bf16)
    chosen = nn(owner, place) == (iota((slots, tokens), 0) % cap).astype(f32)
    weight_hi = weight.astype(bf16)
    weight_lo = (weight - weight_hi.astype(f32)).astype(bf16)
    share_hi[...] = jnp.where(chosen, nn(owner, weight_hi), 0.0).astype(bf16)
    share_lo[...] = jnp.where(chosen, nn(owner, weight_lo), 0.0).astype(bf16)
    chosen = chosen.astype(f32).astype(bf16)

    loads[1].wait()
    order = (
        iota((positions, positions), 1)
        == (iota((positions, positions), 0) % CHUNKS) * steps
        + iota((positions, positions), 0) // CHUNKS
    ).astype(f32).astype(bf16)
    order_t = (
        iota((positions, positions), 0)
        == (iota((positions, positions), 1) % CHUNKS) * steps
        + iota((positions, positions), 1) // CHUNKS
    ).astype(f32).astype(bf16)
    step = step_in[...]
    groups = step.shape[0]
    high = step.astype(bf16).astype(f32)
    middle = (step - high).astype(bf16).astype(f32)
    low = step - high - middle
    parts = [high, middle, low]
    padded = -(-3 * groups // 16) * 16
    if padded > 3 * groups:
        parts.append(jnp.zeros((padded - 3 * groups, positions), f32))
    split = jnp.concatenate(parts, axis=0).astype(bf16)
    split = nn(split, order_t).astype(bf16)
    for t in range(tiles):
        lanes = slice(t * tile, (t + 1) * tile)
        source = iota((padded, tile), 0)
        pick = jnp.logical_and(
            source % groups == iota((padded, tile), 1) // states + t * (tile // states),
            source < 3 * groups,
        )
        a_re[:, lanes] = tn(split, pick.astype(f32).astype(bf16))

    for copy in stat_copies:
        copy.wait_recv()
    total = mine_stats[...]
    for k in range(1, count_tp):
        total = total + slot_stats[k]
    total = total.T

    loads[11].wait()
    normed = normalize(b_in[...], total[:tokens], gain_b[...], width).astype(bf16)
    outgoing[...] = nn(chosen, normed).astype(bf16)
    arrivals = [None]
    for k in range(1, count_ep):
        here = pl.ds(k * cap, cap)
        arrivals.append(
            send(
                outgoing.at[here], rows_x.at[here, my_cols], aa_s.at[k], aa_r.at[k],
                ep=partner(me, k),
            )
        )
    rows_x[0:cap, my_cols] = outgoing[0:cap, :]

    per_group = count_ep // groups_y
    group_rows = per_group * cap
    y_arrivals, sib_arrivals = {}, []

    def core_cols(offset):
        owner_tp = lax.rem(my_y + count_y - offset, count_y) * CORES + my_core
        return pl.ds(pl.multiple_of(owner_tp * feats, 128), feats)

    def to_sibling(offset, g):
        here = rows_x.at[pl.ds(g * group_rows, group_rows), core_cols(offset)]
        sib_arrivals.append((g, send(here, here, ds_s.at[offset, g], ds_r.at[offset, g], tp=sibling)))

    def forward(g):
        for k in range(max(1, g * per_group), (g + 1) * per_group):
            arrivals[k].wait_recv()
        here = rows_x.at[pl.ds(g * group_rows, group_rows), my_cols]
        for k in range(1, count_y):
            y_arrivals[k, g] = send(
                here, here, dy_s.at[k, g], dy_r.at[k, g],
                tp=lax.rem(my_y + k, count_y) * CORES + my_core,
            )
        to_sibling(0, g)

    def forward_again(g):
        for k in range(1, count_y):
            y_arrivals[k, g].wait_recv()
            to_sibling(k, g)

    forward(0)

    loads[2].wait()
    normed = normalize(a_in[...], total[tokens:], gain_a[...], width).astype(bf16)
    normed = nn(order, normed).astype(bf16)
    loads[3].wait()
    for i in (4, 5, 6, 7):
        loads[i].wait()
    block = min(32, positions)

    def first_half(t):
        lanes = slice(t * tile, (t + 1) * tile)
        table = slice(t * tile_ch, (t + 1) * tile_ch)
        piece = normed[:, table]
        u_re[:, lanes] = nn(piece, spread(in_re[table, :], group_ch, tile, states))
        u_im[:, lanes] = nn(piece, spread(in_im[table, :], group_ch, tile, states))
        p_re, p_im = pole_in[0:1, lanes], pole_in[1:2, lanes]
        d_re, d_im = pole_in[2:3, lanes], pole_in[3:4, lanes]

        def elementwise(i, passed):
            here = pl.ds(pl.multiple_of(i * block, block), block)
            delta = a_re[here, lanes]
            for j in range(block // CHUNKS):
                passed = passed + delta[j * CHUNKS : (j + 1) * CHUNKS]
            magnitude = jnp.exp(p_re * delta)
            sine, cosine = sin_cos(p_im * delta)
            ab_re = magnitude * cosine
            ab_im = magnitude * sine
            numer = ab_re - 1.0
            k_re = numer * d_re + ab_im * d_im
            k_im = ab_im * d_re - numer * d_im
            v_re, v_im = u_re[here, lanes], u_im[here, lanes]
            a_re[here, lanes] = ab_re
            a_im[here, lanes] = ab_im
            u_re[here, lanes] = k_re * v_re - k_im * v_im
            u_im[here, lanes] = k_re * v_im + k_im * v_re
            return passed

        passed = lax.fori_loop(
            0, positions // block, elementwise, jnp.zeros((CHUNKS, tile), f32)
        )
        magnitude = jnp.exp(p_re * passed)
        sine, cosine = sin_cos(p_im * passed)
        sums[0, :, lanes] = magnitude * cosine
        sums[1, :, lanes] = magnitude * sine

    span = min(1024, flat)

    def chunk_sums(base):
        lanes = slice(base, base + span)

        def one(s, carried):
            s_re, s_im = carried
            here = pl.ds(pl.multiple_of(s * CHUNKS, CHUNKS), CHUNKS)
            b_re, b_im = a_re[here, lanes], a_im[here, lanes]
            return (
                b_re * s_re - b_im * s_im + u_re[here, lanes],
                b_re * s_im + b_im * s_re + u_im[here, lanes],
            )

        zero = jnp.zeros((CHUNKS, span), f32)
        sums[2, :, lanes], sums[3, :, lanes] = lax.fori_loop(0, steps, one, (zero, zero), unroll=2)

    work = [functools.partial(first_half, t) for t in range(tiles)]
    work += [functools.partial(chunk_sums, base) for base in range(0, flat, span)]
    early = groups_y // 2
    for n, do in enumerate(work):
        do()
        if n + 1 < early:
            forward(n + 1)
        if 0 <= n - 1 < early:
            forward_again(n - 1)
    done = len(work)
    for g in range(done + 1, early):
        forward(g)
    for g in range(max(0, done - 1), early):
        forward_again(g)

    def chunk(index, c):
        return sums[index, c : c + 1, :]

    c_re, c_im, s_re, s_im = (chunk(index, 0) for index in range(4))
    for c in range(1, CHUNKS):
        b_re, b_im = chunk(0, c), chunk(1, c)
        c_re, c_im = b_re * c_re - b_im * c_im, b_re * c_im + b_im * c_re
        s_re, s_im = (
            b_re * s_re - b_im * s_im + chunk(2, c),
            b_re * s_im + b_im * s_re + chunk(3, c),
        )
    mine_state[0:1, :] = c_re
    mine_state[1:2, :] = c_im
    mine_state[2:3, :] = s_re
    mine_state[3:4, :] = s_im
    state_copies = [
        send(mine_state, slot_state.at[me], hs_s.at[k], hs_r.at[k], ep=partner(me, k))
        for k in range(1, count_ep)
    ]

    expert_half = slots // halves
    columns = min(256, hid)
    out_columns = min(256, feats)
    groups_half = groups_y // halves

    def hidden_units(h, between):
        top = pl.ds(h * expert_half, expert_half)
        for n in range(hid // columns):
            cols = slice(n * columns, (n + 1) * columns)
            gate = nn(rows_x[top, :], w_gate[:, cols])
            up = nn(rows_x[top, :], w_up[:, cols])
            hidden[top, cols] = (gate * jax.nn.sigmoid(gate) * up).astype(bf16)
            between(n)

    sib_copies, y_copies = {}, {}

    def down(h, target_tp, store):
        top = slice(h * expert_half, (h + 1) * expert_half)
        for n in range(feats // out_columns):
            first = pl.multiple_of(target_tp * feats + n * out_columns, 128)
            store(
                top, slice(n * out_columns, (n + 1) * out_columns),
                nn(hidden[top, :], w_down[:, pl.ds(first, out_columns)]),
            )

    def give_back(h):
        top = slice(h * expert_half, (h + 1) * expert_half)
        for offset in list(range(1, count_y)) + [0]:
            yt = lax.rem(my_y + offset, count_y) * CORES

            def to_send(rows, cols, value, offset=offset):
                sib_send[offset, rows, cols] = value.astype(bf16)

            def to_own(rows, cols, value):
                own[rows, cols] = value

            down(h, yt + 1 - my_core, to_send)
            window = pl.ds(h * expert_half, expert_half)
            sib_copies[h, offset] = send(
                sib_send.at[offset, window], sib_recv.at[offset, window],
                rs_s.at[offset, h], rs_r.at[offset, h], tp=sibling,
            )
            down(h, yt + my_core, to_own)
            if offset == 0:
                continue
            sib_copies[h, offset].wait_recv()
            y_send[offset, top, :] = (
                own[top, :] + sib_recv[offset, top, :].astype(f32)
            ).astype(bf16)
            for g in range(h * groups_half, (h + 1) * groups_half):
                window = pl.ds(g * group_rows, group_rows)
                y_copies[offset, g] = send(
                    y_send.at[offset, window], y_recv.at[offset, window],
                    ry_s.at[offset, g], ry_r.at[offset, g], tp=yt + my_core,
                )

    back_copies = {}

    def finish(g):
        window = slice(g * group_rows, (g + 1) * group_rows)
        total = own[window, :] + sib_recv[0, window, :].astype(f32)
        for offset in range(1, count_y):
            y_copies[offset, g].wait_recv()
            total = total + y_recv[offset, window, :].astype(f32)
        total = total.astype(bf16)
        final[window, :] = total
        if g == 0:
            returned[0:cap, :] = total[0:cap]
        for k in range(max(1, g * per_group), (g + 1) * per_group):
            here = pl.ds(k * cap, cap)
            back_copies[k] = send(
                final.at[here], returned.at[here], ra_s.at[k], ra_r.at[k], ep=partner(me, k)
            )

    def rows_ready(low, high):
        for g, copy in list(sib_arrivals):
            if low <= g < high:
                copy.wait_recv()

    loads[14].wait()
    loads[15].wait()
    rows_ready(0, early)

    def forwards(n):
        if early + n < groups_y:
            forward(early + n)

    hidden_units(0, forwards)
    for g in range(early + hid // columns, groups_y):
        forward(g)
    loads[16].wait()
    give_back(0)
    for g in range(early, groups_y):
        forward_again(g)

    for copy in state_copies:
        copy.wait_recv()

    def fold(q, carried):
        h_re, h_im = carried
        b_re, b_im = slot_state[q, 0:1, :], slot_state[q, 1:2, :]
        return (
            b_re * h_re - b_im * h_im + slot_state[q, 2:3, :],
            b_re * h_im + b_im * h_re + slot_state[q, 3:4, :],
        )

    blank = jnp.zeros((1, flat), f32)
    h_re, h_im = lax.fori_loop(0, me, fold, (blank, blank))
    for c in range(CHUNKS):
        enter[0, c : c + 1, :] = h_re
        enter[1, c : c + 1, :] = h_im
        b_re, b_im = chunk(0, c), chunk(1, c)
        h_re, h_im = (
            b_re * h_re - b_im * h_im + chunk(2, c),
            b_re * h_im + b_im * h_re + chunk(3, c),
        )
    for base in range(0, flat, span):
        lanes = slice(base, base + span)

        def advance(s, carried, lanes=lanes):
            s_re, s_im = carried
            found_re, found_im = [], []
            for j in range(2):
                here = pl.ds(pl.multiple_of(s * 2 * CHUNKS + j * CHUNKS, CHUNKS), CHUNKS)
                b_re, b_im = a_re[here, lanes], a_im[here, lanes]
                s_re, s_im = (
                    b_re * s_re - b_im * s_im + u_re[here, lanes],
                    b_re * s_im + b_im * s_re + u_im[here, lanes],
                )
                found_re.append(s_re)
                found_im.append(s_im)
            both = pl.ds(pl.multiple_of(s * 2 * CHUNKS, 2 * CHUNKS), 2 * CHUNKS)
            n_re[both, lanes] = jnp.concatenate(found_re, axis=0).astype(bf16)
            n_im[both, lanes] = jnp.concatenate(found_im, axis=0).astype(bf16)
            return s_re, s_im

        lax.fori_loop(0, steps // 2, advance, (enter[0, :, lanes], enter[1, :, lanes]))
    for t in range(tiles):
        lanes = slice(t * tile, (t + 1) * tile)
        table = slice(t * tile_ch, (t + 1) * tile_ch)
        response = nt(n_re[:, lanes], spread(rd_re[table, :], group_ch, tile, states)) - nt(
            n_im[:, lanes], spread(rd_im[table, :], group_ch, tile, states)
        )
        mixed[:, table] = jax.nn.gelu(response).astype(bf16)
    mixed_cols = pl.ds(pl.multiple_of(tp * channels, 128), channels)
    mixed_all[:, mixed_cols] = nn(order_t, mixed[...]).astype(bf16)

    def mixed_window(offset):
        owner_tp = lax.rem(my_y + count_y - offset, count_y) * CORES + my_core
        return mixed_all.at[:, pl.ds(pl.multiple_of(owner_tp * channels, 128), channels)]

    mixed_y = {}
    for k in range(1, count_y):
        mixed_y[k] = send(
            mixed_window(0), mixed_window(0), my_s.at[k], my_r.at[k],
            tp=lax.rem(my_y + k, count_y) * CORES + my_core,
        )
    mixed_sib = [send(mixed_window(0), mixed_window(0), ms_s.at[0], ms_r.at[0], tp=sibling)]

    if halves > 1:
        rows_ready(early, groups_y)
        hidden_units(1, lambda n: None)
    for k in range(1, count_y):
        mixed_y[k].wait_recv()
        mixed_sib.append(
            send(mixed_window(k), mixed_window(k), ms_s.at[k], ms_r.at[k], tp=sibling)
        )
    if halves > 1:
        sib_copies[0, 0].wait_recv()
        for g in range(groups_half):
            finish(g)
        give_back(1)

    loads[8].wait()
    loads[9].wait()
    for copy in mixed_sib:
        copy.wait_recv()
    out_a_cols = min(256, out_a.shape[1])
    for n in range(out_a.shape[1] // out_a_cols):
        cols = slice(n * out_a_cols, (n + 1) * out_a_cols)
        value = nn(mixed_all[...], w_value[:, cols])
        gate = nn(mixed_all[...], w_gate_out[:, cols])
        out_a[:, cols] = (value * jax.nn.sigmoid(gate)).astype(bf16)

    sib_copies[halves - 1, 0].wait_recv()
    for g in range(groups_half * (halves - 1), groups_y):
        finish(g)
    for k in range(1, count_ep):
        back_copies[k].wait_recv()
    out_b[...] = (tn(share_hi[...], returned[...]) + tn(share_lo[...], returned[...])).astype(bf16)
    for copy in pending:
        copy.wait_send()


def fused(args, state_size, capacity):
    count_ep, count_tp = lax.axis_size("ep"), lax.axis_size("tp")
    count_y = count_tp // CORES
    positions, channels = args[0].shape
    groups = args[1].shape[0]
    tokens, feats = args[10].shape
    flat = args[3].shape[1]
    slots = count_ep * capacity
    hid = args[14].shape[1]
    width = feats * count_tp
    groups_y, halves = min(count_ep, 8), 2
    dma = pltpu.SemaphoreType.DMA
    vmem = pltpu.VMEM
    scratch = [vmem(x.shape, x.dtype) for x in args] + [
        vmem((8, tokens + positions), f32),
        vmem((count_tp, 8, tokens + positions), f32),
        vmem((slots, feats), bf16),
        vmem((slots, width), bf16),
        vmem((slots, tokens), bf16),
        vmem((slots, tokens), bf16),
        vmem((positions, flat), f32),
        vmem((positions, flat), f32),
        vmem((positions, flat), f32),
        vmem((positions, flat), f32),
        vmem((4, CHUNKS, flat), f32),
        vmem((2, CHUNKS, flat), f32),
        vmem((4, flat), f32),
        vmem((count_ep, 4, flat), f32),
        vmem((positions, flat), bf16),
        vmem((positions, flat), bf16),
        vmem((positions, channels), bf16),
        vmem((positions, channels * count_tp), bf16),
        vmem((slots, hid), bf16),
        vmem((slots, feats), f32),
        vmem((count_y, slots, feats), bf16),
        vmem((count_y, slots, feats), bf16),
        vmem((count_y, slots, feats), bf16),
        vmem((count_y, slots, feats), bf16),
        vmem((slots, feats), bf16),
        vmem((slots, feats), bf16),
        dma((len(args),)),
        dma((count_tp,)), dma((count_tp,)),
        dma((count_ep,)), dma((count_ep,)),
        dma((count_y, groups_y)), dma((count_y, groups_y)),
        dma((count_y, groups_y)), dma((count_y, groups_y)),
        dma((count_ep,)), dma((count_ep,)),
        dma((count_y,)), dma((count_y,)),
        dma((count_y,)), dma((count_y,)),
        dma((count_y, halves)), dma((count_y, halves)),
        dma((count_y, groups_y)), dma((count_y, groups_y)),
        dma((count_ep,)), dma((count_ep,)),
    ]
    return pl.pallas_call(
        functools.partial(kernel, (count_ep, count_tp, groups_y, halves, state_size)),
        out_shape=[
            jax.ShapeDtypeStruct((positions, args[8].shape[1]), bf16),
            jax.ShapeDtypeStruct((tokens, feats), bf16),
        ],
        in_specs=[pl.BlockSpec(memory_space=pl.ANY)] * len(args),
        out_specs=[pl.BlockSpec(memory_space=pltpu.VMEM)] * 2,
        scratch_shapes=scratch,
        compiler_params=pltpu.CompilerParams(
            collective_id=0, has_side_effects=True, vmem_limit_bytes=60 * 1024 * 1024
        ),
    )(*args)


def shards(
    mixer_input, mixer_gain, time_step, pole_real, pole_imag, input_real, input_imag,
    read_real, read_imag, out_value, out_gate, expert_input, expert_gain, routes,
    route_weight, expert_gate, expert_up, expert_down,
):
    tokens, top = routes.shape
    capacity = 2 * top * tokens // lax.axis_size("ep")
    flat_real = pole_real.reshape(-1)
    flat_imag = pole_imag.reshape(-1)
    denom = flat_real * flat_real + flat_imag * flat_imag
    pole = jnp.stack([flat_real, flat_imag, flat_real / denom, flat_imag / denom])

    def by_channel(table):
        return jnp.swapaxes(table, 1, 2).reshape(-1, table.shape[1])

    args = (
        mixer_input, time_step.T, mixer_gain[None, :], pole,
        by_channel(input_real), by_channel(input_imag),
        read_real.reshape(-1, read_real.shape[2]), read_imag.reshape(-1, read_imag.shape[2]),
        out_value, out_gate, expert_input, expert_gain[None, :], routes.T, route_weight.T,
        expert_gate[0], expert_up[0], expert_down[0],
    )
    return tuple(fused(args, pole_real.shape[1], capacity))


def solution(mesh):
    return jax.shard_map(
        shards,
        mesh=mesh,
        in_specs=(
            P("ep", "tp"), P("tp"), P("ep", "tp"), P("tp", None), P("tp", None),
            P("tp", None, None), P("tp", None, None), P("tp", None, None), P("tp", None, None),
            P(None, "tp"), P(None, "tp"), P("ep", "tp"), P("tp"), P("ep", None), P("ep", None),
            P("ep", None, "tp"), P("ep", None, "tp"), P("ep", "tp", None),
        ),
        out_specs=(P("ep", "tp"), P("ep", "tp")),
        check_vma=False,
    )
```

```python
import functools
import jax
import jax.numpy as jnp
from jax import lax
from jax.experimental import pallas as pl
from jax.experimental.pallas import tpu as pltpu
from jax.sharding import PartitionSpec as P

norm_eps = 1e-05
CHUNKS = 8
CORES = 2
f32 = jnp.float32
bf16 = jnp.bfloat16


def sin_cos(angle):
    turns = jnp.round(angle * 0.6366197723675814)
    left = angle - turns * 1.5703125
    left = left - turns * 4.83751296997e-4
    left = left - turns * 7.549789948768648e-8
    sq = left * left
    sine = ((-1.9515295891e-4 * sq + 8.3321608736e-3) * sq - 1.6666654611e-1) * sq * left + left
    cosine = (
        ((2.443315711809948e-5 * sq - 1.388731625493765e-3) * sq + 4.166664568298827e-2) * sq * sq
        - 0.5 * sq
        + 1.0
    )
    quadrant = turns.astype(jnp.int32)
    odd = (quadrant & 1) == 1
    sin_out = jnp.where(odd, cosine, sine)
    cos_out = jnp.where(odd, sine, cosine)
    sin_out = jnp.where((quadrant & 2) == 2, -sin_out, sin_out)
    cos_out = jnp.where(((quadrant + 1) & 2) == 2, -cos_out, cos_out)
    return sin_out, cos_out


def iota(shape, dim):
    return lax.broadcasted_iota(jnp.int32, shape, dim)


def nn(left, right):
    return jnp.dot(left, right, preferred_element_type=f32)


def nt(left, right):
    return lax.dot_general(left, right, (((1,), (1,)), ((), ())), preferred_element_type=f32)


def tn(left, right):
    return lax.dot_general(left, right, (((0,), (0,)), ((), ())), preferred_element_type=f32)


def partner(me, k):
    other, bit = me, 1
    while bit <= k:
        if k & bit:
            other = other + bit * (1 - 2 * ((me // bit) % 2))
        bit *= 2
    return other


def spread(table, row_div, lanes, lane_div):
    rows, width = table.shape
    pick = (iota((width, lanes), 0) == iota((width, lanes), 1) % width).astype(bf16)
    wide = nn(table.astype(bf16), pick)
    same = iota((rows, lanes), 0) // row_div == iota((rows, lanes), 1) // lane_div
    return jnp.where(same, wide, 0.0).astype(bf16)


def row_sums(rows):
    ones = jnp.ones((16, rows.shape[1]), bf16)
    wide = rows.astype(f32)
    square = wide * wide
    high = square.astype(bf16)
    low = (square - high.astype(f32)).astype(bf16)
    sums = nt(ones, rows)
    squares = nt(ones, high) + nt(ones, low)
    return jnp.where(iota((8, 1), 0) == 0, sums[:8], squares[:8])


def normalize(rows, stats, gain, width):
    average = stats[:, 0:1] / width
    variance = stats[:, 1:2] / width - average * average
    return (rows.astype(f32) - average) * lax.rsqrt(variance + norm_eps) * gain


def kernel(dims, *refs):
    count_ep, count_tp, groups_y, halves, state_size = dims
    hbm, refs = refs[:18], refs[18:]
    (out_a, out_b), refs = refs[:2], refs[2:]
    vm, refs = refs[:18], refs[18:]
    (
        mine_stats, slot_stats, pole, tokens_far, routes_far, gain_all, rows_n, outgoing, rows_x, share_hi, share_lo, a_re, a_im, u_re, u_im,
        sums, enter, mine_state, slot_state, n_re, n_im, mixed, mixed_all, hidden, own,
        sib_send, sib_recv, y_send, y_recv, final, returned,
        sem_in, far_s, far_r, gn_s, gn_r, st_s, st_r, aa_s, aa_r, dy_s, dy_r, ds_s, ds_r, hs_s, hs_r,
        my_s, my_r, ms_s, ms_r, rs_s, rs_r, ry_s, ry_r, ra_s, ra_r,
    ) = refs
    (
        a_in, step_in, gain_a, real_in, in_re, in_im, rd_re, rd_im, w_value, w_gate_out,
        b_in, gain_b, routes_in, weight_in, w_gate, w_up, w_down, imag_in,
    ) = vm

    me = lax.axis_index("ep")
    tp = lax.axis_index("tp")
    count_y = count_tp // CORES
    my_y = tp // CORES
    my_core = tp % CORES
    sibling = my_y * CORES + 1 - my_core

    barrier = pltpu.get_barrier_semaphore()
    for k in range(1, count_ep):
        pl.semaphore_signal(
            barrier, inc=1, device_id={"ep": partner(me, k)}, device_id_type=pl.DeviceIdType.MESH
        )
    for k in range(1, count_tp):
        pl.semaphore_signal(
            barrier, inc=1, device_id={"tp": lax.rem(tp + k, count_tp)},
            device_id_type=pl.DeviceIdType.MESH,
        )

    loads = [
        pltpu.make_async_copy(source, target, sem_in.at[i])
        for i, (source, target) in enumerate(zip(hbm, vm))
    ]
    for i in (10, 12, 11, 0, 1, 3, 17, 2, 13, 4, 5, 6, 7, 14, 15, 16, 8, 9):
        loads[i].start()

    pending = []

    def send(source, target, send_sem, recv_sem, **where):
        copy = pltpu.make_async_remote_copy(
            src_ref=source, dst_ref=target, send_sem=send_sem, recv_sem=recv_sem,
            device_id=where, device_id_type=pl.DeviceIdType.MESH,
        )
        copy.start()
        pending.append(copy)
        return copy

    positions, channels = a_in.shape
    tokens, feats = b_in.shape
    width = feats * count_tp
    flat = a_re.shape[1]
    states = state_size
    group_ch = in_re.shape[0] * states // flat
    slots = rows_x.shape[0]
    cap = slots // count_ep
    tile = min(256, flat)
    tiles = flat // tile
    tile_ch = tile // states * group_ch
    steps = positions // CHUNKS
    hid = w_gate.shape[1]
    expert_rows = max(16, count_ep)
    my_cols = pl.ds(pl.multiple_of(tp * feats, 128), feats)

    portal = partner(me, count_ep // 2)
    for i in (12, 11, 10):
        loads[i].wait()
    pl.semaphore_wait(barrier, count_ep + count_tp - 2)
    far_routes = send(routes_in, routes_far, far_s.at[0], far_r.at[0], ep=portal)
    far_tokens = send(b_in, tokens_far, far_s.at[1], far_r.at[1], ep=portal)
    gain_copies = [
        send(
            gain_b, gain_all.at[:, my_cols], gn_s.at[k], gn_r.at[k], tp=lax.rem(tp + k, count_tp)
        )
        for k in range(1, count_tp)
    ]
    gain_all[:, my_cols] = gain_b[...]
    near = count_ep // 2
    expert_of = iota((expert_rows, tokens), 0)
    before = (iota((tokens, tokens), 0) < iota((tokens, tokens), 1)).astype(bf16)

    def places(routes):
        hit = jnp.zeros((expert_rows, tokens), jnp.bool_)
        for k in range(routes.shape[0]):
            hit = jnp.logical_or(hit, routes[k : k + 1, :] == expert_of)
        place = nn(hit.astype(f32).astype(bf16), before)
        return jnp.where(hit, place, -1.0).astype(bf16)

    def owners(low, high):
        return jnp.concatenate(
            [
                (iota((cap, expert_rows), 1) == partner(me, k)).astype(f32)
                for k in range(low, high)
            ],
            axis=0,
        ).astype(bf16)

    def select(owner, place):
        return nn(owner, place) == (iota((owner.shape[0], tokens), 0) % cap).astype(f32)

    place_own = places(routes_in[...])
    owner_near = owners(0, near)
    chosen_near = select(owner_near, place_own)
    chosen = chosen_near.astype(f32).astype(bf16)

    arrivals = {}

    def hand_out(base, values):
        outgoing[base * cap : (base + near) * cap, :] = values
        for k in range(1, near):
            here = pl.ds((base + k) * cap, cap)
            arrivals[base + k] = send(
                outgoing.at[here], rows_x.at[here, my_cols], aa_s.at[base + k],
                aa_r.at[base + k], ep=partner(me, k),
            )
        rows_x[base * cap : (base + 1) * cap, my_cols] = values[0:cap]

    per_group = count_ep // groups_y
    group_rows = per_group * cap
    y_arrivals, sib_arrivals = {}, []

    def core_cols(offset):
        owner_tp = lax.rem(my_y + count_y - offset, count_y) * CORES + my_core
        return pl.ds(pl.multiple_of(owner_tp * feats, 128), feats)

    def to_sibling(offset, g):
        here = rows_x.at[pl.ds(g * group_rows, group_rows), core_cols(offset)]
        sib_arrivals.append((g, send(here, here, ds_s.at[offset, g], ds_r.at[offset, g], tp=sibling)))

    def forward(g):
        for k in range(g * per_group, (g + 1) * per_group):
            if k in arrivals:
                arrivals[k].wait_recv()
        here = rows_x.at[pl.ds(g * group_rows, group_rows), my_cols]
        for k in range(1, count_y):
            y_arrivals[k, g] = send(
                here, here, dy_s.at[k, g], dy_r.at[k, g],
                tp=lax.rem(my_y + k, count_y) * CORES + my_core,
            )
        to_sibling(0, g)

    def forward_again(g):
        for k in range(1, count_y):
            y_arrivals[k, g].wait_recv()
            to_sibling(k, g)

    hand_out(0, nn(chosen, b_in[...]).astype(bf16))
    forward(0)
    loads[0].wait()
    mine_stats[...] = row_sums(a_in[...])
    stat_copies = [
        send(mine_stats, slot_stats.at[k], st_s.at[k], st_r.at[k], tp=lax.rem(tp + k, count_tp))
        for k in range(1, count_tp)
    ]

    loads[1].wait()
    order = (
        iota((positions, positions), 1)
        == (iota((positions, positions), 0) % CHUNKS) * steps
        + iota((positions, positions), 0) // CHUNKS
    ).astype(f32).astype(bf16)
    order_t = (
        iota((positions, positions), 0)
        == (iota((positions, positions), 1) % CHUNKS) * steps
        + iota((positions, positions), 1) // CHUNKS
    ).astype(f32).astype(bf16)
    step = step_in[...]
    groups = step.shape[0]
    high = step.astype(bf16).astype(f32)
    middle = (step - high).astype(bf16).astype(f32)
    low = step - high - middle
    parts = [high, middle, low]
    padded = -(-3 * groups // 16) * 16
    if padded > 3 * groups:
        parts.append(jnp.zeros((padded - 3 * groups, positions), f32))
    split = jnp.concatenate(parts, axis=0).astype(bf16)
    split = nn(split, order_t).astype(bf16)
    for t in range(tiles):
        lanes = slice(t * tile, (t + 1) * tile)
        source = iota((padded, tile), 0)
        pick = jnp.logical_and(
            source % groups == iota((padded, tile), 1) // states + t * (tile // states),
            source < 3 * groups,
        )
        a_re[:, lanes] = tn(split, pick.astype(f32).astype(bf16))

    loads[3].wait()
    loads[17].wait()
    pick = (iota((states, flat), 0) == iota((states, flat), 1) % states).astype(f32).astype(bf16)
    own_lane = iota((groups, flat), 0) == iota((groups, flat), 1) // states

    def to_lanes(table):
        high = table.astype(bf16)
        rest = table - high.astype(f32)
        middle = rest.astype(bf16)
        low = (rest - middle.astype(f32)).astype(bf16)
        wide = nn(high, pick) + (nn(middle, pick) + nn(low, pick))
        return jnp.sum(jnp.where(own_lane, wide, 0.0), axis=0, keepdims=True)

    real, imag = to_lanes(real_in[...]), to_lanes(imag_in[...])
    denom = real * real + imag * imag
    pole[0:1, :] = real
    pole[1:2, :] = imag
    pole[2:3, :] = real / denom
    pole[3:4, :] = imag / denom
    block = min(32, positions)

    def steps_of(t):
        lanes = slice(t * tile, (t + 1) * tile)
        p_re, p_im = pole[0:1, lanes], pole[1:2, lanes]
        d_re, d_im = pole[2:3, lanes], pole[3:4, lanes]

        def elementwise(i, passed):
            here = pl.ds(pl.multiple_of(i * block, block), block)
            delta = a_re[here, lanes]
            for j in range(block // CHUNKS):
                passed = passed + delta[j * CHUNKS : (j + 1) * CHUNKS]
            magnitude = jnp.exp(p_re * delta)
            sine, cosine = sin_cos(p_im * delta)
            ab_re = magnitude * cosine
            ab_im = magnitude * sine
            numer = ab_re - 1.0
            a_re[here, lanes] = ab_re
            a_im[here, lanes] = ab_im
            u_re[here, lanes] = numer * d_re + ab_im * d_im
            u_im[here, lanes] = ab_im * d_re - numer * d_im
            return passed

        passed = lax.fori_loop(
            0, positions // block, elementwise, jnp.zeros((CHUNKS, tile), f32)
        )
        magnitude = jnp.exp(p_re * passed)
        sine, cosine = sin_cos(p_im * passed)
        sums[0, :, lanes] = magnitude * cosine
        sums[1, :, lanes] = magnitude * sine

    forward(1)
    for t in range(tiles):
        steps_of(t)
    forward_again(0)
    far_routes.wait_recv()
    chosen_far = select(owner_near, places(routes_far[...])).astype(f32).astype(bf16)
    for copy in stat_copies:
        copy.wait_recv()
    total = mine_stats[...]
    for k in range(1, count_tp):
        total = total + slot_stats[k]
    total = total.T

    loads[2].wait()
    normed = normalize(a_in[...], total, gain_a[...], width).astype(bf16)
    normed = nn(order, normed).astype(bf16)
    for i in (4, 5, 6, 7):
        loads[i].wait()

    def first_half(t):
        lanes = slice(t * tile, (t + 1) * tile)
        table = slice(t * tile_ch, (t + 1) * tile_ch)
        piece = normed[:, table]
        v_re = nn(piece, spread(in_re[table, :], group_ch, tile, states))
        v_im = nn(piece, spread(in_im[table, :], group_ch, tile, states))
        k_re, k_im = u_re[:, lanes], u_im[:, lanes]
        u_re[:, lanes] = k_re * v_re - k_im * v_im
        u_im[:, lanes] = k_re * v_im + k_im * v_re

    span = min(1024, flat)

    def chunk_sums(base):
        lanes = slice(base, base + span)

        def one(s, carried):
            s_re, s_im = carried
            here = pl.ds(pl.multiple_of(s * CHUNKS, CHUNKS), CHUNKS)
            b_re, b_im = a_re[here, lanes], a_im[here, lanes]
            return (
                b_re * s_re - b_im * s_im + u_re[here, lanes],
                b_re * s_im + b_im * s_re + u_im[here, lanes],
            )

        zero = jnp.zeros((CHUNKS, span), f32)
        sums[2, :, lanes], sums[3, :, lanes] = lax.fori_loop(0, steps, one, (zero, zero), unroll=2)

    early = groups_y // 2
    for t in range(tiles // 2):
        first_half(t)
    for g in range(2, early):
        forward(g)
    for t in range(tiles // 2, tiles):
        first_half(t)
    for base in range(0, flat, span):
        chunk_sums(base)
    def chunk(index, c):
        return sums[index, c : c + 1, :]

    c_re, c_im, s_re, s_im = (chunk(index, 0) for index in range(4))
    for c in range(1, CHUNKS):
        b_re, b_im = chunk(0, c), chunk(1, c)
        c_re, c_im = b_re * c_re - b_im * c_im, b_re * c_im + b_im * c_re
        s_re, s_im = (
            b_re * s_re - b_im * s_im + chunk(2, c),
            b_re * s_im + b_im * s_re + chunk(3, c),
        )
    mine_state[0:1, :] = c_re
    mine_state[1:2, :] = c_im
    mine_state[2:3, :] = s_re
    mine_state[3:4, :] = s_im
    state_copies = [
        send(mine_state, slot_state.at[me], hs_s.at[k], hs_r.at[k], ep=partner(me, k))
        for k in range(1, count_ep)
    ]

    far_tokens.wait_recv()
    hand_out(near, nn(chosen_far, tokens_far[...]).astype(bf16))
    forward(early)
    for g in range(1, early):
        forward_again(g)
    loads[13].wait()
    weight = jnp.zeros((expert_rows, tokens), f32)
    for k in range(routes_in.shape[0]):
        this = routes_in[k : k + 1, :] == expert_of
        weight = jnp.where(this, weight_in[k : k + 1, :], weight)
    weight_hi = weight.astype(bf16)
    weight_lo = (weight - weight_hi.astype(f32)).astype(bf16)
    owner_far = owners(near, count_ep)
    for rows, owner, here in (
        (slice(0, near * cap), owner_near, chosen_near),
        (slice(near * cap, slots), owner_far, select(owner_far, place_own)),
    ):
        share_hi[rows, :] = jnp.where(here, nn(owner, weight_hi), 0.0).astype(bf16)
        share_lo[rows, :] = jnp.where(here, nn(owner, weight_lo), 0.0).astype(bf16)

    expert_half = slots // halves
    columns = min(256, hid)
    out_columns = min(256, feats)
    groups_half = groups_y // halves

    def normalize_rows(h):
        step_rows = min(64, expert_half)
        for r in range(h * expert_half, (h + 1) * expert_half, step_rows):
            rows = slice(r, r + step_rows)
            wide = rows_x[rows, :].astype(f32)
            average = jnp.sum(wide, axis=1, keepdims=True) / width
            square = jnp.sum(wide * wide, axis=1, keepdims=True) / width
            variance = square - average * average
            wide = (wide - average) * lax.rsqrt(variance + norm_eps) * gain_all[...]
            rows_n[rows, :] = wide.astype(bf16)

    def hidden_units(h, between):
        top = pl.ds(h * expert_half, expert_half)
        for n in range(hid // columns):
            cols = slice(n * columns, (n + 1) * columns)
            gate = nn(rows_n[top, :], w_gate[:, cols])
            up = nn(rows_n[top, :], w_up[:, cols])
            hidden[top, cols] = (gate * jax.nn.sigmoid(gate) * up).astype(bf16)
            between(n)

    sib_copies, y_copies = {}, {}

    def down(h, target_tp, store):
        top = slice(h * expert_half, (h + 1) * expert_half)
        for n in range(feats // out_columns):
            first = pl.multiple_of(target_tp * feats + n * out_columns, 128)
            store(
                top, slice(n * out_columns, (n + 1) * out_columns),
                nn(hidden[top, :], w_down[:, pl.ds(first, out_columns)]),
            )

    def give_back(h, offsets):
        top = slice(h * expert_half, (h + 1) * expert_half)
        for offset in offsets:
            yt = lax.rem(my_y + offset, count_y) * CORES

            def to_send(rows, cols, value, offset=offset):
                sib_send[offset, rows, cols] = value.astype(bf16)

            def to_own(rows, cols, value):
                own[rows, cols] = value

            down(h, yt + 1 - my_core, to_send)
            window = pl.ds(h * expert_half, expert_half)
            sib_copies[h, offset] = send(
                sib_send.at[offset, window], sib_recv.at[offset, window],
                rs_s.at[offset, h], rs_r.at[offset, h], tp=sibling,
            )
            down(h, yt + my_core, to_own)
            if offset == 0:
                continue
            sib_copies[h, offset].wait_recv()
            y_send[offset, top, :] = (
                own[top, :] + sib_recv[offset, top, :].astype(f32)
            ).astype(bf16)
            for g in range(h * groups_half, (h + 1) * groups_half):
                window = pl.ds(g * group_rows, group_rows)
                y_copies[offset, g] = send(
                    y_send.at[offset, window], y_recv.at[offset, window],
                    ry_s.at[offset, g], ry_r.at[offset, g], tp=yt + my_core,
                )

    back_copies = {}

    def finish(g):
        window = slice(g * group_rows, (g + 1) * group_rows)
        total = own[window, :] + sib_recv[0, window, :].astype(f32)
        for offset in range(1, count_y):
            y_copies[offset, g].wait_recv()
            total = total + y_recv[offset, window, :].astype(f32)
        total = total.astype(bf16)
        final[window, :] = total
        if g == 0:
            returned[0:cap, :] = total[0:cap]
        for k in range(max(1, g * per_group), (g + 1) * per_group):
            here = pl.ds(k * cap, cap)
            back_copies[k] = send(
                final.at[here], returned.at[here], ra_s.at[k], ra_r.at[k], ep=partner(me, k)
            )

    def rows_ready(low, high):
        for g, copy in list(sib_arrivals):
            if low <= g < high:
                copy.wait_recv()

    rows_ready(0, early)
    for copy in gain_copies:
        copy.wait_recv()
    normalize_rows(0)
    forward(early + 1)
    loads[14].wait()
    loads[15].wait()

    def forwards(n):
        if early + 2 + n < groups_y:
            forward(early + 2 + n)

    hidden_units(0, forwards)
    for g in range(early + 2 + hid // columns, groups_y):
        forward(g)
    forward_again(early)
    forward_again(early + 1)
    for copy in state_copies:
        copy.wait_recv()

    def fold(q, carried):
        h_re, h_im = carried
        b_re, b_im = slot_state[q, 0:1, :], slot_state[q, 1:2, :]
        return (
            b_re * h_re - b_im * h_im + slot_state[q, 2:3, :],
            b_re * h_im + b_im * h_re + slot_state[q, 3:4, :],
        )

    blank = jnp.zeros((1, flat), f32)
    h_re, h_im = lax.fori_loop(0, me, fold, (blank, blank))
    for c in range(CHUNKS):
        enter[0, c : c + 1, :] = h_re
        enter[1, c : c + 1, :] = h_im
        b_re, b_im = chunk(0, c), chunk(1, c)
        h_re, h_im = (
            b_re * h_re - b_im * h_im + chunk(2, c),
            b_re * h_im + b_im * h_re + chunk(3, c),
        )
    for base in range(0, flat, span):
        lanes = slice(base, base + span)

        def advance(s, carried, lanes=lanes):
            s_re, s_im = carried
            found_re, found_im = [], []
            for j in range(2):
                here = pl.ds(pl.multiple_of(s * 2 * CHUNKS + j * CHUNKS, CHUNKS), CHUNKS)
                b_re, b_im = a_re[here, lanes], a_im[here, lanes]
                s_re, s_im = (
                    b_re * s_re - b_im * s_im + u_re[here, lanes],
                    b_re * s_im + b_im * s_re + u_im[here, lanes],
                )
                found_re.append(s_re)
                found_im.append(s_im)
            both = pl.ds(pl.multiple_of(s * 2 * CHUNKS, 2 * CHUNKS), 2 * CHUNKS)
            n_re[both, lanes] = jnp.concatenate(found_re, axis=0).astype(bf16)
            n_im[both, lanes] = jnp.concatenate(found_im, axis=0).astype(bf16)
            return s_re, s_im

        lax.fori_loop(0, steps // 2, advance, (enter[0, :, lanes], enter[1, :, lanes]))
    for t in range(tiles):
        lanes = slice(t * tile, (t + 1) * tile)
        table = slice(t * tile_ch, (t + 1) * tile_ch)
        response = nt(n_re[:, lanes], spread(rd_re[table, :], group_ch, tile, states)) - nt(
            n_im[:, lanes], spread(rd_im[table, :], group_ch, tile, states)
        )
        mixed[:, table] = jax.nn.gelu(response).astype(bf16)
    mixed_cols = pl.ds(pl.multiple_of(tp * channels, 128), channels)
    mixed_all[:, mixed_cols] = nn(order_t, mixed[...]).astype(bf16)

    def mixed_window(offset):
        owner_tp = lax.rem(my_y + count_y - offset, count_y) * CORES + my_core
        return mixed_all.at[:, pl.ds(pl.multiple_of(owner_tp * channels, 128), channels)]

    mixed_y = {}
    for k in range(1, count_y):
        mixed_y[k] = send(
            mixed_window(0), mixed_window(0), my_s.at[k], my_r.at[k],
            tp=lax.rem(my_y + k, count_y) * CORES + my_core,
        )
    mixed_sib = [send(mixed_window(0), mixed_window(0), ms_s.at[0], ms_r.at[0], tp=sibling)]

    for g in range(early + 2, groups_y):
        forward_again(g)
    rows_ready(early, groups_y)
    normalize_rows(1)
    hidden_units(1, lambda n: None)
    others = list(range(1, count_y))
    loads[16].wait()
    give_back(1, others)
    give_back(0, others)
    give_back(1, [0])
    sib_copies[1, 0].wait_recv()
    finish(groups_half)
    give_back(0, [0])
    for g in range(groups_half + 1, groups_half + 2):
        finish(g)
    for k in range(1, count_y):
        mixed_y[k].wait_recv()
        mixed_sib.append(
            send(mixed_window(k), mixed_window(k), ms_s.at[k], ms_r.at[k], tp=sibling)
        )
    for g in range(groups_half + 2, groups_y):
        finish(g)
    loads[8].wait()
    loads[9].wait()
    for copy in mixed_sib:
        copy.wait_recv()
    out_a_cols = min(256, out_a.shape[1])
    for n in range(out_a.shape[1] // out_a_cols):
        cols = slice(n * out_a_cols, (n + 1) * out_a_cols)
        value = nn(mixed_all[...], w_value[:, cols])
        gate = nn(mixed_all[...], w_gate_out[:, cols])
        out_a[:, cols] = (value * jax.nn.sigmoid(gate)).astype(bf16)
    sib_copies[0, 0].wait_recv()
    for g in range(groups_half):
        finish(g)
    for k in range(1, count_ep):
        back_copies[k].wait_recv()
    out_b[...] = (tn(share_hi[...], returned[...]) + tn(share_lo[...], returned[...])).astype(bf16)
    for copy in pending:
        copy.wait_send()


def fused(args, state_size, capacity):
    count_ep, count_tp = lax.axis_size("ep"), lax.axis_size("tp")
    count_y = count_tp // CORES
    positions, channels = args[0].shape
    groups = args[1].shape[0]
    tokens, feats = args[10].shape
    flat = args[3].shape[0] * args[3].shape[1]
    slots = count_ep * capacity
    hid = args[14].shape[1]
    width = feats * count_tp
    groups_y, halves = min(count_ep, 8), 2
    dma = pltpu.SemaphoreType.DMA
    vmem = pltpu.VMEM
    scratch = [vmem(x.shape, x.dtype) for x in args] + [
        vmem((8, positions), f32),
        vmem((count_tp, 8, positions), f32),
        vmem((4, flat), f32),
        vmem((tokens, feats), bf16),
        vmem(args[12].shape, args[12].dtype),
        vmem((1, width), f32),
        vmem((slots, width), bf16),
        vmem((slots, feats), bf16),
        vmem((slots, width), bf16),
        vmem((slots, tokens), bf16),
        vmem((slots, tokens), bf16),
        vmem((positions, flat), f32),
        vmem((positions, flat), f32),
        vmem((positions, flat), f32),
        vmem((positions, flat), f32),
        vmem((4, CHUNKS, flat), f32),
        vmem((2, CHUNKS, flat), f32),
        vmem((4, flat), f32),
        vmem((count_ep, 4, flat), f32),
        vmem((positions, flat), bf16),
        vmem((positions, flat), bf16),
        vmem((positions, channels), bf16),
        vmem((positions, channels * count_tp), bf16),
        vmem((slots, hid), bf16),
        vmem((slots, feats), f32),
        vmem((count_y, slots, feats), bf16),
        vmem((count_y, slots, feats), bf16),
        vmem((count_y, slots, feats), bf16),
        vmem((count_y, slots, feats), bf16),
        vmem((slots, feats), bf16),
        vmem((slots, feats), bf16),
        dma((len(args),)),
        dma((2,)), dma((2,)),
        dma((count_tp,)), dma((count_tp,)),
        dma((count_tp,)), dma((count_tp,)),
        dma((count_ep,)), dma((count_ep,)),
        dma((count_y, groups_y)), dma((count_y, groups_y)),
        dma((count_y, groups_y)), dma((count_y, groups_y)),
        dma((count_ep,)), dma((count_ep,)),
        dma((count_y,)), dma((count_y,)),
        dma((count_y,)), dma((count_y,)),
        dma((count_y, halves)), dma((count_y, halves)),
        dma((count_y, groups_y)), dma((count_y, groups_y)),
        dma((count_ep,)), dma((count_ep,)),
    ]
    return pl.pallas_call(
        functools.partial(kernel, (count_ep, count_tp, groups_y, halves, state_size)),
        out_shape=[
            vmem((positions, args[8].shape[1]), bf16),
            vmem((tokens, feats), bf16),
        ],
        in_specs=[pl.BlockSpec(memory_space=pltpu.HBM)] * len(args),
        out_specs=[pl.BlockSpec(memory_space=pltpu.VMEM)] * 2,
        scratch_shapes=scratch,
        compiler_params=pltpu.CompilerParams(
            collective_id=0, has_side_effects=True, vmem_limit_bytes=60 * 1024 * 1024
        ),
    )(*args)


def shards(
    mixer_input, mixer_gain, time_step, pole_real, pole_imag, input_real, input_imag,
    read_real, read_imag, out_value, out_gate, expert_input, expert_gain, routes,
    route_weight, expert_gate, expert_up, expert_down,
):
    tokens, top = routes.shape
    capacity = 2 * top * tokens // lax.axis_size("ep")
    def by_channel(table):
        return jnp.swapaxes(table, 1, 2).reshape(-1, table.shape[1])

    args = (
        mixer_input, time_step.T, mixer_gain[None, :], pole_real,
        by_channel(input_real), by_channel(input_imag),
        read_real.reshape(-1, read_real.shape[2]), read_imag.reshape(-1, read_imag.shape[2]),
        out_value, out_gate, expert_input, expert_gain[None, :], routes.T, route_weight.T,
        expert_gate[0], expert_up[0], expert_down[0], pole_imag,
    )
    return tuple(fused(args, pole_real.shape[1], capacity))


def solution(mesh):
    return jax.shard_map(
        shards,
        mesh=mesh,
        in_specs=(
            P("ep", "tp"), P("tp"), P("ep", "tp"), P("tp", None), P("tp", None),
            P("tp", None, None), P("tp", None, None), P("tp", None, None), P("tp", None, None),
            P(None, "tp"), P(None, "tp"), P("ep", "tp"), P("tp"), P("ep", None), P("ep", None),
            P("ep", None, "tp"), P("ep", None, "tp"), P("ep", "tp", None),
        ),
        out_specs=(P("ep", "tp"), P("ep", "tp")),
        check_vma=False,
    )
```

```python
import functools
import jax
import jax.numpy as jnp
from jax import lax
from jax.experimental import pallas as pl
from jax.experimental.pallas import tpu as pltpu
from jax.sharding import PartitionSpec as P

norm_eps = 1e-05
CHUNKS = 8
CORES = 2
f32 = jnp.float32
bf16 = jnp.bfloat16


def sin_cos(angle):
    turns = jnp.round(angle * 0.6366197723675814)
    left = angle - turns * 1.5703125
    left = left - turns * 4.83751296997e-4
    left = left - turns * 7.549789948768648e-8
    sq = left * left
    sine = ((-1.9515295891e-4 * sq + 8.3321608736e-3) * sq - 1.6666654611e-1) * sq * left + left
    cosine = (
        ((2.443315711809948e-5 * sq - 1.388731625493765e-3) * sq + 4.166664568298827e-2) * sq * sq
        - 0.5 * sq
        + 1.0
    )
    quadrant = turns.astype(jnp.int32)
    odd = (quadrant & 1) == 1
    sin_out = jnp.where(odd, cosine, sine)
    cos_out = jnp.where(odd, sine, cosine)
    sin_out = jnp.where((quadrant & 2) == 2, -sin_out, sin_out)
    cos_out = jnp.where(((quadrant + 1) & 2) == 2, -cos_out, cos_out)
    return sin_out, cos_out


def iota(shape, dim):
    return lax.broadcasted_iota(jnp.int32, shape, dim)


def nn(left, right):
    return jnp.dot(left, right, preferred_element_type=f32)


def nt(left, right):
    return lax.dot_general(left, right, (((1,), (1,)), ((), ())), preferred_element_type=f32)


def tn(left, right):
    return lax.dot_general(left, right, (((0,), (0,)), ((), ())), preferred_element_type=f32)


def partner(me, k):
    other, bit = me, 1
    while bit <= k:
        if k & bit:
            other = other + bit * (1 - 2 * ((me // bit) % 2))
        bit *= 2
    return other


def spread(table, row_div, lanes, lane_div):
    rows, width = table.shape
    pick = (iota((width, lanes), 0) == iota((width, lanes), 1) % width).astype(bf16)
    wide = nn(table.astype(bf16), pick)
    same = iota((rows, lanes), 0) // row_div == iota((rows, lanes), 1) // lane_div
    return jnp.where(same, wide, 0.0).astype(bf16)


def row_sums(rows):
    ones = jnp.ones((16, rows.shape[1]), bf16)
    wide = rows.astype(f32)
    square = wide * wide
    high = square.astype(bf16)
    low = (square - high.astype(f32)).astype(bf16)
    sums = nt(ones, rows)
    squares = nt(ones, high) + nt(ones, low)
    return jnp.where(iota((8, 1), 0) == 0, sums[:8], squares[:8])


def normalize(rows, stats, gain, width):
    average = stats[:, 0:1] / width
    variance = stats[:, 1:2] / width - average * average
    return (rows.astype(f32) - average) * lax.rsqrt(variance + norm_eps) * gain


def kernel(dims, *refs):
    count_ep, count_tp, groups_y, pieces, state_size = dims
    hbm, refs = refs[:18], refs[18:]
    (out_a, out_b), refs = refs[:2], refs[2:]
    vm, refs = refs[:18], refs[18:]
    (
        mine_stats, slot_stats, pole, tokens_far, routes_far, gain_all, rows_n, outgoing, rows_x, share_hi, share_lo, a_re, a_im, u_re, u_im,
        sums, enter, mine_state, slot_state, n_re, n_im, mixed, mixed_all, hidden, own,
        sib_send, sib_recv, y_send, y_recv, final, returned,
        sem_in, far_s, far_r, gn_s, gn_r, st_s, st_r, aa_s, aa_r, dy_s, dy_r, ds_s, ds_r, hs_s, hs_r,
        my_s, my_r, ms_s, ms_r, rs_s, rs_r, ry_s, ry_r, ra_s, ra_r,
    ) = refs
    (
        a_in, step_in, gain_a, real_in, in_re, in_im, rd_re, rd_im, w_value, w_gate_out,
        b_in, gain_b, routes_in, weight_in, w_gate, w_up, w_down, imag_in,
    ) = vm

    me = lax.axis_index("ep")
    tp = lax.axis_index("tp")
    count_y = count_tp // CORES
    my_y = tp // CORES
    my_core = tp % CORES
    sibling = my_y * CORES + 1 - my_core

    barrier = pltpu.get_barrier_semaphore()
    for k in range(1, count_ep):
        pl.semaphore_signal(
            barrier, inc=1, device_id={"ep": partner(me, k)}, device_id_type=pl.DeviceIdType.MESH
        )
    for k in range(1, count_tp):
        pl.semaphore_signal(
            barrier, inc=1, device_id={"tp": lax.rem(tp + k, count_tp)},
            device_id_type=pl.DeviceIdType.MESH,
        )

    loads = [
        pltpu.make_async_copy(source, target, sem_in.at[i])
        for i, (source, target) in enumerate(zip(hbm, vm))
    ]
    for i in (10, 12, 11, 0, 1, 3, 17, 2, 13, 4, 5, 6, 7, 14, 15, 16, 8, 9):
        loads[i].start()

    pending = []

    def send(source, target, send_sem, recv_sem, **where):
        copy = pltpu.make_async_remote_copy(
            src_ref=source, dst_ref=target, send_sem=send_sem, recv_sem=recv_sem,
            device_id=where, device_id_type=pl.DeviceIdType.MESH,
        )
        copy.start()
        pending.append(copy)
        return copy

    positions, channels = a_in.shape
    tokens, feats = b_in.shape
    width = feats * count_tp
    flat = a_re.shape[1]
    states = state_size
    group_ch = in_re.shape[0] * states // flat
    slots = rows_x.shape[0]
    cap = slots // count_ep
    tile = min(256, flat)
    tiles = flat // tile
    tile_ch = tile // states * group_ch
    steps = positions // CHUNKS
    hid = w_gate.shape[1]
    expert_rows = max(16, count_ep)
    my_cols = pl.ds(pl.multiple_of(tp * feats, 128), feats)

    portal = partner(me, count_ep // 2)
    for i in (12, 11, 10):
        loads[i].wait()
    pl.semaphore_wait(barrier, count_ep + count_tp - 2)
    far_routes = send(routes_in, routes_far, far_s.at[0], far_r.at[0], ep=portal)
    cuts = 2 if feats % 256 == 0 else 1
    cut = [slice(c * feats // cuts, (c + 1) * feats // cuts) for c in range(cuts)]
    far_tokens = [
        send(
            b_in.at[:, cut[c]], tokens_far.at[:, cut[c]], far_s.at[1 + c], far_r.at[1 + c],
            ep=portal,
        )
        for c in range(cuts)
    ]
    gain_copies = [
        send(
            gain_b, gain_all.at[:, my_cols], gn_s.at[k], gn_r.at[k], tp=lax.rem(tp + k, count_tp)
        )
        for k in range(1, count_tp)
    ]
    gain_all[:, my_cols] = gain_b[...]
    near = count_ep // 2
    expert_of = iota((expert_rows, tokens), 0)
    before = (iota((tokens, tokens), 0) < iota((tokens, tokens), 1)).astype(bf16)

    def places(routes):
        hit = jnp.zeros((expert_rows, tokens), jnp.bool_)
        for k in range(routes.shape[0]):
            hit = jnp.logical_or(hit, routes[k : k + 1, :] == expert_of)
        place = nn(hit.astype(f32).astype(bf16), before)
        return jnp.where(hit, place, -1.0).astype(bf16)

    def owners(low, high):
        return jnp.concatenate(
            [
                (iota((cap, expert_rows), 1) == partner(me, k)).astype(f32)
                for k in range(low, high)
            ],
            axis=0,
        ).astype(bf16)

    def select(owner, place):
        return nn(owner, place) == (iota((owner.shape[0], tokens), 0) % cap).astype(f32)

    place_own = places(routes_in[...])
    owner_near = owners(0, near)
    chosen_near = select(owner_near, place_own)
    chosen = chosen_near.astype(f32).astype(bf16)

    arrivals = {}

    def hand_out(base, columns, values, c):
        outgoing[base * cap : (base + near) * cap, columns] = values
        size = columns.stop - columns.start
        there = pl.ds(pl.multiple_of(tp * feats + columns.start, 128), size)
        for k in range(1, near):
            here = pl.ds((base + k) * cap, cap)
            arrivals.setdefault(base + k, []).append(
                send(
                    outgoing.at[here, columns], rows_x.at[here, there], aa_s.at[c, base + k],
                    aa_r.at[c, base + k], ep=partner(me, k),
                )
            )
        rows_x[base * cap : (base + 1) * cap, there] = values[0:cap]

    per_group = count_ep // groups_y
    group_rows = per_group * cap
    y_arrivals, sib_arrivals = {}, []

    def core_cols(offset):
        owner_tp = lax.rem(my_y + count_y - offset, count_y) * CORES + my_core
        return pl.ds(pl.multiple_of(owner_tp * feats, 128), feats)

    def to_sibling(offset, g):
        here = rows_x.at[pl.ds(g * group_rows, group_rows), core_cols(offset)]
        sib_arrivals.append((g, send(here, here, ds_s.at[offset, g], ds_r.at[offset, g], tp=sibling)))

    def forward(g):
        for k in range(g * per_group, (g + 1) * per_group):
            for copy in arrivals.get(k, []):
                copy.wait_recv()
        here = rows_x.at[pl.ds(g * group_rows, group_rows), my_cols]
        for k in range(1, count_y):
            y_arrivals[k, g] = send(
                here, here, dy_s.at[k, g], dy_r.at[k, g],
                tp=lax.rem(my_y + k, count_y) * CORES + my_core,
            )
        to_sibling(0, g)

    def forward_again(g):
        for k in range(1, count_y):
            y_arrivals[k, g].wait_recv()
            to_sibling(k, g)

    hand_out(0, slice(0, feats), nn(chosen, b_in[...]).astype(bf16), 0)
    forward(0)
    loads[0].wait()
    mine_stats[...] = row_sums(a_in[...])
    stat_copies = [
        send(mine_stats, slot_stats.at[k], st_s.at[k], st_r.at[k], tp=lax.rem(tp + k, count_tp))
        for k in range(1, count_tp)
    ]

    loads[1].wait()
    order = (
        iota((positions, positions), 1)
        == (iota((positions, positions), 0) % CHUNKS) * steps
        + iota((positions, positions), 0) // CHUNKS
    ).astype(f32).astype(bf16)
    order_t = (
        iota((positions, positions), 0)
        == (iota((positions, positions), 1) % CHUNKS) * steps
        + iota((positions, positions), 1) // CHUNKS
    ).astype(f32).astype(bf16)
    step = step_in[...]
    groups = step.shape[0]
    high = step.astype(bf16).astype(f32)
    middle = (step - high).astype(bf16).astype(f32)
    low = step - high - middle
    parts = [high, middle, low]
    padded = -(-3 * groups // 16) * 16
    if padded > 3 * groups:
        parts.append(jnp.zeros((padded - 3 * groups, positions), f32))
    split = jnp.concatenate(parts, axis=0).astype(bf16)
    split = nn(split, order_t).astype(bf16)
    for t in range(tiles):
        lanes = slice(t * tile, (t + 1) * tile)
        source = iota((padded, tile), 0)
        pick = jnp.logical_and(
            source % groups == iota((padded, tile), 1) // states + t * (tile // states),
            source < 3 * groups,
        )
        a_re[:, lanes] = tn(split, pick.astype(f32).astype(bf16))

    loads[3].wait()
    loads[17].wait()
    pick = (iota((states, flat), 0) == iota((states, flat), 1) % states).astype(f32).astype(bf16)
    own_lane = iota((groups, flat), 0) == iota((groups, flat), 1) // states

    def to_lanes(table):
        high = table.astype(bf16)
        rest = table - high.astype(f32)
        middle = rest.astype(bf16)
        low = (rest - middle.astype(f32)).astype(bf16)
        wide = nn(high, pick) + (nn(middle, pick) + nn(low, pick))
        return jnp.sum(jnp.where(own_lane, wide, 0.0), axis=0, keepdims=True)

    real, imag = to_lanes(real_in[...]), to_lanes(imag_in[...])
    denom = real * real + imag * imag
    pole[0:1, :] = real
    pole[1:2, :] = imag
    pole[2:3, :] = real / denom
    pole[3:4, :] = imag / denom
    block = min(32, positions)

    def steps_of(t):
        lanes = slice(t * tile, (t + 1) * tile)
        p_re, p_im = pole[0:1, lanes], pole[1:2, lanes]
        d_re, d_im = pole[2:3, lanes], pole[3:4, lanes]

        def elementwise(i, passed):
            here = pl.ds(pl.multiple_of(i * block, block), block)
            delta = a_re[here, lanes]
            for j in range(block // CHUNKS):
                passed = passed + delta[j * CHUNKS : (j + 1) * CHUNKS]
            magnitude = jnp.exp(p_re * delta)
            sine, cosine = sin_cos(p_im * delta)
            ab_re = magnitude * cosine
            ab_im = magnitude * sine
            numer = ab_re - 1.0
            a_re[here, lanes] = ab_re
            a_im[here, lanes] = ab_im
            u_re[here, lanes] = numer * d_re + ab_im * d_im
            u_im[here, lanes] = ab_im * d_re - numer * d_im
            return passed

        passed = lax.fori_loop(
            0, positions // block, elementwise, jnp.zeros((CHUNKS, tile), f32)
        )
        magnitude = jnp.exp(p_re * passed)
        sine, cosine = sin_cos(p_im * passed)
        sums[0, :, lanes] = magnitude * cosine
        sums[1, :, lanes] = magnitude * sine

    for t in range(tiles):
        steps_of(t)
    forward(1)
    forward_again(0)
    far_routes.wait_recv()
    chosen_far = select(owner_near, places(routes_far[...])).astype(f32).astype(bf16)

    def hand_out_far(c):
        far_tokens[c].wait_recv()
        hand_out(near, cut[c], nn(chosen_far, tokens_far[:, cut[c]]).astype(bf16), c)

    for c in range(cuts - 1):
        hand_out_far(c)
    for copy in stat_copies:
        copy.wait_recv()
    total = mine_stats[...]
    for k in range(1, count_tp):
        total = total + slot_stats[k]
    total = total.T

    loads[2].wait()
    normed = normalize(a_in[...], total, gain_a[...], width).astype(bf16)
    normed = nn(order, normed).astype(bf16)
    for i in (4, 5, 6, 7):
        loads[i].wait()

    def first_half(t):
        lanes = slice(t * tile, (t + 1) * tile)
        table = slice(t * tile_ch, (t + 1) * tile_ch)
        piece = normed[:, table]
        v_re = nn(piece, spread(in_re[table, :], group_ch, tile, states))
        v_im = nn(piece, spread(in_im[table, :], group_ch, tile, states))
        k_re, k_im = u_re[:, lanes], u_im[:, lanes]
        u_re[:, lanes] = k_re * v_re - k_im * v_im
        u_im[:, lanes] = k_re * v_im + k_im * v_re

    span = min(1024, flat)

    def chunk_sums(base):
        lanes = slice(base, base + span)

        def one(s, carried):
            s_re, s_im = carried
            here = pl.ds(pl.multiple_of(s * CHUNKS, CHUNKS), CHUNKS)
            b_re, b_im = a_re[here, lanes], a_im[here, lanes]
            return (
                b_re * s_re - b_im * s_im + u_re[here, lanes],
                b_re * s_im + b_im * s_re + u_im[here, lanes],
            )

        zero = jnp.zeros((CHUNKS, span), f32)
        sums[2, :, lanes], sums[3, :, lanes] = lax.fori_loop(0, steps, one, (zero, zero), unroll=2)

    early = groups_y // 2
    for t in range(tiles):
        first_half(t)
    for base in range(0, flat, span):
        chunk_sums(base)
    def chunk(index, c):
        return sums[index, c : c + 1, :]

    c_re, c_im, s_re, s_im = (chunk(index, 0) for index in range(4))
    for c in range(1, CHUNKS):
        b_re, b_im = chunk(0, c), chunk(1, c)
        c_re, c_im = b_re * c_re - b_im * c_im, b_re * c_im + b_im * c_re
        s_re, s_im = (
            b_re * s_re - b_im * s_im + chunk(2, c),
            b_re * s_im + b_im * s_re + chunk(3, c),
        )
    mine_state[0:1, :] = c_re
    mine_state[1:2, :] = c_im
    mine_state[2:3, :] = s_re
    mine_state[3:4, :] = s_im
    state_copies = []
    for k in range(1, count_ep):
        other = partner(me, k)
        copy = pltpu.make_async_remote_copy(
            src_ref=mine_state, dst_ref=slot_state.at[me], send_sem=hs_s.at[k], recv_sem=hs_r.at[k],
            device_id={"ep": other}, device_id_type=pl.DeviceIdType.MESH,
        )
        state_copies.append((other, copy))

        @pl.when(other > me)
        def _(copy=copy):
            copy.start()

    hand_out_far(cuts - 1)
    forward(early)
    for g in range(2, early - 1):
        forward(g)
    forward_again(1)
    loads[13].wait()
    weight = jnp.zeros((expert_rows, tokens), f32)
    for k in range(routes_in.shape[0]):
        this = routes_in[k : k + 1, :] == expert_of
        weight = jnp.where(this, weight_in[k : k + 1, :], weight)
    weight_hi = weight.astype(bf16)
    weight_lo = (weight - weight_hi.astype(f32)).astype(bf16)
    owner_far = owners(near, count_ep)
    for rows, owner, here in (
        (slice(0, near * cap), owner_near, chosen_near),
        (slice(near * cap, slots), owner_far, select(owner_far, place_own)),
    ):
        share_hi[rows, :] = jnp.where(here, nn(owner, weight_hi), 0.0).astype(bf16)
        share_lo[rows, :] = jnp.where(here, nn(owner, weight_lo), 0.0).astype(bf16)

    columns = min(256, hid)
    out_columns = min(256, feats)
    middle = early + (groups_y - early) // 2
    split = early // 2
    blocks = ((0, split), (early, middle), (middle, groups_y), (split, early))

    def rows_of(b):
        return slice(blocks[b][0] * group_rows, blocks[b][1] * group_rows)


    def normalize_rows(b):
        step_rows = min(64, group_rows)
        for r in range(rows_of(b).start, rows_of(b).stop, step_rows):
            rows = slice(r, r + step_rows)
            wide = rows_x[rows, :].astype(f32)
            average = jnp.sum(wide, axis=1, keepdims=True) / width
            square = jnp.sum(wide * wide, axis=1, keepdims=True) / width
            variance = square - average * average
            wide = (wide - average) * lax.rsqrt(variance + norm_eps) * gain_all[...]
            rows_n[rows, :] = wide.astype(bf16)

    def hidden_units(b, between):
        top = rows_of(b)
        for n in range(hid // columns):
            cols = slice(n * columns, (n + 1) * columns)
            gate = nn(rows_n[top, :], w_gate[:, cols])
            up = nn(rows_n[top, :], w_up[:, cols])
            hidden[top, cols] = (gate * jax.nn.sigmoid(gate) * up).astype(bf16)
            between(n)

    sib_copies, y_copies = {}, {}

    def down(b, target_tp, store):
        top = rows_of(b)
        for n in range(feats // out_columns):
            first = pl.multiple_of(target_tp * feats + n * out_columns, 128)
            store(
                top, slice(n * out_columns, (n + 1) * out_columns),
                nn(hidden[top, :], w_down[:, pl.ds(first, out_columns)]),
            )

    def give_back(b, offsets):
        for offset in offsets:
            yt = lax.rem(my_y + offset, count_y) * CORES

            def to_send(rows, cols, value, offset=offset):
                sib_send[offset, rows, cols] = value.astype(bf16)

            def to_own(rows, cols, value, offset=offset):
                own[offset, rows, cols] = value

            down(b, yt + 1 - my_core, to_send)
            window = pl.ds(rows_of(b).start, rows_of(b).stop - rows_of(b).start)
            sib_copies[b, offset] = send(
                sib_send.at[offset, window], sib_recv.at[offset, window],
                rs_s.at[offset, b], rs_r.at[offset, b], tp=sibling,
            )
            down(b, yt + my_core, to_own)

    def sum_y(b):
        for offset in range(1, count_y):
            sib_copies[b, offset].wait_recv()
            rows = rows_of(b)
            y_send[offset, rows, :] = (
                own[offset, rows, :] + sib_recv[offset, rows, :].astype(f32)
            ).astype(bf16)

    def send_y(g):
        for offset in range(1, count_y):
            window = pl.ds(g * group_rows, group_rows)
            y_copies[offset, g] = send(
                y_send.at[offset, window], y_recv.at[offset, window],
                ry_s.at[offset, g], ry_r.at[offset, g],
                tp=lax.rem(my_y + offset, count_y) * CORES + my_core,
            )

    back_copies = {}

    def finish(g):
        window = slice(g * group_rows, (g + 1) * group_rows)
        total = own[0, window, :] + sib_recv[0, window, :].astype(f32)
        for offset in range(1, count_y):
            y_copies[offset, g].wait_recv()
            total = total + y_recv[offset, window, :].astype(f32)
        total = total.astype(bf16)
        final[window, :] = total
        if g == 0:
            returned[0:cap, :] = total[0:cap]
        for k in range(max(1, g * per_group), (g + 1) * per_group):
            here = pl.ds(k * cap, cap)
            back_copies[k] = send(
                final.at[here], returned.at[here], ra_s.at[k], ra_r.at[k], ep=partner(me, k)
            )

    def rows_ready(low, high):
        for g, copy in list(sib_arrivals):
            if low <= g < high:
                copy.wait_recv()

    others = list(range(1, count_y))
    chunks = hid // columns

    def spread_out(tasks):
        def between(n):
            for task in tasks[n * len(tasks) // chunks : (n + 1) * len(tasks) // chunks]:
                task()

        return between

    def tasks_of(function, items):
        return [functools.partial(function, item) for item in items]

    rows_ready(*blocks[0])
    for copy in gain_copies:
        copy.wait_recv()
    normalize_rows(0)
    loads[14].wait()
    loads[15].wait()
    first = [early + 1, *range(early + 2, groups_y)]
    after = [[] for n in range(chunks)]
    after[max(0, chunks // 2 - 1)] += tasks_of(forward, first[:1])
    after[max(0, chunks // 2 - 1)] += tasks_of(forward_again, [early])
    after[-1] += tasks_of(forward, first[1:2])

    def between(n):
        for task in after[n]:
            task()

    hidden_units(0, between)
    loads[16].wait()
    give_back(0, others)
    for g in first[2:]:
        forward(g)
    for g in range(max(2, early - 1), early):
        forward(g)
    for g in range(2, early - 1):
        forward_again(g)
    give_back(0, [0])
    forward_again(early + 1)
    for other, copy in state_copies:

        @pl.when(other < me)
        def _(copy=copy):
            copy.wait_recv()


    def fold(q, carried):
        h_re, h_im = carried
        b_re, b_im = slot_state[q, 0:1, :], slot_state[q, 1:2, :]
        return (
            b_re * h_re - b_im * h_im + slot_state[q, 2:3, :],
            b_re * h_im + b_im * h_re + slot_state[q, 3:4, :],
        )

    blank = jnp.zeros((1, flat), f32)
    h_re, h_im = lax.fori_loop(0, me, fold, (blank, blank))
    for c in range(CHUNKS):
        enter[0, c : c + 1, :] = h_re
        enter[1, c : c + 1, :] = h_im
        b_re, b_im = chunk(0, c), chunk(1, c)
        h_re, h_im = (
            b_re * h_re - b_im * h_im + chunk(2, c),
            b_re * h_im + b_im * h_re + chunk(3, c),
        )
    for base in range(0, flat, span):
        lanes = slice(base, base + span)

        def advance(s, carried, lanes=lanes):
            s_re, s_im = carried
            found_re, found_im = [], []
            for j in range(2):
                here = pl.ds(pl.multiple_of(s * 2 * CHUNKS + j * CHUNKS, CHUNKS), CHUNKS)
                b_re, b_im = a_re[here, lanes], a_im[here, lanes]
                s_re, s_im = (
                    b_re * s_re - b_im * s_im + u_re[here, lanes],
                    b_re * s_im + b_im * s_re + u_im[here, lanes],
                )
                found_re.append(s_re)
                found_im.append(s_im)
            both = pl.ds(pl.multiple_of(s * 2 * CHUNKS, 2 * CHUNKS), 2 * CHUNKS)
            n_re[both, lanes] = jnp.concatenate(found_re, axis=0).astype(bf16)
            n_im[both, lanes] = jnp.concatenate(found_im, axis=0).astype(bf16)
            return s_re, s_im

        lax.fori_loop(0, steps // 2, advance, (enter[0, :, lanes], enter[1, :, lanes]))
    for t in range(tiles):
        lanes = slice(t * tile, (t + 1) * tile)
        table = slice(t * tile_ch, (t + 1) * tile_ch)
        response = nt(n_re[:, lanes], spread(rd_re[table, :], group_ch, tile, states)) - nt(
            n_im[:, lanes], spread(rd_im[table, :], group_ch, tile, states)
        )
        mixed[:, table] = jax.nn.gelu(response).astype(bf16)
    mixed_cols = pl.ds(pl.multiple_of(tp * channels, 128), channels)
    mixed_all[:, mixed_cols] = nn(order_t, mixed[...]).astype(bf16)

    piece_rows = positions // pieces

    def mixed_window(offset, p):
        owner_tp = lax.rem(my_y + count_y - offset, count_y) * CORES + my_core
        return mixed_all.at[
            pl.ds(p * piece_rows, piece_rows),
            pl.ds(pl.multiple_of(owner_tp * channels, 128), channels),
        ]

    mixed_y, mixed_sib = {}, []

    def mixed_to_sibling(offset, p):
        here = mixed_window(offset, p)
        mixed_sib.append(
            (p, send(here, here, ms_s.at[offset, p], ms_r.at[offset, p], tp=sibling))
        )

    def send_mixed(p):
        here = mixed_window(0, p)
        for k in range(1, count_y):
            mixed_y[k, p] = send(
                here, here, my_s.at[k, p], my_r.at[k, p],
                tp=lax.rem(my_y + k, count_y) * CORES + my_core,
            )
        mixed_to_sibling(0, p)

    def forward_mixed(p):
        for k in range(1, count_y):
            mixed_y[k, p].wait_recv()
            mixed_to_sibling(k, p)

    send_mixed(0)
    rows_ready(*blocks[1])
    normalize_rows(1)
    hidden_units(1, spread_out(tasks_of(forward_again, range(early + 2, groups_y))))
    give_back(1, others + [0])
    sum_y(1)
    for g in reversed(range(*blocks[1])):
        send_y(g)
    for g in range(max(2, early - 1), early):
        forward_again(g)
    rows_ready(*blocks[2])
    normalize_rows(2)
    hidden_units(2, lambda n: None)
    give_back(2, others + [0])
    sum_y(2)
    for g in reversed(range(*blocks[2])):
        send_y(g)
    for p in range(1, pieces):
        send_mixed(p)
    forward_mixed(0)
    rows_ready(*blocks[3])
    sib_copies[1, 0].wait_recv()
    sib_copies[2, 0].wait_recv()
    for g in reversed(range(*blocks[1])):
        finish(g)
    normalize_rows(3)
    hidden_units(3, lambda n: None)
    give_back(3, others + [0])
    sum_y(3)
    for g in reversed(range(*blocks[3])):
        send_y(g)
    sum_y(0)
    for g in reversed(range(*blocks[0])):
        send_y(g)
    for g in reversed(range(*blocks[2])):
        finish(g)
    loads[8].wait()
    loads[9].wait()

    def project(p):
        for copy in [copy for q, copy in mixed_sib if q == p]:
            copy.wait_recv()
        rows = slice(p * piece_rows, (p + 1) * piece_rows)
        out_a_cols = min(256, out_a.shape[1])
        for n in range(out_a.shape[1] // out_a_cols):
            cols = slice(n * out_a_cols, (n + 1) * out_a_cols)
            value = nn(mixed_all[rows, :], w_value[:, cols])
            gate = nn(mixed_all[rows, :], w_gate_out[:, cols])
            out_a[rows, cols] = (value * jax.nn.sigmoid(gate)).astype(bf16)

    project(0)
    for p in range(1, pieces):
        forward_mixed(p)
    sib_copies[0, 0].wait_recv()
    sib_copies[3, 0].wait_recv()
    for g in reversed(range(*blocks[3])):
        finish(g)
    for p in range(1, pieces):
        project(p)
    for g in reversed(range(*blocks[0])):
        finish(g)
    for k in range(1, count_ep):
        back_copies[k].wait_recv()
    out_b[...] = (tn(share_hi[...], returned[...]) + tn(share_lo[...], returned[...])).astype(bf16)
    for other, copy in state_copies:

        @pl.when(other > me)
        def _(copy=copy):
            copy.wait_send()

    for copy in pending:
        copy.wait_send()


def fused(args, state_size, capacity):
    count_ep, count_tp = lax.axis_size("ep"), lax.axis_size("tp")
    count_y = count_tp // CORES
    positions, channels = args[0].shape
    groups = args[1].shape[0]
    tokens, feats = args[10].shape
    flat = args[3].shape[0] * args[3].shape[1]
    slots = count_ep * capacity
    hid = args[14].shape[1]
    width = feats * count_tp
    groups_y, pieces = min(count_ep, 8), 2
    dma = pltpu.SemaphoreType.DMA
    vmem = pltpu.VMEM
    scratch = [vmem(x.shape, x.dtype) for x in args] + [
        vmem((8, positions), f32),
        vmem((count_tp, 8, positions), f32),
        vmem((4, flat), f32),
        vmem((tokens, feats), bf16),
        vmem(args[12].shape, args[12].dtype),
        vmem((1, width), f32),
        vmem((slots, width), bf16),
        vmem((slots, feats), bf16),
        vmem((slots, width), bf16),
        vmem((slots, tokens), bf16),
        vmem((slots, tokens), bf16),
        vmem((positions, flat), f32),
        vmem((positions, flat), f32),
        vmem((positions, flat), f32),
        vmem((positions, flat), f32),
        vmem((4, CHUNKS, flat), f32),
        vmem((2, CHUNKS, flat), f32),
        vmem((4, flat), f32),
        vmem((count_ep, 4, flat), f32),
        vmem((positions, flat), bf16),
        vmem((positions, flat), bf16),
        vmem((positions, channels), bf16),
        vmem((positions, channels * count_tp), bf16),
        vmem((slots, hid), bf16),
        vmem((count_y, slots, feats), f32),
        vmem((count_y, slots, feats), bf16),
        vmem((count_y, slots, feats), bf16),
        vmem((count_y, slots, feats), bf16),
        vmem((count_y, slots, feats), bf16),
        vmem((slots, feats), bf16),
        vmem((slots, feats), bf16),
        dma((len(args),)),
        dma((3,)), dma((3,)),
        dma((count_tp,)), dma((count_tp,)),
        dma((count_tp,)), dma((count_tp,)),
        dma((2, count_ep)), dma((2, count_ep)),
        dma((count_y, groups_y)), dma((count_y, groups_y)),
        dma((count_y, groups_y)), dma((count_y, groups_y)),
        dma((count_ep,)), dma((count_ep,)),
        dma((count_y, pieces)), dma((count_y, pieces)),
        dma((count_y, pieces)), dma((count_y, pieces)),
        dma((count_y, 4)), dma((count_y, 4)),
        dma((count_y, groups_y)), dma((count_y, groups_y)),
        dma((count_ep,)), dma((count_ep,)),
    ]
    return pl.pallas_call(
        functools.partial(kernel, (count_ep, count_tp, groups_y, pieces, state_size)),
        out_shape=[
            vmem((positions, args[8].shape[1]), bf16),
            vmem((tokens, feats), bf16),
        ],
        in_specs=[pl.BlockSpec(memory_space=pltpu.HBM)] * len(args),
        out_specs=[pl.BlockSpec(memory_space=pltpu.VMEM)] * 2,
        scratch_shapes=scratch,
        compiler_params=pltpu.CompilerParams(
            collective_id=0, has_side_effects=True, vmem_limit_bytes=60 * 1024 * 1024
        ),
    )(*args)


def shards(
    mixer_input, mixer_gain, time_step, pole_real, pole_imag, input_real, input_imag,
    read_real, read_imag, out_value, out_gate, expert_input, expert_gain, routes,
    route_weight, expert_gate, expert_up, expert_down,
):
    tokens, top = routes.shape
    capacity = 2 * top * tokens // lax.axis_size("ep")
    def by_channel(table):
        return jnp.swapaxes(table, 1, 2).reshape(-1, table.shape[1])

    args = (
        mixer_input, time_step.T, mixer_gain[None, :], pole_real,
        by_channel(input_real), by_channel(input_imag),
        read_real.reshape(-1, read_real.shape[2]), read_imag.reshape(-1, read_imag.shape[2]),
        out_value, out_gate, expert_input, expert_gain[None, :], routes.T, route_weight.T,
        expert_gate[0], expert_up[0], expert_down[0], pole_imag,
    )
    return tuple(fused(args, pole_real.shape[1], capacity))


def solution(mesh):
    return jax.shard_map(
        shards,
        mesh=mesh,
        in_specs=(
            P("ep", "tp"), P("tp"), P("ep", "tp"), P("tp", None), P("tp", None),
            P("tp", None, None), P("tp", None, None), P("tp", None, None), P("tp", None, None),
            P(None, "tp"), P(None, "tp"), P("ep", "tp"), P("tp"), P("ep", None), P("ep", None),
            P("ep", None, "tp"), P("ep", None, "tp"), P("ep", "tp", None),
        ),
        out_specs=(P("ep", "tp"), P("ep", "tp")),
        check_vma=False,
    )
```

```python
import functools
import jax
import jax.numpy as jnp
from jax import lax
from jax.experimental import pallas as pl
from jax.experimental.pallas import tpu as pltpu
from jax.sharding import PartitionSpec as P

norm_eps = 1e-05
CHUNKS = 8
CORES = 2
f32 = jnp.float32
bf16 = jnp.bfloat16


def sin_cos(angle):
    turns = jnp.round(angle * 0.6366197723675814)
    left = angle - turns * 1.5703125
    left = left - turns * 4.83751296997e-4
    left = left - turns * 7.549789948768648e-8
    sq = left * left
    sine = ((-1.9515295891e-4 * sq + 8.3321608736e-3) * sq - 1.6666654611e-1) * sq * left + left
    cosine = (
        ((2.443315711809948e-5 * sq - 1.388731625493765e-3) * sq + 4.166664568298827e-2) * sq * sq
        - 0.5 * sq
        + 1.0
    )
    quadrant = turns.astype(jnp.int32)
    odd = (quadrant & 1) == 1
    sin_out = jnp.where(odd, cosine, sine)
    cos_out = jnp.where(odd, sine, cosine)
    sin_out = jnp.where((quadrant & 2) == 2, -sin_out, sin_out)
    cos_out = jnp.where(((quadrant + 1) & 2) == 2, -cos_out, cos_out)
    return sin_out, cos_out


def iota(shape, dim):
    return lax.broadcasted_iota(jnp.int32, shape, dim)


def nn(left, right):
    return jnp.dot(left, right, preferred_element_type=f32)


def nt(left, right):
    return lax.dot_general(left, right, (((1,), (1,)), ((), ())), preferred_element_type=f32)


def tn(left, right):
    return lax.dot_general(left, right, (((0,), (0,)), ((), ())), preferred_element_type=f32)


def partner(me, k):
    other, bit = me, 1
    while bit <= k:
        if k & bit:
            other = other + bit * (1 - 2 * ((me // bit) % 2))
        bit *= 2
    return other


def spread(table, row_div, lanes, lane_div):
    rows, width = table.shape
    pick = (iota((width, lanes), 0) == iota((width, lanes), 1) % width).astype(bf16)
    wide = nn(table.astype(bf16), pick)
    same = iota((rows, lanes), 0) // row_div == iota((rows, lanes), 1) // lane_div
    return jnp.where(same, wide, 0.0).astype(bf16)


def row_sums(rows):
    ones = jnp.ones((16, rows.shape[1]), bf16)
    wide = rows.astype(f32)
    square = wide * wide
    high = square.astype(bf16)
    low = (square - high.astype(f32)).astype(bf16)
    sums = nt(ones, rows)
    squares = nt(ones, high) + nt(ones, low)
    return jnp.where(iota((8, 1), 0) == 0, sums[:8], squares[:8])


def normalize(rows, stats, gain, width):
    average = stats[:, 0:1] / width
    variance = stats[:, 1:2] / width - average * average
    return (rows.astype(f32) - average) * lax.rsqrt(variance + norm_eps) * gain


def kernel(dims, *refs):
    count_ep, count_tp, groups_y, pieces, state_size = dims
    hbm, refs = refs[:18], refs[18:]
    (out_a, out_b), refs = refs[:2], refs[2:]
    vm, refs = refs[:18], refs[18:]
    (
        mine_stats, slot_stats, pole, tokens_far, routes_far, gain_all, rows_n, outgoing, rows_x, share_hi, share_lo, a_re, a_im, u_re, u_im,
        sums, enter, mine_state, slot_state, n_re, n_im, mixed, mixed_all, hidden, own,
        sib_send, sib_recv, y_send, y_recv, final, returned,
        sem_in, sem_far, sem_small, sem_send, aa_r, dy_r, ds_r, hs_s, hs_r, my_r, ms_r, rs_r, ry_r,
    ) = refs
    (
        a_in, step_in, gain_a, real_in, in_re, in_im, rd_re, rd_im, w_value, w_gate_out,
        b_in, gain_b, routes_in, weight_in, w_gate, w_up, w_down, imag_in,
    ) = vm

    me = lax.axis_index("ep")
    tp = lax.axis_index("tp")
    count_y = count_tp // CORES
    my_y = tp // CORES
    my_core = tp % CORES
    sibling = my_y * CORES + 1 - my_core

    barrier = pltpu.get_barrier_semaphore()
    for k in range(1, count_ep):
        pl.semaphore_signal(
            barrier, inc=1, device_id={"ep": partner(me, k)}, device_id_type=pl.DeviceIdType.MESH
        )
    for k in range(1, count_tp):
        pl.semaphore_signal(
            barrier, inc=1, device_id={"tp": lax.rem(tp + k, count_tp)},
            device_id_type=pl.DeviceIdType.MESH,
        )

    loads = [
        pltpu.make_async_copy(source, target, sem_in.at[i])
        for i, (source, target) in enumerate(zip(hbm, vm))
    ]
    for i in (10, 12, 11, 0, 1, 3, 17, 2, 13, 4, 5, 6, 7, 14, 15, 16, 8, 9):
        loads[i].start()

    def send(source, target, send_sem, recv_sem, **where):
        copy = pltpu.make_async_remote_copy(
            src_ref=source, dst_ref=target, send_sem=send_sem, recv_sem=recv_sem,
            device_id=where, device_id_type=pl.DeviceIdType.MESH,
        )
        copy.start()
        return copy

    def drain(sem, ref):
        pltpu.make_async_copy(ref, ref, sem).wait()

    positions, channels = a_in.shape
    tokens, feats = b_in.shape
    width = feats * count_tp
    flat = a_re.shape[1]
    states = state_size
    group_ch = in_re.shape[0] * states // flat
    slots = rows_x.shape[0]
    cap = slots // count_ep
    tile = min(256, flat)
    tiles = flat // tile
    tile_ch = tile // states * group_ch
    steps = positions // CHUNKS
    hid = w_gate.shape[1]
    expert_rows = max(16, count_ep)
    my_cols = pl.ds(pl.multiple_of(tp * feats, 128), feats)

    portal = partner(me, count_ep // 2)
    for i in (12, 11, 10):
        loads[i].wait()
    pl.semaphore_wait(barrier, count_ep + count_tp - 2)
    far_routes = send(routes_in, routes_far, sem_far.at[0], sem_far.at[1], ep=portal)
    cuts = 2 if feats % 256 == 0 else 1
    cut = [slice(c * feats // cuts, (c + 1) * feats // cuts) for c in range(cuts)]
    far_tokens = [
        send(
            b_in.at[:, cut[c]], tokens_far.at[:, cut[c]], sem_far.at[2], sem_far.at[3 + c],
            ep=portal,
        )
        for c in range(cuts)
    ]
    gain_copies = [
        send(
            gain_b, gain_all.at[:, my_cols], sem_small.at[0], sem_small.at[1], tp=lax.rem(tp + k, count_tp)
        )
        for k in range(1, count_tp)
    ]
    gain_all[:, my_cols] = gain_b[...]
    near = count_ep // 2
    expert_of = iota((expert_rows, tokens), 0)
    before = (iota((tokens, tokens), 0) < iota((tokens, tokens), 1)).astype(bf16)

    def places(routes):
        hit = jnp.zeros((expert_rows, tokens), jnp.bool_)
        for k in range(routes.shape[0]):
            hit = jnp.logical_or(hit, routes[k : k + 1, :] == expert_of)
        place = nn(hit.astype(f32).astype(bf16), before)
        return jnp.where(hit, place, -1.0).astype(bf16)

    def owners(low, high):
        return jnp.concatenate(
            [
                (iota((cap, expert_rows), 1) == partner(me, k)).astype(f32)
                for k in range(low, high)
            ],
            axis=0,
        ).astype(bf16)

    def select(owner, place):
        return nn(owner, place) == (iota((owner.shape[0], tokens), 0) % cap).astype(f32)

    place_own = places(routes_in[...])
    owner_near = owners(0, near)
    chosen_near = select(owner_near, place_own)
    chosen = chosen_near.astype(f32).astype(bf16)

    arrivals = set()

    def hand_out(base, columns, values, c):
        outgoing[base * cap : (base + near) * cap, columns] = values
        size = columns.stop - columns.start
        there = pl.ds(pl.multiple_of(tp * feats + columns.start, 128), size)
        for k in range(1, near):
            here = pl.ds((base + k) * cap, cap)
            arrivals.add(base + k)
            send(
                outgoing.at[here, columns], rows_x.at[here, there], sem_send.at[0],
                aa_r.at[base + k], ep=partner(me, k),
            )
        rows_x[base * cap : (base + 1) * cap, there] = values[0:cap]

    per_group = count_ep // groups_y
    group_rows = per_group * cap
    y_arrivals = {}
    block_of = [g // (groups_y // 4) if groups_y >= 4 else g for g in range(groups_y)]

    def core_cols(offset):
        owner_tp = lax.rem(my_y + count_y - offset, count_y) * CORES + my_core
        return pl.ds(pl.multiple_of(owner_tp * feats, 128), feats)

    def to_sibling(offset, g):
        here = rows_x.at[pl.ds(g * group_rows, group_rows), core_cols(offset)]
        send(here, here, sem_send.at[1], ds_r.at[block_of[g]], tp=sibling)

    def forward(g):
        for k in range(g * per_group, (g + 1) * per_group):
            if k in arrivals:
                drain(aa_r.at[k], final.at[pl.ds(0, cap)])
        here = rows_x.at[pl.ds(g * group_rows, group_rows), my_cols]
        for k in range(1, count_y):
            y_arrivals[k, g] = send(
                here, here, sem_send.at[2], dy_r.at[k - 1, g],
                tp=lax.rem(my_y + k, count_y) * CORES + my_core,
            )
        to_sibling(0, g)

    def forward_again(g):
        for k in range(1, count_y):
            y_arrivals[k, g].wait_recv()
            to_sibling(k, g)

    hand_out(0, slice(0, feats), nn(chosen, b_in[...]).astype(bf16), 0)
    forward(0)
    loads[0].wait()
    mine_stats[...] = row_sums(a_in[...])
    stat_copies = [
        send(mine_stats, slot_stats.at[k], sem_small.at[2], sem_small.at[3], tp=lax.rem(tp + k, count_tp))
        for k in range(1, count_tp)
    ]

    loads[1].wait()
    order = (
        iota((positions, positions), 1)
        == (iota((positions, positions), 0) % CHUNKS) * steps
        + iota((positions, positions), 0) // CHUNKS
    ).astype(f32).astype(bf16)
    order_t = (
        iota((positions, positions), 0)
        == (iota((positions, positions), 1) % CHUNKS) * steps
        + iota((positions, positions), 1) // CHUNKS
    ).astype(f32).astype(bf16)
    step = step_in[...]
    groups = step.shape[0]
    high = step.astype(bf16).astype(f32)
    middle = (step - high).astype(bf16).astype(f32)
    low = step - high - middle
    parts = [high, middle, low]
    padded = -(-3 * groups // 16) * 16
    if padded > 3 * groups:
        parts.append(jnp.zeros((padded - 3 * groups, positions), f32))
    split = jnp.concatenate(parts, axis=0).astype(bf16)
    split = nn(split, order_t).astype(bf16)
    for t in range(tiles):
        lanes = slice(t * tile, (t + 1) * tile)
        source = iota((padded, tile), 0)
        pick = jnp.logical_and(
            source % groups == iota((padded, tile), 1) // states + t * (tile // states),
            source < 3 * groups,
        )
        a_re[:, lanes] = tn(split, pick.astype(f32).astype(bf16))

    loads[3].wait()
    loads[17].wait()
    pick = (iota((states, flat), 0) == iota((states, flat), 1) % states).astype(f32).astype(bf16)
    own_lane = iota((groups, flat), 0) == iota((groups, flat), 1) // states

    def to_lanes(table):
        high = table.astype(bf16)
        rest = table - high.astype(f32)
        middle = rest.astype(bf16)
        low = (rest - middle.astype(f32)).astype(bf16)
        wide = nn(high, pick) + (nn(middle, pick) + nn(low, pick))
        return jnp.sum(jnp.where(own_lane, wide, 0.0), axis=0, keepdims=True)

    real, imag = to_lanes(real_in[...]), to_lanes(imag_in[...])
    denom = real * real + imag * imag
    pole[0:1, :] = real
    pole[1:2, :] = imag
    pole[2:3, :] = real / denom
    pole[3:4, :] = imag / denom
    block = min(32, positions)

    def steps_of(t):
        lanes = slice(t * tile, (t + 1) * tile)
        p_re, p_im = pole[0:1, lanes], pole[1:2, lanes]
        d_re, d_im = pole[2:3, lanes], pole[3:4, lanes]

        def elementwise(i, passed):
            here = pl.ds(pl.multiple_of(i * block, block), block)
            delta = a_re[here, lanes]
            for j in range(block // CHUNKS):
                passed = passed + delta[j * CHUNKS : (j + 1) * CHUNKS]
            magnitude = jnp.exp(p_re * delta)
            sine, cosine = sin_cos(p_im * delta)
            ab_re = magnitude * cosine
            ab_im = magnitude * sine
            numer = ab_re - 1.0
            a_re[here, lanes] = ab_re
            a_im[here, lanes] = ab_im
            u_re[here, lanes] = numer * d_re + ab_im * d_im
            u_im[here, lanes] = ab_im * d_re - numer * d_im
            return passed

        passed = lax.fori_loop(
            0, positions // block, elementwise, jnp.zeros((CHUNKS, tile), f32)
        )
        magnitude = jnp.exp(p_re * passed)
        sine, cosine = sin_cos(p_im * passed)
        sums[0, :, lanes] = magnitude * cosine
        sums[1, :, lanes] = magnitude * sine

    for t in range(tiles):
        steps_of(t)
    forward(1)
    forward_again(0)
    far_routes.wait_recv()
    chosen_far = select(owner_near, places(routes_far[...])).astype(f32).astype(bf16)

    def hand_out_far(c):
        far_tokens[c].wait_recv()
        hand_out(near, cut[c], nn(chosen_far, tokens_far[:, cut[c]]).astype(bf16), c)

    for c in range(cuts - 1):
        hand_out_far(c)
    drain(sem_small.at[3], slot_stats.at[pl.ds(1, count_tp - 1)])
    total = mine_stats[...]
    for k in range(1, count_tp):
        total = total + slot_stats[k]
    total = total.T

    loads[2].wait()
    normed = normalize(a_in[...], total, gain_a[...], width).astype(bf16)
    normed = nn(order, normed).astype(bf16)
    for i in (4, 5, 6, 7):
        loads[i].wait()

    def first_half(t):
        lanes = slice(t * tile, (t + 1) * tile)
        table = slice(t * tile_ch, (t + 1) * tile_ch)
        piece = normed[:, table]
        v_re = nn(piece, spread(in_re[table, :], group_ch, tile, states))
        v_im = nn(piece, spread(in_im[table, :], group_ch, tile, states))
        k_re, k_im = u_re[:, lanes], u_im[:, lanes]
        u_re[:, lanes] = k_re * v_re - k_im * v_im
        u_im[:, lanes] = k_re * v_im + k_im * v_re

    span = min(1024, flat)

    def chunk_sums(base):
        lanes = slice(base, base + span)

        def one(s, carried):
            s_re, s_im = carried
            here = pl.ds(pl.multiple_of(s * CHUNKS, CHUNKS), CHUNKS)
            b_re, b_im = a_re[here, lanes], a_im[here, lanes]
            return (
                b_re * s_re - b_im * s_im + u_re[here, lanes],
                b_re * s_im + b_im * s_re + u_im[here, lanes],
            )

        zero = jnp.zeros((CHUNKS, span), f32)
        sums[2, :, lanes], sums[3, :, lanes] = lax.fori_loop(0, steps, one, (zero, zero), unroll=2)

    early = groups_y // 2
    for t in range(tiles):
        first_half(t)
    for base in range(0, flat, span):
        chunk_sums(base)
    def chunk(index, c):
        return sums[index, c : c + 1, :]

    c_re, c_im, s_re, s_im = (chunk(index, 0) for index in range(4))
    for c in range(1, CHUNKS):
        b_re, b_im = chunk(0, c), chunk(1, c)
        c_re, c_im = b_re * c_re - b_im * c_im, b_re * c_im + b_im * c_re
        s_re, s_im = (
            b_re * s_re - b_im * s_im + chunk(2, c),
            b_re * s_im + b_im * s_re + chunk(3, c),
        )
    mine_state[0:1, :] = c_re
    mine_state[1:2, :] = c_im
    mine_state[2:3, :] = s_re
    mine_state[3:4, :] = s_im
    state_copies = []
    for k in range(1, count_ep):
        other = partner(me, k)
        copy = pltpu.make_async_remote_copy(
            src_ref=mine_state, dst_ref=slot_state.at[me], send_sem=hs_s.at[k], recv_sem=hs_r.at[k],
            device_id={"ep": other}, device_id_type=pl.DeviceIdType.MESH,
        )
        state_copies.append((other, copy))

        @pl.when(other > me)
        def _(copy=copy):
            copy.start()

    hand_out_far(cuts - 1)
    forward(early)
    for g in range(2, early - 1):
        forward(g)
    forward_again(1)
    loads[13].wait()
    weight = jnp.zeros((expert_rows, tokens), f32)
    for k in range(routes_in.shape[0]):
        this = routes_in[k : k + 1, :] == expert_of
        weight = jnp.where(this, weight_in[k : k + 1, :], weight)
    weight_hi = weight.astype(bf16)
    weight_lo = (weight - weight_hi.astype(f32)).astype(bf16)
    owner_far = owners(near, count_ep)
    for rows, owner, here in (
        (slice(0, near * cap), owner_near, chosen_near),
        (slice(near * cap, slots), owner_far, select(owner_far, place_own)),
    ):
        share_hi[rows, :] = jnp.where(here, nn(owner, weight_hi), 0.0).astype(bf16)
        share_lo[rows, :] = jnp.where(here, nn(owner, weight_lo), 0.0).astype(bf16)

    columns = min(256, hid)
    out_columns = min(256, feats)
    middle = early + (groups_y - early) // 2
    split = early // 2
    blocks = ((0, split), (early, middle), (middle, groups_y), (split, early))

    def rows_of(b):
        return slice(blocks[b][0] * group_rows, blocks[b][1] * group_rows)


    def normalize_rows(b):
        step_rows = min(64, group_rows)
        for r in range(rows_of(b).start, rows_of(b).stop, step_rows):
            rows = slice(r, r + step_rows)
            wide = rows_x[rows, :].astype(f32)
            average = jnp.sum(wide, axis=1, keepdims=True) / width
            square = jnp.sum(wide * wide, axis=1, keepdims=True) / width
            variance = square - average * average
            wide = (wide - average) * lax.rsqrt(variance + norm_eps) * gain_all[...]
            rows_n[rows, :] = wide.astype(bf16)

    def hidden_units(b, between):
        top = rows_of(b)
        for n in range(hid // columns):
            cols = slice(n * columns, (n + 1) * columns)
            gate = nn(rows_n[top, :], w_gate[:, cols])
            up = nn(rows_n[top, :], w_up[:, cols])
            hidden[top, cols] = (gate * jax.nn.sigmoid(gate) * up).astype(bf16)
            between(n)

    sib_copies, y_copies = {}, {}

    def down(b, target_tp, store):
        top = rows_of(b)
        for n in range(feats // out_columns):
            first = pl.multiple_of(target_tp * feats + n * out_columns, 128)
            store(
                top, slice(n * out_columns, (n + 1) * out_columns),
                nn(hidden[top, :], w_down[:, pl.ds(first, out_columns)]),
            )

    def give_back(b, offsets):
        for offset in offsets:
            yt = lax.rem(my_y + offset, count_y) * CORES

            def to_send(rows, cols, value, offset=offset):
                sib_send[offset, rows, cols] = value.astype(bf16)

            def to_own(rows, cols, value, offset=offset):
                own[offset, rows, cols] = value

            down(b, yt + 1 - my_core, to_send)
            window = pl.ds(rows_of(b).start, rows_of(b).stop - rows_of(b).start)
            sib_copies[b, offset] = send(
                sib_send.at[offset, window], sib_recv.at[offset, window],
                sem_send.at[3], rs_r.at[offset, b], tp=sibling,
            )
            down(b, yt + my_core, to_own)

    def sum_y(b):
        for offset in range(1, count_y):
            sib_copies[b, offset].wait_recv()
            rows = rows_of(b)
            y_send[offset, rows, :] = (
                own[offset, rows, :] + sib_recv[offset, rows, :].astype(f32)
            ).astype(bf16)

    def send_y(g):
        for offset in range(1, count_y):
            window = pl.ds(g * group_rows, group_rows)
            y_copies[offset, g] = send(
                y_send.at[offset, window], y_recv.at[offset, window],
                sem_send.at[4], ry_r.at[offset - 1, g],
                tp=lax.rem(my_y + offset, count_y) * CORES + my_core,
            )

    back_copies = {}

    def finish(g):
        window = slice(g * group_rows, (g + 1) * group_rows)
        total = own[0, window, :] + sib_recv[0, window, :].astype(f32)
        for offset in range(1, count_y):
            y_copies[offset, g].wait_recv()
            total = total + y_recv[offset, window, :].astype(f32)
        total = total.astype(bf16)
        final[window, :] = total
        if g == 0:
            returned[0:cap, :] = total[0:cap]
        for k in range(max(1, g * per_group), (g + 1) * per_group):
            here = pl.ds(k * cap, cap)
            back_copies[k] = send(
                final.at[here], returned.at[here], sem_send.at[5], sem_small.at[4], ep=partner(me, k)
            )

    def rows_ready(low, high):
        size = (high - low) * group_rows
        drain_rows(ds_r.at[block_of[low]], count_y * size)

    def drain_rows(sem, count):
        if count <= slots:
            drain(sem, final.at[pl.ds(0, count)])
        else:
            drain(sem, rows_x.at[:, pl.ds(0, count // slots * feats)])

    others = list(range(1, count_y))
    chunks = hid // columns

    def spread_out(tasks):
        def between(n):
            for task in tasks[n * len(tasks) // chunks : (n + 1) * len(tasks) // chunks]:
                task()

        return between

    def tasks_of(function, items):
        return [functools.partial(function, item) for item in items]

    rows_ready(*blocks[0])
    drain(sem_small.at[1], gain_all.at[:, pl.ds(0, width - feats)])
    normalize_rows(0)
    loads[14].wait()
    loads[15].wait()
    first = [early + 1, *range(early + 2, groups_y)]
    after = [[] for n in range(chunks)]
    after[max(0, chunks // 2 - 1)] += tasks_of(forward, first[:1])
    after[max(0, chunks // 2 - 1)] += tasks_of(forward_again, [early])
    after[-1] += tasks_of(forward, first[1:2])

    def between(n):
        for task in after[n]:
            task()

    hidden_units(0, between)
    loads[16].wait()
    give_back(0, others)
    for g in first[2:]:
        forward(g)
    for g in range(max(2, early - 1), early):
        forward(g)
    for g in range(2, early - 1):
        forward_again(g)
    give_back(0, [0])
    forward_again(early + 1)
    for other, copy in state_copies:

        @pl.when(other < me)
        def _(copy=copy):
            copy.wait_recv()


    def fold(q, carried):
        h_re, h_im = carried
        b_re, b_im = slot_state[q, 0:1, :], slot_state[q, 1:2, :]
        return (
            b_re * h_re - b_im * h_im + slot_state[q, 2:3, :],
            b_re * h_im + b_im * h_re + slot_state[q, 3:4, :],
        )

    blank = jnp.zeros((1, flat), f32)
    h_re, h_im = lax.fori_loop(0, me, fold, (blank, blank))
    for c in range(CHUNKS):
        enter[0, c : c + 1, :] = h_re
        enter[1, c : c + 1, :] = h_im
        b_re, b_im = chunk(0, c), chunk(1, c)
        h_re, h_im = (
            b_re * h_re - b_im * h_im + chunk(2, c),
            b_re * h_im + b_im * h_re + chunk(3, c),
        )
    for base in range(0, flat, span):
        lanes = slice(base, base + span)

        def advance(s, carried, lanes=lanes):
            s_re, s_im = carried
            found_re, found_im = [], []
            for j in range(2):
                here = pl.ds(pl.multiple_of(s * 2 * CHUNKS + j * CHUNKS, CHUNKS), CHUNKS)
                b_re, b_im = a_re[here, lanes], a_im[here, lanes]
                s_re, s_im = (
                    b_re * s_re - b_im * s_im + u_re[here, lanes],
                    b_re * s_im + b_im * s_re + u_im[here, lanes],
                )
                found_re.append(s_re)
                found_im.append(s_im)
            both = pl.ds(pl.multiple_of(s * 2 * CHUNKS, 2 * CHUNKS), 2 * CHUNKS)
            n_re[both, lanes] = jnp.concatenate(found_re, axis=0).astype(bf16)
            n_im[both, lanes] = jnp.concatenate(found_im, axis=0).astype(bf16)
            return s_re, s_im

        lax.fori_loop(0, steps // 2, advance, (enter[0, :, lanes], enter[1, :, lanes]))
    for t in range(tiles):
        lanes = slice(t * tile, (t + 1) * tile)
        table = slice(t * tile_ch, (t + 1) * tile_ch)
        response = nt(n_re[:, lanes], spread(rd_re[table, :], group_ch, tile, states)) - nt(
            n_im[:, lanes], spread(rd_im[table, :], group_ch, tile, states)
        )
        mixed[:, table] = jax.nn.gelu(response).astype(bf16)
    mixed_cols = pl.ds(pl.multiple_of(tp * channels, 128), channels)
    mixed_all[:, mixed_cols] = nn(order_t, mixed[...]).astype(bf16)

    piece_rows = positions // pieces

    def mixed_window(offset, p):
        owner_tp = lax.rem(my_y + count_y - offset, count_y) * CORES + my_core
        return mixed_all.at[
            pl.ds(p * piece_rows, piece_rows),
            pl.ds(pl.multiple_of(owner_tp * channels, 128), channels),
        ]

    mixed_y = {}

    def mixed_to_sibling(offset, p):
        here = mixed_window(offset, p)
        send(here, here, sem_send.at[6], ms_r.at[p], tp=sibling)

    def send_mixed(p):
        here = mixed_window(0, p)
        for k in range(1, count_y):
            mixed_y[k, p] = send(
                here, here, sem_send.at[7], my_r.at[k - 1, p],
                tp=lax.rem(my_y + k, count_y) * CORES + my_core,
            )
        mixed_to_sibling(0, p)

    def forward_mixed(p):
        for k in range(1, count_y):
            mixed_y[k, p].wait_recv()
            mixed_to_sibling(k, p)

    send_mixed(0)
    rows_ready(*blocks[1])
    normalize_rows(1)
    hidden_units(1, spread_out(tasks_of(forward_again, range(early + 2, groups_y))))
    give_back(1, others + [0])
    sum_y(1)
    for g in reversed(range(*blocks[1])):
        send_y(g)
    for g in range(max(2, early - 1), early):
        forward_again(g)
    rows_ready(*blocks[2])
    normalize_rows(2)
    hidden_units(2, lambda n: None)
    give_back(2, others + [0])
    sum_y(2)
    for g in reversed(range(*blocks[2])):
        send_y(g)
    for p in range(1, pieces):
        send_mixed(p)
    forward_mixed(0)
    rows_ready(*blocks[3])
    sib_copies[1, 0].wait_recv()
    sib_copies[2, 0].wait_recv()
    for g in reversed(range(*blocks[1])):
        finish(g)
    normalize_rows(3)
    hidden_units(3, lambda n: None)
    give_back(3, others + [0])
    sum_y(3)
    for g in reversed(range(*blocks[3])):
        send_y(g)
    sum_y(0)
    for g in reversed(range(*blocks[0])):
        send_y(g)
    for g in reversed(range(*blocks[2])):
        finish(g)
    loads[8].wait()
    loads[9].wait()

    def project(p):
        drain(ms_r.at[p], mixed_all.at[pl.ds(0, piece_rows), pl.ds(0, count_y * channels)])
        rows = slice(p * piece_rows, (p + 1) * piece_rows)
        out_a_cols = min(256, out_a.shape[1])
        for n in range(out_a.shape[1] // out_a_cols):
            cols = slice(n * out_a_cols, (n + 1) * out_a_cols)
            value = nn(mixed_all[rows, :], w_value[:, cols])
            gate = nn(mixed_all[rows, :], w_gate_out[:, cols])
            out_a[rows, cols] = (value * jax.nn.sigmoid(gate)).astype(bf16)

    project(0)
    for p in range(1, pieces):
        forward_mixed(p)
    sib_copies[0, 0].wait_recv()
    sib_copies[3, 0].wait_recv()
    for g in reversed(range(*blocks[3])):
        finish(g)
    for p in range(1, pieces):
        project(p)
    for g in reversed(range(*blocks[0])):
        finish(g)
    drain(sem_small.at[4], returned.at[pl.ds(cap, slots - cap)])
    out_b[...] = (tn(share_hi[...], returned[...]) + tn(share_lo[...], returned[...])).astype(bf16)
    for other, copy in state_copies:

        @pl.when(other > me)
        def _(copy=copy):
            copy.wait_send()

    far_routes.wait_send()
    drain(sem_far.at[2], tokens_far)
    drain(sem_small.at[0], gain_all.at[:, pl.ds(0, width - feats)])
    drain(sem_small.at[2], slot_stats.at[pl.ds(1, count_tp - 1)])
    drain_rows(sem_send.at[0], 2 * (near - 1) * cap)
    drain_rows(sem_send.at[1], count_y * slots)
    drain_rows(sem_send.at[2], (count_y - 1) * slots)
    drain_rows(sem_send.at[3], count_y * slots)
    drain_rows(sem_send.at[4], (count_y - 1) * slots)
    drain_rows(sem_send.at[5], slots - cap)
    drain(sem_send.at[6], mixed_all.at[:, pl.ds(0, count_y * channels)])
    drain(sem_send.at[7], mixed_all.at[:, pl.ds(0, (count_y - 1) * channels)])


def fused(args, state_size, capacity):
    count_ep, count_tp = lax.axis_size("ep"), lax.axis_size("tp")
    count_y = count_tp // CORES
    positions, channels = args[0].shape
    groups = args[1].shape[0]
    tokens, feats = args[10].shape
    flat = args[3].shape[0] * args[3].shape[1]
    slots = count_ep * capacity
    hid = args[14].shape[1]
    width = feats * count_tp
    groups_y, pieces = min(count_ep, 8), 2
    dma = pltpu.SemaphoreType.DMA
    vmem = pltpu.VMEM
    scratch = [vmem(x.shape, x.dtype) for x in args] + [
        vmem((8, positions), f32),
        vmem((count_tp, 8, positions), f32),
        vmem((4, flat), f32),
        vmem((tokens, feats), bf16),
        vmem(args[12].shape, args[12].dtype),
        vmem((1, width), f32),
        vmem((slots, width), bf16),
        vmem((slots, feats), bf16),
        vmem((slots, width), bf16),
        vmem((slots, tokens), bf16),
        vmem((slots, tokens), bf16),
        vmem((positions, flat), f32),
        vmem((positions, flat), f32),
        vmem((positions, flat), f32),
        vmem((positions, flat), f32),
        vmem((4, CHUNKS, flat), f32),
        vmem((2, CHUNKS, flat), f32),
        vmem((4, flat), f32),
        vmem((count_ep, 4, flat), f32),
        vmem((positions, flat), bf16),
        vmem((positions, flat), bf16),
        vmem((positions, channels), bf16),
        vmem((positions, channels * count_tp), bf16),
        vmem((slots, hid), bf16),
        vmem((count_y, slots, feats), f32),
        vmem((count_y, slots, feats), bf16),
        vmem((count_y, slots, feats), bf16),
        vmem((count_y, slots, feats), bf16),
        vmem((count_y, slots, feats), bf16),
        vmem((slots, feats), bf16),
        vmem((slots, feats), bf16),
        dma((len(args),)),
        dma((5,)),
        dma((5,)),
        dma((8,)),
        dma((count_ep,)),
        dma((count_y - 1, groups_y)),
        dma((4,)),
        dma((count_ep,)), dma((count_ep,)),
        dma((count_y - 1, pieces)),
        dma((pieces,)),
        dma((count_y, 4)),
        dma((count_y - 1, groups_y)),
    ]
    return pl.pallas_call(
        functools.partial(kernel, (count_ep, count_tp, groups_y, pieces, state_size)),
        out_shape=[
            vmem((positions, args[8].shape[1]), bf16),
            vmem((tokens, feats), bf16),
        ],
        in_specs=[pl.BlockSpec(memory_space=pltpu.HBM)] * len(args),
        out_specs=[pl.BlockSpec(memory_space=pltpu.VMEM)] * 2,
        scratch_shapes=scratch,
        compiler_params=pltpu.CompilerParams(
            collective_id=0, has_side_effects=True, vmem_limit_bytes=60 * 1024 * 1024
        ),
    )(*args)


def write_out(a_ref, b_ref, a_out, b_out, sems):
    copies = [
        pltpu.make_async_copy(source, target, sems.at[i])
        for i, (source, target) in enumerate(((a_ref, a_out), (b_ref, b_out)))
    ]
    for copy in copies:
        copy.start()
    for copy in copies:
        copy.wait()


def shards(
    mixer_input, mixer_gain, time_step, pole_real, pole_imag, input_real, input_imag,
    read_real, read_imag, out_value, out_gate, expert_input, expert_gain, routes,
    route_weight, expert_gate, expert_up, expert_down,
):
    tokens, top = routes.shape
    capacity = 2 * top * tokens // lax.axis_size("ep")
    def by_channel(table):
        return jnp.swapaxes(table, 1, 2).reshape(-1, table.shape[1])

    args = (
        mixer_input, time_step.T, mixer_gain[None, :], pole_real,
        by_channel(input_real), by_channel(input_imag),
        read_real.reshape(-1, read_real.shape[2]), read_imag.reshape(-1, read_imag.shape[2]),
        out_value, out_gate, expert_input, expert_gain[None, :], routes.T, route_weight.T,
        expert_gate[0], expert_up[0], expert_down[0], pole_imag,
    )
    results = fused(args, pole_real.shape[1], capacity)
    return tuple(
        pl.pallas_call(
            write_out,
            out_shape=[jax.ShapeDtypeStruct(x.shape, x.dtype) for x in results],
            in_specs=[pl.BlockSpec(memory_space=pltpu.VMEM)] * 2,
            out_specs=[pl.BlockSpec(memory_space=pltpu.HBM)] * 2,
            scratch_shapes=[pltpu.SemaphoreType.DMA((2,))],
            compiler_params=pltpu.CompilerParams(vmem_limit_bytes=1024 * 1024),
        )(*results)
    )


def solution(mesh):
    return jax.shard_map(
        shards,
        mesh=mesh,
        in_specs=(
            P("ep", "tp"), P("tp"), P("ep", "tp"), P("tp", None), P("tp", None),
            P("tp", None, None), P("tp", None, None), P("tp", None, None), P("tp", None, None),
            P(None, "tp"), P(None, "tp"), P("ep", "tp"), P("tp"), P("ep", None), P("ep", None),
            P("ep", None, "tp"), P("ep", None, "tp"), P("ep", "tp", None),
        ),
        out_specs=(P("ep", "tp"), P("ep", "tp")),
        check_vma=False,
    )
```

```python
import functools
import jax
import jax.numpy as jnp
from jax import lax
from jax.experimental import pallas as pl
from jax.experimental.pallas import tpu as pltpu
from jax.sharding import PartitionSpec as P

norm_eps = 1e-05
CHUNKS = 8
CORES = 2
f32 = jnp.float32
bf16 = jnp.bfloat16


def sin_cos(angle):
    turns = jnp.round(angle * 0.6366197723675814)
    left = angle - turns * 1.5703125
    left = left - turns * 4.83751296997e-4
    left = left - turns * 7.549789948768648e-8
    sq = left * left
    sine = ((-1.9515295891e-4 * sq + 8.3321608736e-3) * sq - 1.6666654611e-1) * sq * left + left
    cosine = (
        ((2.443315711809948e-5 * sq - 1.388731625493765e-3) * sq + 4.166664568298827e-2) * sq * sq
        - 0.5 * sq
        + 1.0
    )
    quadrant = turns.astype(jnp.int32)
    odd = (quadrant & 1) == 1
    sin_out = jnp.where(odd, cosine, sine)
    cos_out = jnp.where(odd, sine, cosine)
    sin_out = jnp.where((quadrant & 2) == 2, -sin_out, sin_out)
    cos_out = jnp.where(((quadrant + 1) & 2) == 2, -cos_out, cos_out)
    return sin_out, cos_out


def iota(shape, dim):
    return lax.broadcasted_iota(jnp.int32, shape, dim)


def nn(left, right):
    return jnp.dot(left, right, preferred_element_type=f32)


def nt(left, right):
    return lax.dot_general(left, right, (((1,), (1,)), ((), ())), preferred_element_type=f32)


def tn(left, right):
    return lax.dot_general(left, right, (((0,), (0,)), ((), ())), preferred_element_type=f32)


def partner(me, k):
    other, bit = me, 1
    while bit <= k:
        if k & bit:
            other = other + bit * (1 - 2 * ((me // bit) % 2))
        bit *= 2
    return other


def spread(table, row_div, lanes, lane_div):
    rows, width = table.shape
    pick = (iota((width, lanes), 0) == iota((width, lanes), 1) % width).astype(bf16)
    wide = nn(table.astype(bf16), pick)
    same = iota((rows, lanes), 0) // row_div == iota((rows, lanes), 1) // lane_div
    return jnp.where(same, wide, 0.0).astype(bf16)


def row_sums(rows):
    ones = jnp.ones((16, rows.shape[1]), bf16)
    wide = rows.astype(f32)
    square = wide * wide
    high = square.astype(bf16)
    low = (square - high.astype(f32)).astype(bf16)
    sums = nt(ones, rows)
    squares = nt(ones, high) + nt(ones, low)
    return jnp.where(iota((8, 1), 0) == 0, sums[:8], squares[:8])


def normalize(rows, stats, gain, width):
    average = stats[:, 0:1] / width
    variance = stats[:, 1:2] / width - average * average
    return (rows.astype(f32) - average) * lax.rsqrt(variance + norm_eps) * gain


def kernel(dims, *refs):
    count_ep, count_tp, groups_y, pieces, state_size = dims
    hbm, refs = refs[:18], refs[18:]
    (out_a, out_b), refs = refs[:2], refs[2:]
    vm, refs = refs[:18], refs[18:]
    (
        mine_stats, slot_stats, pole, tokens_far, routes_far, gain_all, rows_n, outgoing, rows_x, share_hi, share_lo, a_re, a_im, u_re, u_im,
        sums, enter, mine_state, slot_state, n_re, n_im, mixed, mixed_all, hidden, own,
        sib_send, sib_recv, y_send, y_recv, final, returned,
        sem_in, sem_far, sem_small, sem_send, aa_r, dy_r, ds_r, hs_s, hs_r, my_r, ms_r, rs_r, ry_r,
    ) = refs
    (
        a_in, step_in, gain_a, real_in, in_re, in_im, rd_re, rd_im, w_value, w_gate_out,
        b_in, gain_b, routes_in, weight_in, w_gate, w_up, w_down, imag_in,
    ) = vm

    me = lax.axis_index("ep")
    tp = lax.axis_index("tp")
    count_y = count_tp // CORES
    my_y = tp // CORES
    my_core = tp % CORES
    sibling = my_y * CORES + 1 - my_core

    barrier = pltpu.get_barrier_semaphore()
    for k in range(1, count_ep):
        pl.semaphore_signal(
            barrier, inc=1, device_id={"ep": partner(me, k)}, device_id_type=pl.DeviceIdType.MESH
        )
    for k in range(1, count_tp):
        pl.semaphore_signal(
            barrier, inc=1, device_id={"tp": lax.rem(tp + k, count_tp)},
            device_id_type=pl.DeviceIdType.MESH,
        )

    loads = [
        pltpu.make_async_copy(source, target, sem_in.at[i])
        for i, (source, target) in enumerate(zip(hbm, vm))
    ]
    for i in (10, 12, 11, 0, 1, 3, 17, 2, 13, 4, 5, 6, 7, 14, 15, 16, 8, 9):
        loads[i].start()

    def send(source, target, send_sem, recv_sem, **where):
        copy = pltpu.make_async_remote_copy(
            src_ref=source, dst_ref=target, send_sem=send_sem, recv_sem=recv_sem,
            device_id=where, device_id_type=pl.DeviceIdType.MESH,
        )
        copy.start()
        return copy

    def drain(sem, ref):
        pltpu.make_async_copy(ref, ref, sem).wait()

    positions, channels = a_in.shape
    tokens, feats = b_in.shape
    width = feats * count_tp
    flat = a_re.shape[1]
    states = state_size
    group_ch = in_re.shape[0] * states // flat
    slots = rows_x.shape[0]
    cap = slots // count_ep
    tile = min(256, flat)
    tiles = flat // tile
    tile_ch = tile // states * group_ch
    steps = positions // CHUNKS
    hid = w_gate.shape[1]
    expert_rows = max(16, count_ep)
    my_cols = pl.ds(pl.multiple_of(tp * feats, 128), feats)

    portal = partner(me, count_ep // 2)
    for i in (12, 11, 10):
        loads[i].wait()
    pl.semaphore_wait(barrier, count_ep + count_tp - 2)
    far_routes = send(routes_in, routes_far, sem_far.at[0], sem_far.at[1], ep=portal)
    cuts = 2 if feats % 256 == 0 else 1
    cut = [slice(c * feats // cuts, (c + 1) * feats // cuts) for c in range(cuts)]
    far_tokens = [
        send(
            b_in.at[:, cut[c]], tokens_far.at[:, cut[c]], sem_far.at[2], sem_far.at[3 + c],
            ep=portal,
        )
        for c in range(cuts)
    ]
    gain_copies = [
        send(
            gain_b, gain_all.at[:, my_cols], sem_small.at[0], sem_small.at[1], tp=lax.rem(tp + k, count_tp)
        )
        for k in range(1, count_tp)
    ]
    gain_all[:, my_cols] = gain_b[...]
    near = count_ep // 2
    expert_of = iota((expert_rows, tokens), 0)
    before = (iota((tokens, tokens), 0) < iota((tokens, tokens), 1)).astype(bf16)

    def places(routes):
        hit = jnp.zeros((expert_rows, tokens), jnp.bool_)
        for k in range(routes.shape[0]):
            hit = jnp.logical_or(hit, routes[k : k + 1, :] == expert_of)
        place = nn(hit.astype(f32).astype(bf16), before)
        return jnp.where(hit, place, -1.0).astype(bf16)

    def owners(low, high):
        return jnp.concatenate(
            [
                (iota((cap, expert_rows), 1) == partner(me, k)).astype(f32)
                for k in range(low, high)
            ],
            axis=0,
        ).astype(bf16)

    def select(owner, place):
        return nn(owner, place) == (iota((owner.shape[0], tokens), 0) % cap).astype(f32)

    place_own = places(routes_in[...])
    owner_near = owners(0, near)
    chosen_near = select(owner_near, place_own)
    chosen = chosen_near.astype(f32).astype(bf16)

    arrivals = set()

    def hand_out(base, columns, values, ks):
        outgoing[base * cap : (base + near) * cap, columns] = values
        rows_x[base * cap : (base + 1) * cap, window_of(columns)] = values[0:cap]
        send_slabs(base, columns, ks)

    def window_of(columns):
        size = columns.stop - columns.start
        return pl.ds(pl.multiple_of(tp * feats + columns.start, 128), size)

    def send_slabs(base, columns, ks):
        for k in ks:
            here = pl.ds((base + k) * cap, cap)
            arrivals.add(base + k)
            send(
                outgoing.at[here, columns], rows_x.at[here, window_of(columns)], sem_send.at[0],
                aa_r.at[base + k], ep=partner(me, k),
            )

    per_group = count_ep // groups_y
    group_rows = per_group * cap
    y_arrivals = {}
    block_of = [g // (groups_y // 4) if groups_y >= 4 else g for g in range(groups_y)]

    def core_cols(offset):
        owner_tp = lax.rem(my_y + count_y - offset, count_y) * CORES + my_core
        return pl.ds(pl.multiple_of(owner_tp * feats, 128), feats)

    def to_sibling(offset, g):
        here = rows_x.at[pl.ds(g * group_rows, group_rows), core_cols(offset)]
        send(here, here, sem_send.at[1], ds_r.at[block_of[g]], tp=sibling)

    def forward(g):
        for k in range(g * per_group, (g + 1) * per_group):
            if k in arrivals:
                drain(aa_r.at[k], final.at[pl.ds(0, cap)])
        here = rows_x.at[pl.ds(g * group_rows, group_rows), my_cols]
        for k in range(1, count_y):
            y_arrivals[k, g] = send(
                here, here, sem_send.at[2], dy_r.at[k - 1, g],
                tp=lax.rem(my_y + k, count_y) * CORES + my_core,
            )
        to_sibling(0, g)

    def forward_again(g):
        for k in range(1, count_y):
            y_arrivals[k, g].wait_recv()
            to_sibling(k, g)

    near_first = max(2, near // 2)
    hand_out(0, slice(0, feats), nn(chosen, b_in[...]).astype(bf16), range(1, near))
    forward(0)
    loads[0].wait()
    mine_stats[...] = row_sums(a_in[...])
    stat_copies = [
        send(mine_stats, slot_stats.at[k], sem_small.at[2], sem_small.at[3], tp=lax.rem(tp + k, count_tp))
        for k in range(1, count_tp)
    ]

    loads[1].wait()
    order = (
        iota((positions, positions), 1)
        == (iota((positions, positions), 0) % CHUNKS) * steps
        + iota((positions, positions), 0) // CHUNKS
    ).astype(f32).astype(bf16)
    order_t = (
        iota((positions, positions), 0)
        == (iota((positions, positions), 1) % CHUNKS) * steps
        + iota((positions, positions), 1) // CHUNKS
    ).astype(f32).astype(bf16)
    step = step_in[...]
    groups = step.shape[0]
    high = step.astype(bf16).astype(f32)
    middle = (step - high).astype(bf16).astype(f32)
    low = step - high - middle
    parts = [high, middle, low]
    padded = -(-3 * groups // 16) * 16
    if padded > 3 * groups:
        parts.append(jnp.zeros((padded - 3 * groups, positions), f32))
    split = jnp.concatenate(parts, axis=0).astype(bf16)
    split = nn(split, order_t).astype(bf16)
    for t in range(tiles):
        lanes = slice(t * tile, (t + 1) * tile)
        source = iota((padded, tile), 0)
        pick = jnp.logical_and(
            source % groups == iota((padded, tile), 1) // states + t * (tile // states),
            source < 3 * groups,
        )
        a_re[:, lanes] = tn(split, pick.astype(f32).astype(bf16))

    loads[3].wait()
    loads[17].wait()
    pick = (iota((states, flat), 0) == iota((states, flat), 1) % states).astype(f32).astype(bf16)
    own_lane = iota((groups, flat), 0) == iota((groups, flat), 1) // states

    def to_lanes(table):
        high = table.astype(bf16)
        rest = table - high.astype(f32)
        middle = rest.astype(bf16)
        low = (rest - middle.astype(f32)).astype(bf16)
        wide = nn(high, pick) + (nn(middle, pick) + nn(low, pick))
        return jnp.sum(jnp.where(own_lane, wide, 0.0), axis=0, keepdims=True)

    real, imag = to_lanes(real_in[...]), to_lanes(imag_in[...])
    denom = real * real + imag * imag
    pole[0:1, :] = real
    pole[1:2, :] = imag
    pole[2:3, :] = real / denom
    pole[3:4, :] = imag / denom
    block = min(32, positions)

    def steps_of(t):
        lanes = slice(t * tile, (t + 1) * tile)
        p_re, p_im = pole[0:1, lanes], pole[1:2, lanes]
        d_re, d_im = pole[2:3, lanes], pole[3:4, lanes]

        def elementwise(i, passed):
            here = pl.ds(pl.multiple_of(i * block, block), block)
            delta = a_re[here, lanes]
            for j in range(block // CHUNKS):
                passed = passed + delta[j * CHUNKS : (j + 1) * CHUNKS]
            magnitude = jnp.exp(p_re * delta)
            sine, cosine = sin_cos(p_im * delta)
            ab_re = magnitude * cosine
            ab_im = magnitude * sine
            numer = ab_re - 1.0
            a_re[here, lanes] = ab_re
            a_im[here, lanes] = ab_im
            u_re[here, lanes] = numer * d_re + ab_im * d_im
            u_im[here, lanes] = ab_im * d_re - numer * d_im
            return passed

        passed = lax.fori_loop(
            0, positions // block, elementwise, jnp.zeros((CHUNKS, tile), f32)
        )
        magnitude = jnp.exp(p_re * passed)
        sine, cosine = sin_cos(p_im * passed)
        sums[0, :, lanes] = magnitude * cosine
        sums[1, :, lanes] = magnitude * sine

    for t in range(tiles):
        steps_of(t)
    forward(1)
    forward_again(0)
    far_routes.wait_recv()
    chosen_far = select(owner_near, places(routes_far[...])).astype(f32).astype(bf16)

    def hand_out_far(c):
        far_tokens[c].wait_recv()
        hand_out(near, cut[c], nn(chosen_far, tokens_far[:, cut[c]]).astype(bf16), range(1, near))

    for c in range(cuts - 1):
        hand_out_far(c)
    drain(sem_small.at[3], slot_stats.at[pl.ds(1, count_tp - 1)])
    total = mine_stats[...]
    for k in range(1, count_tp):
        total = total + slot_stats[k]
    total = total.T

    loads[2].wait()
    normed = normalize(a_in[...], total, gain_a[...], width).astype(bf16)
    normed = nn(order, normed).astype(bf16)
    for i in (4, 5, 6, 7):
        loads[i].wait()

    def first_half(t):
        lanes = slice(t * tile, (t + 1) * tile)
        table = slice(t * tile_ch, (t + 1) * tile_ch)
        piece = normed[:, table]
        v_re = nn(piece, spread(in_re[table, :], group_ch, tile, states))
        v_im = nn(piece, spread(in_im[table, :], group_ch, tile, states))
        k_re, k_im = u_re[:, lanes], u_im[:, lanes]
        u_re[:, lanes] = k_re * v_re - k_im * v_im
        u_im[:, lanes] = k_re * v_im + k_im * v_re

    span = min(1024, flat)

    def chunk_sums(base):
        lanes = slice(base, base + span)

        def one(s, carried):
            s_re, s_im = carried
            here = pl.ds(pl.multiple_of(s * CHUNKS, CHUNKS), CHUNKS)
            b_re, b_im = a_re[here, lanes], a_im[here, lanes]
            return (
                b_re * s_re - b_im * s_im + u_re[here, lanes],
                b_re * s_im + b_im * s_re + u_im[here, lanes],
            )

        zero = jnp.zeros((CHUNKS, span), f32)
        sums[2, :, lanes], sums[3, :, lanes] = lax.fori_loop(0, steps, one, (zero, zero), unroll=2)

    early = groups_y // 2
    for t in range(tiles // 2):
        first_half(t)
    hand_out_far(cuts - 1)
    forward(early)
    for t in range(tiles // 2, tiles):
        first_half(t)
    for base in range(0, flat, span):
        chunk_sums(base)
    def chunk(index, c):
        return sums[index, c : c + 1, :]

    c_re, c_im, s_re, s_im = (chunk(index, 0) for index in range(4))
    for c in range(1, CHUNKS):
        b_re, b_im = chunk(0, c), chunk(1, c)
        c_re, c_im = b_re * c_re - b_im * c_im, b_re * c_im + b_im * c_re
        s_re, s_im = (
            b_re * s_re - b_im * s_im + chunk(2, c),
            b_re * s_im + b_im * s_re + chunk(3, c),
        )
    mine_state[0:1, :] = c_re
    mine_state[1:2, :] = c_im
    mine_state[2:3, :] = s_re
    mine_state[3:4, :] = s_im
    state_copies = []
    for k in range(1, count_ep):
        other = partner(me, k)
        copy = pltpu.make_async_remote_copy(
            src_ref=mine_state, dst_ref=slot_state.at[me], send_sem=hs_s.at[k], recv_sem=hs_r.at[k],
            device_id={"ep": other}, device_id_type=pl.DeviceIdType.MESH,
        )
        state_copies.append((other, copy))

        @pl.when(other > me)
        def _(copy=copy):
            copy.start()

    for g in range(2, min(3, early)):
        forward(g)
    forward_again(1)
    loads[13].wait()
    weight = jnp.zeros((expert_rows, tokens), f32)
    for k in range(routes_in.shape[0]):
        this = routes_in[k : k + 1, :] == expert_of
        weight = jnp.where(this, weight_in[k : k + 1, :], weight)
    weight_hi = weight.astype(bf16)
    weight_lo = (weight - weight_hi.astype(f32)).astype(bf16)
    owner_far = owners(near, count_ep)
    for rows, owner, here in (
        (slice(0, near * cap), owner_near, chosen_near),
        (slice(near * cap, slots), owner_far, select(owner_far, place_own)),
    ):
        share_hi[rows, :] = jnp.where(here, nn(owner, weight_hi), 0.0).astype(bf16)
        share_lo[rows, :] = jnp.where(here, nn(owner, weight_lo), 0.0).astype(bf16)

    columns = min(256, hid)
    out_columns = min(256, feats)
    middle = early + (groups_y - early) // 2
    split = early // 2
    blocks = ((0, split), (early, middle), (middle, groups_y), (split, early))

    def rows_of(b):
        return slice(blocks[b][0] * group_rows, blocks[b][1] * group_rows)


    def normalize_rows(b):
        step_rows = min(64, group_rows)
        for r in range(rows_of(b).start, rows_of(b).stop, step_rows):
            rows = slice(r, r + step_rows)
            wide = rows_x[rows, :].astype(f32)
            average = jnp.sum(wide, axis=1, keepdims=True) / width
            square = jnp.sum(wide * wide, axis=1, keepdims=True) / width
            variance = square - average * average
            wide = (wide - average) * lax.rsqrt(variance + norm_eps) * gain_all[...]
            rows_n[rows, :] = wide.astype(bf16)

    def hidden_units(b, between):
        top = rows_of(b)
        for n in range(hid // columns):
            cols = slice(n * columns, (n + 1) * columns)
            gate = nn(rows_n[top, :], w_gate[:, cols])
            up = nn(rows_n[top, :], w_up[:, cols])
            hidden[top, cols] = (gate * jax.nn.sigmoid(gate) * up).astype(bf16)
            between(n)

    sib_copies, y_copies = {}, {}

    def down(b, target_tp, store):
        top = rows_of(b)
        for n in range(feats // out_columns):
            first = pl.multiple_of(target_tp * feats + n * out_columns, 128)
            store(
                top, slice(n * out_columns, (n + 1) * out_columns),
                nn(hidden[top, :], w_down[:, pl.ds(first, out_columns)]),
            )

    def give_back(b, offsets):
        for offset in offsets:
            yt = lax.rem(my_y + offset, count_y) * CORES

            def to_send(rows, cols, value, offset=offset):
                sib_send[offset, rows, cols] = value.astype(bf16)

            def to_own(rows, cols, value, offset=offset):
                own[offset, rows, cols] = value

            down(b, yt + 1 - my_core, to_send)
            window = pl.ds(rows_of(b).start, rows_of(b).stop - rows_of(b).start)
            sib_copies[b, offset] = send(
                sib_send.at[offset, window], sib_recv.at[offset, window],
                sem_send.at[3], rs_r.at[offset, b], tp=sibling,
            )
            down(b, yt + my_core, to_own)

    def sum_y(b):
        for offset in range(1, count_y):
            sib_copies[b, offset].wait_recv()
            rows = rows_of(b)
            y_send[offset, rows, :] = (
                own[offset, rows, :] + sib_recv[offset, rows, :].astype(f32)
            ).astype(bf16)

    def send_y(g):
        for offset in range(1, count_y):
            window = pl.ds(g * group_rows, group_rows)
            y_copies[offset, g] = send(
                y_send.at[offset, window], y_recv.at[offset, window],
                sem_send.at[4], ry_r.at[offset - 1, g],
                tp=lax.rem(my_y + offset, count_y) * CORES + my_core,
            )

    back_copies = {}

    def finish(g):
        window = slice(g * group_rows, (g + 1) * group_rows)
        total = own[0, window, :] + sib_recv[0, window, :].astype(f32)
        for offset in range(1, count_y):
            y_copies[offset, g].wait_recv()
            total = total + y_recv[offset, window, :].astype(f32)
        total = total.astype(bf16)
        final[window, :] = total
        if g == 0:
            returned[0:cap, :] = total[0:cap]
        for k in range(max(1, g * per_group), (g + 1) * per_group):
            here = pl.ds(k * cap, cap)
            back_copies[k] = send(
                final.at[here], returned.at[here], sem_send.at[5], sem_small.at[4], ep=partner(me, k)
            )

    def rows_ready(low, high):
        size = (high - low) * group_rows
        drain_rows(ds_r.at[block_of[low]], count_y * size)

    def drain_rows(sem, count):
        if count <= slots:
            drain(sem, final.at[pl.ds(0, count)])
        else:
            drain(sem, rows_x.at[:, pl.ds(0, count // slots * feats)])

    others = list(range(1, count_y))
    chunks = hid // columns

    def spread_out(tasks):
        def between(n):
            for task in tasks[n * len(tasks) // chunks : (n + 1) * len(tasks) // chunks]:
                task()

        return between

    def tasks_of(function, items):
        return [functools.partial(function, item) for item in items]

    rows_ready(*blocks[0])
    drain(sem_small.at[1], gain_all.at[:, pl.ds(0, width - feats)])
    normalize_rows(0)
    loads[14].wait()
    loads[15].wait()
    first = [early + 1, *range(early + 2, groups_y)]
    after = [[] for n in range(chunks)]
    after[max(0, chunks // 2 - 1)] += tasks_of(forward, first[:1])
    after[max(0, chunks // 2 - 1)] += tasks_of(forward_again, [early])
    after[-1] += tasks_of(forward, first[1:2])

    def between(n):
        for task in after[n]:
            task()

    hidden_units(0, between)
    loads[16].wait()
    give_back(0, others)
    for g in first[2:]:
        forward(g)
    give_back(0, [0])
    forward_again(early + 1)
    for other, copy in state_copies:

        @pl.when(other < me)
        def _(copy=copy):
            copy.wait_recv()


    def fold(q, carried):
        h_re, h_im = carried
        b_re, b_im = slot_state[q, 0:1, :], slot_state[q, 1:2, :]
        return (
            b_re * h_re - b_im * h_im + slot_state[q, 2:3, :],
            b_re * h_im + b_im * h_re + slot_state[q, 3:4, :],
        )

    blank = jnp.zeros((1, flat), f32)
    h_re, h_im = lax.fori_loop(0, me, fold, (blank, blank))
    for c in range(CHUNKS):
        enter[0, c : c + 1, :] = h_re
        enter[1, c : c + 1, :] = h_im
        b_re, b_im = chunk(0, c), chunk(1, c)
        h_re, h_im = (
            b_re * h_re - b_im * h_im + chunk(2, c),
            b_re * h_im + b_im * h_re + chunk(3, c),
        )
    for base in range(0, flat, span):
        lanes = slice(base, base + span)

        def advance(s, carried, lanes=lanes):
            s_re, s_im = carried
            found_re, found_im = [], []
            for j in range(2):
                here = pl.ds(pl.multiple_of(s * 2 * CHUNKS + j * CHUNKS, CHUNKS), CHUNKS)
                b_re, b_im = a_re[here, lanes], a_im[here, lanes]
                s_re, s_im = (
                    b_re * s_re - b_im * s_im + u_re[here, lanes],
                    b_re * s_im + b_im * s_re + u_im[here, lanes],
                )
                found_re.append(s_re)
                found_im.append(s_im)
            both = pl.ds(pl.multiple_of(s * 2 * CHUNKS, 2 * CHUNKS), 2 * CHUNKS)
            n_re[both, lanes] = jnp.concatenate(found_re, axis=0).astype(bf16)
            n_im[both, lanes] = jnp.concatenate(found_im, axis=0).astype(bf16)
            return s_re, s_im

        lax.fori_loop(0, steps // 2, advance, (enter[0, :, lanes], enter[1, :, lanes]))
    for g in range(3, early):
        forward(g)
    for t in range(tiles):
        lanes = slice(t * tile, (t + 1) * tile)
        table = slice(t * tile_ch, (t + 1) * tile_ch)
        response = nt(n_re[:, lanes], spread(rd_re[table, :], group_ch, tile, states)) - nt(
            n_im[:, lanes], spread(rd_im[table, :], group_ch, tile, states)
        )
        mixed[:, table] = jax.nn.gelu(response).astype(bf16)
    mixed_cols = pl.ds(pl.multiple_of(tp * channels, 128), channels)
    mixed_all[:, mixed_cols] = nn(order_t, mixed[...]).astype(bf16)

    piece_rows = positions // pieces

    def mixed_window(offset, p):
        owner_tp = lax.rem(my_y + count_y - offset, count_y) * CORES + my_core
        return mixed_all.at[
            pl.ds(p * piece_rows, piece_rows),
            pl.ds(pl.multiple_of(owner_tp * channels, 128), channels),
        ]

    mixed_y = {}

    def mixed_to_sibling(offset, p):
        here = mixed_window(offset, p)
        send(here, here, sem_send.at[6], ms_r.at[p], tp=sibling)

    def send_mixed(p):
        here = mixed_window(0, p)
        for k in range(1, count_y):
            mixed_y[k, p] = send(
                here, here, sem_send.at[7], my_r.at[k - 1, p],
                tp=lax.rem(my_y + k, count_y) * CORES + my_core,
            )
        mixed_to_sibling(0, p)

    def forward_mixed(p):
        for k in range(1, count_y):
            mixed_y[k, p].wait_recv()
            mixed_to_sibling(k, p)

    send_mixed(0)
    rows_ready(*blocks[1])
    normalize_rows(1)
    hidden_units(1, spread_out(tasks_of(forward_again, range(early + 2, groups_y))))
    give_back(1, others + [0])
    sum_y(1)
    for g in reversed(range(*blocks[1])):
        send_y(g)
    rows_ready(*blocks[2])
    normalize_rows(2)
    hidden_units(2, spread_out(tasks_of(forward_again, range(2, early))))
    give_back(2, others + [0])
    sum_y(2)
    for g in reversed(range(*blocks[2])):
        send_y(g)
    sum_y(0)
    for g in reversed(range(1, split)):
        send_y(g)
    forward_mixed(0)
    rows_ready(*blocks[3])
    normalize_rows(3)
    sib_copies[1, 0].wait_recv()
    sib_copies[2, 0].wait_recv()
    far_order = list(reversed(range(*blocks[1]))) + list(reversed(range(*blocks[2])))

    def one_finish(n):
        if n == chunks - 1:
            finish(far_order[0])
            finish(far_order[1])

    hidden_units(3, one_finish)
    give_back(3, others + [0])
    sum_y(3)
    for g in reversed(range(*blocks[3])):
        send_y(g)
    for p in range(1, pieces):
        send_mixed(p)
    send_y(0)
    for g in far_order[2:]:
        finish(g)
    loads[8].wait()
    loads[9].wait()

    def project(p):
        drain(ms_r.at[p], mixed_all.at[pl.ds(0, piece_rows), pl.ds(0, count_y * channels)])
        rows = slice(p * piece_rows, (p + 1) * piece_rows)
        out_a_cols = min(256, out_a.shape[1])
        for n in range(out_a.shape[1] // out_a_cols):
            cols = slice(n * out_a_cols, (n + 1) * out_a_cols)
            value = nn(mixed_all[rows, :], w_value[:, cols])
            gate = nn(mixed_all[rows, :], w_gate_out[:, cols])
            out_a[rows, cols] = (value * jax.nn.sigmoid(gate)).astype(bf16)

    project(0)
    sib_copies[0, 0].wait_recv()
    sib_copies[3, 0].wait_recv()
    for g in reversed(range(1, split)):
        finish(g)
    for g in reversed(range(*blocks[3])):
        finish(g)
    for p in range(1, pieces):
        forward_mixed(p)
    finish(0)
    for p in range(1, pieces):
        project(p)
    drain(sem_small.at[4], returned.at[pl.ds(cap, slots - cap)])
    out_b[...] = (tn(share_hi[...], returned[...]) + tn(share_lo[...], returned[...])).astype(bf16)
    for other, copy in state_copies:

        @pl.when(other > me)
        def _(copy=copy):
            copy.wait_send()

    far_routes.wait_send()
    drain(sem_far.at[2], tokens_far)
    drain(sem_small.at[0], gain_all.at[:, pl.ds(0, width - feats)])
    drain(sem_small.at[2], slot_stats.at[pl.ds(1, count_tp - 1)])
    drain_rows(sem_send.at[0], 2 * (near - 1) * cap)
    drain_rows(sem_send.at[1], count_y * slots)
    drain_rows(sem_send.at[2], (count_y - 1) * slots)
    drain_rows(sem_send.at[3], count_y * slots)
    drain_rows(sem_send.at[4], (count_y - 1) * slots)
    drain_rows(sem_send.at[5], slots - cap)
    drain(sem_send.at[6], mixed_all.at[:, pl.ds(0, count_y * channels)])
    drain(sem_send.at[7], mixed_all.at[:, pl.ds(0, (count_y - 1) * channels)])


def fused(args, state_size, capacity):
    count_ep, count_tp = lax.axis_size("ep"), lax.axis_size("tp")
    count_y = count_tp // CORES
    positions, channels = args[0].shape
    groups = args[1].shape[0]
    tokens, feats = args[10].shape
    flat = args[3].shape[0] * args[3].shape[1]
    slots = count_ep * capacity
    hid = args[14].shape[1]
    width = feats * count_tp
    groups_y, pieces = min(count_ep, 8), 2
    dma = pltpu.SemaphoreType.DMA
    vmem = pltpu.VMEM
    scratch = [vmem(x.shape, x.dtype) for x in args] + [
        vmem((8, positions), f32),
        vmem((count_tp, 8, positions), f32),
        vmem((4, flat), f32),
        vmem((tokens, feats), bf16),
        vmem(args[12].shape, args[12].dtype),
        vmem((1, width), f32),
        vmem((slots, width), bf16),
        vmem((slots, feats), bf16),
        vmem((slots, width), bf16),
        vmem((slots, tokens), bf16),
        vmem((slots, tokens), bf16),
        vmem((positions, flat), f32),
        vmem((positions, flat), f32),
        vmem((positions, flat), f32),
        vmem((positions, flat), f32),
        vmem((4, CHUNKS, flat), f32),
        vmem((2, CHUNKS, flat), f32),
        vmem((4, flat), f32),
        vmem((count_ep, 4, flat), f32),
        vmem((positions, flat), bf16),
        vmem((positions, flat), bf16),
        vmem((positions, channels), bf16),
        vmem((positions, channels * count_tp), bf16),
        vmem((slots, hid), bf16),
        vmem((count_y, slots, feats), f32),
        vmem((count_y, slots, feats), bf16),
        vmem((count_y, slots, feats), bf16),
        vmem((count_y, slots, feats), bf16),
        vmem((count_y, slots, feats), bf16),
        vmem((slots, feats), bf16),
        vmem((slots, feats), bf16),
        dma((len(args),)),
        dma((5,)),
        dma((5,)),
        dma((8,)),
        dma((count_ep,)),
        dma((count_y - 1, groups_y)),
        dma((4,)),
        dma((count_ep,)), dma((count_ep,)),
        dma((count_y - 1, pieces)),
        dma((pieces,)),
        dma((count_y, 4)),
        dma((count_y - 1, groups_y)),
    ]
    return pl.pallas_call(
        functools.partial(kernel, (count_ep, count_tp, groups_y, pieces, state_size)),
        out_shape=[
            vmem((positions, args[8].shape[1]), bf16),
            vmem((tokens, feats), bf16),
        ],
        in_specs=[pl.BlockSpec(memory_space=pltpu.HBM)] * len(args),
        out_specs=[pl.BlockSpec(memory_space=pltpu.VMEM)] * 2,
        scratch_shapes=scratch,
        compiler_params=pltpu.CompilerParams(
            collective_id=0, has_side_effects=True, vmem_limit_bytes=60 * 1024 * 1024
        ),
    )(*args)


def write_out(a_ref, b_ref, a_out, b_out, sems):
    copies = [
        pltpu.make_async_copy(source, target, sems.at[i])
        for i, (source, target) in enumerate(((a_ref, a_out), (b_ref, b_out)))
    ]
    for copy in copies:
        copy.start()
    for copy in copies:
        copy.wait()


def shards(
    mixer_input, mixer_gain, time_step, pole_real, pole_imag, input_real, input_imag,
    read_real, read_imag, out_value, out_gate, expert_input, expert_gain, routes,
    route_weight, expert_gate, expert_up, expert_down,
):
    tokens, top = routes.shape
    capacity = 2 * top * tokens // lax.axis_size("ep")
    def by_channel(table):
        return jnp.swapaxes(table, 1, 2).reshape(-1, table.shape[1])

    args = (
        mixer_input, time_step.T, mixer_gain[None, :], pole_real,
        by_channel(input_real), by_channel(input_imag),
        read_real.reshape(-1, read_real.shape[2]), read_imag.reshape(-1, read_imag.shape[2]),
        out_value, out_gate, expert_input, expert_gain[None, :], routes.T, route_weight.T,
        expert_gate[0], expert_up[0], expert_down[0], pole_imag,
    )
    results = fused(args, pole_real.shape[1], capacity)
    return tuple(
        pl.pallas_call(
            write_out,
            out_shape=[jax.ShapeDtypeStruct(x.shape, x.dtype) for x in results],
            in_specs=[pl.BlockSpec(memory_space=pltpu.VMEM)] * 2,
            out_specs=[pl.BlockSpec(memory_space=pltpu.HBM)] * 2,
            scratch_shapes=[pltpu.SemaphoreType.DMA((2,))],
            compiler_params=pltpu.CompilerParams(vmem_limit_bytes=1024 * 1024),
        )(*results)
    )


def solution(mesh):
    return jax.shard_map(
        shards,
        mesh=mesh,
        in_specs=(
            P("ep", "tp"), P("tp"), P("ep", "tp"), P("tp", None), P("tp", None),
            P("tp", None, None), P("tp", None, None), P("tp", None, None), P("tp", None, None),
            P(None, "tp"), P(None, "tp"), P("ep", "tp"), P("tp"), P("ep", None), P("ep", None),
            P("ep", None, "tp"), P("ep", None, "tp"), P("ep", "tp", None),
        ),
        out_specs=(P("ep", "tp"), P("ep", "tp")),
        check_vma=False,
    )
```

```python
import functools
import jax
import jax.numpy as jnp
from jax import lax
from jax.experimental import pallas as pl
from jax.experimental.pallas import tpu as pltpu
from jax.sharding import PartitionSpec as P

norm_eps = 1e-05
CHUNKS = 8
CORES = 2
f32 = jnp.float32
bf16 = jnp.bfloat16


def sin_cos(angle):
    turns = jnp.round(angle * 0.6366197723675814)
    left = angle - turns * 1.5703125
    left = left - turns * 4.83751296997e-4
    left = left - turns * 7.549789948768648e-8
    sq = left * left
    sine = ((-1.9515295891e-4 * sq + 8.3321608736e-3) * sq - 1.6666654611e-1) * sq * left + left
    cosine = (
        ((2.443315711809948e-5 * sq - 1.388731625493765e-3) * sq + 4.166664568298827e-2) * sq * sq
        - 0.5 * sq
        + 1.0
    )
    quadrant = turns.astype(jnp.int32)
    odd = (quadrant & 1) == 1
    sin_out = jnp.where(odd, cosine, sine)
    cos_out = jnp.where(odd, sine, cosine)
    sin_out = jnp.where((quadrant & 2) == 2, -sin_out, sin_out)
    cos_out = jnp.where(((quadrant + 1) & 2) == 2, -cos_out, cos_out)
    return sin_out, cos_out


def iota(shape, dim):
    return lax.broadcasted_iota(jnp.int32, shape, dim)


def nn(left, right):
    return jnp.dot(left, right, preferred_element_type=f32)


def nt(left, right):
    return lax.dot_general(left, right, (((1,), (1,)), ((), ())), preferred_element_type=f32)


def tn(left, right):
    return lax.dot_general(left, right, (((0,), (0,)), ((), ())), preferred_element_type=f32)


def partner(me, k):
    other, bit = me, 1
    while bit <= k:
        if k & bit:
            other = other + bit * (1 - 2 * ((me // bit) % 2))
        bit *= 2
    return other


def spread(table, row_div, lanes, lane_div):
    rows, width = table.shape
    pick = (iota((width, lanes), 0) == iota((width, lanes), 1) % width).astype(bf16)
    wide = nn(table.astype(bf16), pick)
    same = iota((rows, lanes), 0) // row_div == iota((rows, lanes), 1) // lane_div
    return jnp.where(same, wide, 0.0).astype(bf16)


def row_sums(rows):
    ones = jnp.ones((16, rows.shape[1]), bf16)
    wide = rows.astype(f32)
    square = wide * wide
    high = square.astype(bf16)
    low = (square - high.astype(f32)).astype(bf16)
    sums = nt(ones, rows)
    squares = nt(ones, high) + nt(ones, low)
    return jnp.where(iota((8, 1), 0) == 0, sums[:8], squares[:8])


def normalize(rows, stats, gain, width):
    average = stats[:, 0:1] / width
    variance = stats[:, 1:2] / width - average * average
    return (rows.astype(f32) - average) * lax.rsqrt(variance + norm_eps) * gain


def kernel(dims, *refs):
    count_ep, count_tp, groups_y, pieces, state_size = dims
    hbm, refs = refs[:18], refs[18:]
    (out_a, out_b), refs = refs[:2], refs[2:]
    vm, refs = refs[:18], refs[18:]
    (
        mine_stats, slot_stats, pole, tokens_far, routes_far, gain_all, rows_n, outgoing, rows_x, share_hi, share_lo, a_re, a_im, u_re, u_im,
        sums, enter, mine_state, slot_state, n_re, n_im, mixed, mixed_all, hidden, own,
        sib_send, sib_recv, y_send, y_recv, final, returned,
        sem_in, sem_far, sem_small, sem_send, aa_r, dy_r, ds_r, hs_s, hs_r, my_r, ms_r, rs_r, ry_r,
    ) = refs
    (
        a_in, step_in, gain_a, real_in, in_re, in_im, rd_re, rd_im, w_value, w_gate_out,
        b_in, gain_b, routes_in, weight_in, w_gate, w_up, w_down, imag_in,
    ) = vm

    me = lax.axis_index("ep")
    tp = lax.axis_index("tp")
    count_y = count_tp // CORES
    my_y = tp // CORES
    my_core = tp % CORES
    sibling = my_y * CORES + 1 - my_core

    barrier = pltpu.get_barrier_semaphore()
    for k in range(1, count_ep):
        pl.semaphore_signal(
            barrier, inc=1, device_id={"ep": partner(me, k)}, device_id_type=pl.DeviceIdType.MESH
        )
    for k in range(1, count_tp):
        pl.semaphore_signal(
            barrier, inc=1, device_id={"tp": lax.rem(tp + k, count_tp)},
            device_id_type=pl.DeviceIdType.MESH,
        )

    loads = [
        pltpu.make_async_copy(source, target, sem_in.at[i])
        for i, (source, target) in enumerate(zip(hbm, vm))
    ]
    for i in (10, 12, 11, 0, 1, 3, 17, 2, 13, 4, 5, 6, 7, 14, 15, 16, 8, 9):
        loads[i].start()

    def send(source, target, send_sem, recv_sem, **where):
        copy = pltpu.make_async_remote_copy(
            src_ref=source, dst_ref=target, send_sem=send_sem, recv_sem=recv_sem,
            device_id=where, device_id_type=pl.DeviceIdType.MESH,
        )
        copy.start()
        return copy

    def drain(sem, ref):
        pltpu.make_async_copy(ref, ref, sem).wait()

    positions, channels = a_in.shape
    tokens, feats = b_in.shape
    width = feats * count_tp
    flat = a_re.shape[1]
    states = state_size
    group_ch = in_re.shape[0] * states // flat
    slots = rows_x.shape[0]
    cap = slots // count_ep
    tile = min(256, flat)
    tiles = flat // tile
    tile_ch = tile // states * group_ch
    steps = positions // CHUNKS
    hid = w_gate.shape[1]
    expert_rows = max(16, count_ep)
    my_cols = pl.ds(pl.multiple_of(tp * feats, 128), feats)

    portal = partner(me, count_ep // 2)
    for i in (12, 11, 10):
        loads[i].wait()
    pl.semaphore_wait(barrier, count_ep + count_tp - 2)
    far_routes = send(routes_in, routes_far, sem_far.at[0], sem_far.at[1], ep=portal)
    cuts = 2 if feats % 256 == 0 else 1
    cut = [slice(c * feats // cuts, (c + 1) * feats // cuts) for c in range(cuts)]
    far_tokens = [
        send(
            b_in.at[:, cut[c]], tokens_far.at[:, cut[c]], sem_far.at[2], sem_far.at[3 + c],
            ep=portal,
        )
        for c in range(cuts)
    ]
    gain_copies = [
        send(
            gain_b, gain_all.at[:, my_cols], sem_small.at[0], sem_small.at[1], tp=lax.rem(tp + k, count_tp)
        )
        for k in range(1, count_tp)
    ]
    gain_all[:, my_cols] = gain_b[...]
    near = count_ep // 2
    expert_of = iota((expert_rows, tokens), 0)
    before = (iota((tokens, tokens), 0) < iota((tokens, tokens), 1)).astype(bf16)

    def places(routes):
        hit = jnp.zeros((expert_rows, tokens), jnp.bool_)
        for k in range(routes.shape[0]):
            hit = jnp.logical_or(hit, routes[k : k + 1, :] == expert_of)
        place = nn(hit.astype(f32).astype(bf16), before)
        return jnp.where(hit, place, -1.0).astype(bf16)

    def owners(low, high):
        return jnp.concatenate(
            [
                (iota((cap, expert_rows), 1) == partner(me, k)).astype(f32)
                for k in range(low, high)
            ],
            axis=0,
        ).astype(bf16)

    def select(owner, place):
        return nn(owner, place) == (iota((owner.shape[0], tokens), 0) % cap).astype(f32)

    place_own = places(routes_in[...])
    owner_near = owners(0, near)
    chosen_near = select(owner_near, place_own)
    chosen = chosen_near.astype(f32).astype(bf16)

    arrivals = set()

    def hand_out(base, columns, values, ks):
        outgoing[base * cap : (base + near) * cap, columns] = values
        rows_x[base * cap : (base + 1) * cap, window_of(columns)] = values[0:cap]
        send_slabs(base, columns, ks)

    def window_of(columns):
        size = columns.stop - columns.start
        return pl.ds(pl.multiple_of(tp * feats + columns.start, 128), size)

    def send_slabs(base, columns, ks):
        for k in ks:
            here = pl.ds((base + k) * cap, cap)
            arrivals.add(base + k)
            send(
                outgoing.at[here, columns], rows_x.at[here, window_of(columns)], sem_send.at[0],
                aa_r.at[base + k], ep=partner(me, k),
            )

    per_group = count_ep // groups_y
    group_rows = per_group * cap
    y_arrivals = {}
    block_of = [g // (groups_y // 4) if groups_y >= 4 else g for g in range(groups_y)]

    def core_cols(offset):
        owner_tp = lax.rem(my_y + count_y - offset, count_y) * CORES + my_core
        return pl.ds(pl.multiple_of(owner_tp * feats, 128), feats)

    def to_sibling(offset, g):
        here = rows_x.at[pl.ds(g * group_rows, group_rows), core_cols(offset)]
        send(here, here, sem_send.at[1], ds_r.at[block_of[g]], tp=sibling)

    def forward(g):
        for k in range(g * per_group, (g + 1) * per_group):
            if k in arrivals:
                drain(aa_r.at[k], final.at[pl.ds(0, cap)])
        here = rows_x.at[pl.ds(g * group_rows, group_rows), my_cols]
        for k in range(1, count_y):
            y_arrivals[k, g] = send(
                here, here, sem_send.at[2], dy_r.at[k - 1, g],
                tp=lax.rem(my_y + k, count_y) * CORES + my_core,
            )
        to_sibling(0, g)

    def forward_again(g):
        for k in range(1, count_y):
            y_arrivals[k, g].wait_recv()
            to_sibling(k, g)

    near_first = max(2, near // 2)
    hand_out(0, slice(0, feats), nn(chosen, b_in[...]).astype(bf16), range(1, near))
    forward(0)
    loads[0].wait()
    mine_stats[...] = row_sums(a_in[...])
    stat_copies = [
        send(mine_stats, slot_stats.at[k], sem_small.at[2], sem_small.at[3], tp=lax.rem(tp + k, count_tp))
        for k in range(1, count_tp)
    ]

    loads[1].wait()
    order = (
        iota((positions, positions), 1)
        == (iota((positions, positions), 0) % CHUNKS) * steps
        + iota((positions, positions), 0) // CHUNKS
    ).astype(f32).astype(bf16)
    order_t = (
        iota((positions, positions), 0)
        == (iota((positions, positions), 1) % CHUNKS) * steps
        + iota((positions, positions), 1) // CHUNKS
    ).astype(f32).astype(bf16)
    step = step_in[...]
    groups = step.shape[0]
    high = step.astype(bf16).astype(f32)
    middle = (step - high).astype(bf16).astype(f32)
    low = step - high - middle
    parts = [high, middle, low]
    padded = -(-3 * groups // 16) * 16
    if padded > 3 * groups:
        parts.append(jnp.zeros((padded - 3 * groups, positions), f32))
    split = jnp.concatenate(parts, axis=0).astype(bf16)
    split = nn(split, order_t).astype(bf16)
    for t in range(tiles):
        lanes = slice(t * tile, (t + 1) * tile)
        source = iota((padded, tile), 0)
        pick = jnp.logical_and(
            source % groups == iota((padded, tile), 1) // states + t * (tile // states),
            source < 3 * groups,
        )
        a_re[:, lanes] = tn(split, pick.astype(f32).astype(bf16))

    loads[3].wait()
    loads[17].wait()
    pick = (iota((states, flat), 0) == iota((states, flat), 1) % states).astype(f32).astype(bf16)
    own_lane = iota((groups, flat), 0) == iota((groups, flat), 1) // states

    def to_lanes(table):
        high = table.astype(bf16)
        rest = table - high.astype(f32)
        middle = rest.astype(bf16)
        low = (rest - middle.astype(f32)).astype(bf16)
        wide = nn(high, pick) + (nn(middle, pick) + nn(low, pick))
        return jnp.sum(jnp.where(own_lane, wide, 0.0), axis=0, keepdims=True)

    real, imag = to_lanes(real_in[...]), to_lanes(imag_in[...])
    denom = real * real + imag * imag
    pole[0:1, :] = real
    pole[1:2, :] = imag
    pole[2:3, :] = real / denom
    pole[3:4, :] = imag / denom
    block = min(32, positions)

    def steps_of(t):
        lanes = slice(t * tile, (t + 1) * tile)
        p_re, p_im = pole[0:1, lanes], pole[1:2, lanes]
        d_re, d_im = pole[2:3, lanes], pole[3:4, lanes]

        def elementwise(i, passed):
            here = pl.ds(pl.multiple_of(i * block, block), block)
            delta = a_re[here, lanes]
            for j in range(block // CHUNKS):
                passed = passed + delta[j * CHUNKS : (j + 1) * CHUNKS]
            magnitude = jnp.exp(p_re * delta)
            sine, cosine = sin_cos(p_im * delta)
            ab_re = magnitude * cosine
            ab_im = magnitude * sine
            numer = ab_re - 1.0
            a_re[here, lanes] = ab_re
            a_im[here, lanes] = ab_im
            u_re[here, lanes] = numer * d_re + ab_im * d_im
            u_im[here, lanes] = ab_im * d_re - numer * d_im
            return passed

        passed = lax.fori_loop(
            0, positions // block, elementwise, jnp.zeros((CHUNKS, tile), f32)
        )
        magnitude = jnp.exp(p_re * passed)
        sine, cosine = sin_cos(p_im * passed)
        sums[0, :, lanes] = magnitude * cosine
        sums[1, :, lanes] = magnitude * sine

    for t in range(tiles):
        steps_of(t)
    forward(1)
    forward_again(0)
    far_routes.wait_recv()
    chosen_far = select(owner_near, places(routes_far[...])).astype(f32).astype(bf16)

    def hand_out_far(c):
        far_tokens[c].wait_recv()
        hand_out(near, cut[c], nn(chosen_far, tokens_far[:, cut[c]]).astype(bf16), range(1, near))

    for c in range(cuts - 1):
        hand_out_far(c)
    drain(sem_small.at[3], slot_stats.at[pl.ds(1, count_tp - 1)])
    total = mine_stats[...]
    for k in range(1, count_tp):
        total = total + slot_stats[k]
    total = total.T

    loads[2].wait()
    normed = normalize(a_in[...], total, gain_a[...], width).astype(bf16)
    normed = nn(order, normed).astype(bf16)
    for i in (4, 5, 6, 7):
        loads[i].wait()

    def first_half(t):
        lanes = slice(t * tile, (t + 1) * tile)
        table = slice(t * tile_ch, (t + 1) * tile_ch)
        piece = normed[:, table]
        v_re = nn(piece, spread(in_re[table, :], group_ch, tile, states))
        v_im = nn(piece, spread(in_im[table, :], group_ch, tile, states))
        k_re, k_im = u_re[:, lanes], u_im[:, lanes]
        u_re[:, lanes] = k_re * v_re - k_im * v_im
        u_im[:, lanes] = k_re * v_im + k_im * v_re

    span = min(1024, flat)

    def chunk_sums(base):
        lanes = slice(base, base + span)

        def one(s, carried):
            s_re, s_im = carried
            here = pl.ds(pl.multiple_of(s * CHUNKS, CHUNKS), CHUNKS)
            b_re, b_im = a_re[here, lanes], a_im[here, lanes]
            return (
                b_re * s_re - b_im * s_im + u_re[here, lanes],
                b_re * s_im + b_im * s_re + u_im[here, lanes],
            )

        zero = jnp.zeros((CHUNKS, span), f32)
        sums[2, :, lanes], sums[3, :, lanes] = lax.fori_loop(0, steps, one, (zero, zero), unroll=2)

    early = groups_y // 2
    hand_out_far(cuts - 1)
    forward(early)
    for t in range(tiles // 2):
        first_half(t)
    for t in range(tiles // 2, tiles):
        first_half(t)
    for base in range(0, flat, span):
        chunk_sums(base)
    def chunk(index, c):
        return sums[index, c : c + 1, :]

    c_re, c_im, s_re, s_im = (chunk(index, 0) for index in range(4))
    for c in range(1, CHUNKS):
        b_re, b_im = chunk(0, c), chunk(1, c)
        c_re, c_im = b_re * c_re - b_im * c_im, b_re * c_im + b_im * c_re
        s_re, s_im = (
            b_re * s_re - b_im * s_im + chunk(2, c),
            b_re * s_im + b_im * s_re + chunk(3, c),
        )
    mine_state[0:1, :] = c_re
    mine_state[1:2, :] = c_im
    mine_state[2:3, :] = s_re
    mine_state[3:4, :] = s_im
    state_copies = []
    for k in range(1, count_ep):
        other = partner(me, k)
        copy = pltpu.make_async_remote_copy(
            src_ref=mine_state, dst_ref=slot_state.at[me], send_sem=hs_s.at[k], recv_sem=hs_r.at[k],
            device_id={"ep": other}, device_id_type=pl.DeviceIdType.MESH,
        )
        state_copies.append((other, copy))

        @pl.when(other > me)
        def _(copy=copy):
            copy.start()

    for g in range(2, min(3, early)):
        forward(g)
    forward_again(1)
    loads[13].wait()
    weight = jnp.zeros((expert_rows, tokens), f32)
    for k in range(routes_in.shape[0]):
        this = routes_in[k : k + 1, :] == expert_of
        weight = jnp.where(this, weight_in[k : k + 1, :], weight)
    weight_hi = weight.astype(bf16)
    weight_lo = (weight - weight_hi.astype(f32)).astype(bf16)
    owner_far = owners(near, count_ep)
    for rows, owner, here in (
        (slice(0, near * cap), owner_near, chosen_near),
        (slice(near * cap, slots), owner_far, select(owner_far, place_own)),
    ):
        share_hi[rows, :] = jnp.where(here, nn(owner, weight_hi), 0.0).astype(bf16)
        share_lo[rows, :] = jnp.where(here, nn(owner, weight_lo), 0.0).astype(bf16)

    columns = min(256, hid)
    out_columns = min(256, feats)
    middle = early + (groups_y - early) // 2
    split = early // 2
    blocks = ((0, split), (early, middle), (middle, groups_y), (split, early))

    def rows_of(b):
        return slice(blocks[b][0] * group_rows, blocks[b][1] * group_rows)


    def normalize_rows(b):
        step_rows = min(64, group_rows)
        for r in range(rows_of(b).start, rows_of(b).stop, step_rows):
            rows = slice(r, r + step_rows)
            wide = rows_x[rows, :].astype(f32)
            average = jnp.sum(wide, axis=1, keepdims=True) / width
            square = jnp.sum(wide * wide, axis=1, keepdims=True) / width
            variance = square - average * average
            wide = (wide - average) * lax.rsqrt(variance + norm_eps) * gain_all[...]
            rows_n[rows, :] = wide.astype(bf16)

    def hidden_units(b, between):
        top = rows_of(b)
        for n in range(hid // columns):
            cols = slice(n * columns, (n + 1) * columns)
            gate = nn(rows_n[top, :], w_gate[:, cols])
            up = nn(rows_n[top, :], w_up[:, cols])
            hidden[top, cols] = (gate * jax.nn.sigmoid(gate) * up).astype(bf16)
            between(n)

    sib_copies, y_copies = {}, {}

    def down(b, target_tp, store):
        top = rows_of(b)
        for n in range(feats // out_columns):
            first = pl.multiple_of(target_tp * feats + n * out_columns, 128)
            store(
                top, slice(n * out_columns, (n + 1) * out_columns),
                nn(hidden[top, :], w_down[:, pl.ds(first, out_columns)]),
            )

    def give_back(b, offsets):
        for offset in offsets:
            yt = lax.rem(my_y + offset, count_y) * CORES

            def to_send(rows, cols, value, offset=offset):
                sib_send[offset, rows, cols] = value.astype(bf16)

            def to_own(rows, cols, value, offset=offset):
                own[offset, rows, cols] = value

            down(b, yt + 1 - my_core, to_send)
            window = pl.ds(rows_of(b).start, rows_of(b).stop - rows_of(b).start)
            sib_copies[b, offset] = send(
                sib_send.at[offset, window], sib_recv.at[offset, window],
                sem_send.at[3], rs_r.at[offset, b], tp=sibling,
            )
            down(b, yt + my_core, to_own)

    def sum_y(b):
        for offset in range(1, count_y):
            sib_copies[b, offset].wait_recv()
            rows = rows_of(b)
            y_send[offset, rows, :] = (
                own[offset, rows, :] + sib_recv[offset, rows, :].astype(f32)
            ).astype(bf16)

    def send_y(g):
        for offset in range(1, count_y):
            window = pl.ds(g * group_rows, group_rows)
            y_copies[offset, g] = send(
                y_send.at[offset, window], y_recv.at[offset, window],
                sem_send.at[4], ry_r.at[offset - 1, g],
                tp=lax.rem(my_y + offset, count_y) * CORES + my_core,
            )

    back_copies = {}

    def finish(g):
        window = slice(g * group_rows, (g + 1) * group_rows)
        total = own[0, window, :] + sib_recv[0, window, :].astype(f32)
        for offset in range(1, count_y):
            y_copies[offset, g].wait_recv()
            total = total + y_recv[offset, window, :].astype(f32)
        total = total.astype(bf16)
        final[window, :] = total
        if g == 0:
            returned[0:cap, :] = total[0:cap]
        for k in range(max(1, g * per_group), (g + 1) * per_group):
            here = pl.ds(k * cap, cap)
            back_copies[k] = send(
                final.at[here], returned.at[here], sem_send.at[5], sem_small.at[4], ep=partner(me, k)
            )

    def rows_ready(low, high):
        size = (high - low) * group_rows
        drain_rows(ds_r.at[block_of[low]], count_y * size)

    def drain_rows(sem, count):
        if count <= slots:
            drain(sem, final.at[pl.ds(0, count)])
        else:
            drain(sem, rows_x.at[:, pl.ds(0, count // slots * feats)])

    others = list(range(1, count_y))
    chunks = hid // columns

    def spread_out(tasks):
        def between(n):
            for task in tasks[n * len(tasks) // chunks : (n + 1) * len(tasks) // chunks]:
                task()

        return between

    def tasks_of(function, items):
        return [functools.partial(function, item) for item in items]

    forward(early + 1)
    rows_ready(*blocks[0])
    drain(sem_small.at[1], gain_all.at[:, pl.ds(0, width - feats)])
    normalize_rows(0)
    loads[14].wait()
    loads[15].wait()
    first = [early + 1, *range(early + 2, groups_y)]
    after = [[] for n in range(chunks)]
    after[0] += tasks_of(forward_again, [early])
    after[max(0, chunks // 2 - 1)] += tasks_of(forward, first[1:2])
    after[-1] += tasks_of(forward, first[2:3])

    def between(n):
        for task in after[n]:
            task()

    hidden_units(0, between)
    loads[16].wait()
    give_back(0, others)
    for g in first[3:]:
        forward(g)
    give_back(0, [0])
    forward_again(early + 1)
    for other, copy in state_copies:

        @pl.when(other < me)
        def _(copy=copy):
            copy.wait_recv()


    def fold(q, carried):
        h_re, h_im = carried
        b_re, b_im = slot_state[q, 0:1, :], slot_state[q, 1:2, :]
        return (
            b_re * h_re - b_im * h_im + slot_state[q, 2:3, :],
            b_re * h_im + b_im * h_re + slot_state[q, 3:4, :],
        )

    blank = jnp.zeros((1, flat), f32)
    h_re, h_im = lax.fori_loop(0, me, fold, (blank, blank))
    for c in range(CHUNKS):
        enter[0, c : c + 1, :] = h_re
        enter[1, c : c + 1, :] = h_im
        b_re, b_im = chunk(0, c), chunk(1, c)
        h_re, h_im = (
            b_re * h_re - b_im * h_im + chunk(2, c),
            b_re * h_im + b_im * h_re + chunk(3, c),
        )
    for base in range(0, flat, span):
        lanes = slice(base, base + span)

        def advance(s, carried, lanes=lanes):
            s_re, s_im = carried
            found_re, found_im = [], []
            for j in range(2):
                here = pl.ds(pl.multiple_of(s * 2 * CHUNKS + j * CHUNKS, CHUNKS), CHUNKS)
                b_re, b_im = a_re[here, lanes], a_im[here, lanes]
                s_re, s_im = (
                    b_re * s_re - b_im * s_im + u_re[here, lanes],
                    b_re * s_im + b_im * s_re + u_im[here, lanes],
                )
                found_re.append(s_re)
                found_im.append(s_im)
            both = pl.ds(pl.multiple_of(s * 2 * CHUNKS, 2 * CHUNKS), 2 * CHUNKS)
            n_re[both, lanes] = jnp.concatenate(found_re, axis=0).astype(bf16)
            n_im[both, lanes] = jnp.concatenate(found_im, axis=0).astype(bf16)
            return s_re, s_im

        lax.fori_loop(0, steps // 2, advance, (enter[0, :, lanes], enter[1, :, lanes]))
    for g in range(3, early):
        forward(g)
    for t in range(tiles):
        lanes = slice(t * tile, (t + 1) * tile)
        table = slice(t * tile_ch, (t + 1) * tile_ch)
        response = nt(n_re[:, lanes], spread(rd_re[table, :], group_ch, tile, states)) - nt(
            n_im[:, lanes], spread(rd_im[table, :], group_ch, tile, states)
        )
        mixed[:, table] = jax.nn.gelu(response).astype(bf16)
    mixed_cols = pl.ds(pl.multiple_of(tp * channels, 128), channels)
    mixed_all[:, mixed_cols] = nn(order_t, mixed[...]).astype(bf16)

    piece_rows = positions // pieces

    def mixed_window(offset, p):
        owner_tp = lax.rem(my_y + count_y - offset, count_y) * CORES + my_core
        return mixed_all.at[
            pl.ds(p * piece_rows, piece_rows),
            pl.ds(pl.multiple_of(owner_tp * channels, 128), channels),
        ]

    mixed_y = {}

    def mixed_to_sibling(offset, p):
        here = mixed_window(offset, p)
        send(here, here, sem_send.at[6], ms_r.at[p], tp=sibling)

    def send_mixed(p):
        here = mixed_window(0, p)
        for k in range(1, count_y):
            mixed_y[k, p] = send(
                here, here, sem_send.at[7], my_r.at[k - 1, p],
                tp=lax.rem(my_y + k, count_y) * CORES + my_core,
            )
        mixed_to_sibling(0, p)

    def forward_mixed(p):
        for k in range(1, count_y):
            mixed_y[k, p].wait_recv()
            mixed_to_sibling(k, p)

    send_mixed(0)
    rows_ready(*blocks[1])
    normalize_rows(1)
    hidden_units(1, spread_out(tasks_of(forward_again, range(early + 2, groups_y))))
    give_back(1, others + [0])
    sum_y(1)
    for g in reversed(range(*blocks[1])):
        send_y(g)
    rows_ready(*blocks[2])
    normalize_rows(2)
    hidden_units(2, spread_out(tasks_of(forward_again, range(2, early))))
    give_back(2, others + [0])
    sum_y(2)
    for g in reversed(range(*blocks[2])):
        send_y(g)
    sum_y(0)
    for g in reversed(range(1, split)):
        send_y(g)
    forward_mixed(0)
    rows_ready(*blocks[3])
    normalize_rows(3)
    sib_copies[1, 0].wait_recv()
    sib_copies[2, 0].wait_recv()
    far_order = list(reversed(range(*blocks[1]))) + list(reversed(range(*blocks[2])))

    def one_finish(n):
        if n == chunks - 1:
            finish(far_order[0])
            finish(far_order[1])

    hidden_units(3, one_finish)
    give_back(3, others + [0])
    sum_y(3)
    for g in reversed(range(*blocks[3])):
        send_y(g)
    for p in range(1, pieces):
        send_mixed(p)
    send_y(0)
    for g in far_order[2:]:
        finish(g)
    loads[8].wait()
    loads[9].wait()

    def project(p):
        drain(ms_r.at[p], mixed_all.at[pl.ds(0, piece_rows), pl.ds(0, count_y * channels)])
        rows = slice(p * piece_rows, (p + 1) * piece_rows)
        out_a_cols = min(256, out_a.shape[1])
        for n in range(out_a.shape[1] // out_a_cols):
            cols = slice(n * out_a_cols, (n + 1) * out_a_cols)
            value = nn(mixed_all[rows, :], w_value[:, cols])
            gate = nn(mixed_all[rows, :], w_gate_out[:, cols])
            out_a[rows, cols] = (value * jax.nn.sigmoid(gate)).astype(bf16)

    project(0)
    sib_copies[0, 0].wait_recv()
    sib_copies[3, 0].wait_recv()
    for g in reversed(range(1, split)):
        finish(g)
    for g in reversed(range(*blocks[3])):
        finish(g)
    for p in range(1, pieces):
        forward_mixed(p)
    finish(0)
    for p in range(1, pieces):
        project(p)
    drain(sem_small.at[4], returned.at[pl.ds(cap, slots - cap)])
    out_b[...] = (tn(share_hi[...], returned[...]) + tn(share_lo[...], returned[...])).astype(bf16)
    for other, copy in state_copies:

        @pl.when(other > me)
        def _(copy=copy):
            copy.wait_send()

    far_routes.wait_send()
    drain(sem_far.at[2], tokens_far)
    drain(sem_small.at[0], gain_all.at[:, pl.ds(0, width - feats)])
    drain(sem_small.at[2], slot_stats.at[pl.ds(1, count_tp - 1)])
    drain_rows(sem_send.at[0], 2 * (near - 1) * cap)
    drain_rows(sem_send.at[1], count_y * slots)
    drain_rows(sem_send.at[2], (count_y - 1) * slots)
    drain_rows(sem_send.at[3], count_y * slots)
    drain_rows(sem_send.at[4], (count_y - 1) * slots)
    drain_rows(sem_send.at[5], slots - cap)
    drain(sem_send.at[6], mixed_all.at[:, pl.ds(0, count_y * channels)])
    drain(sem_send.at[7], mixed_all.at[:, pl.ds(0, (count_y - 1) * channels)])


def fused(args, state_size, capacity):
    count_ep, count_tp = lax.axis_size("ep"), lax.axis_size("tp")
    count_y = count_tp // CORES
    positions, channels = args[0].shape
    groups = args[1].shape[0]
    tokens, feats = args[10].shape
    flat = args[3].shape[0] * args[3].shape[1]
    slots = count_ep * capacity
    hid = args[14].shape[1]
    width = feats * count_tp
    groups_y, pieces = min(count_ep, 8), 2
    dma = pltpu.SemaphoreType.DMA
    vmem = pltpu.VMEM
    scratch = [vmem(x.shape, x.dtype) for x in args] + [
        vmem((8, positions), f32),
        vmem((count_tp, 8, positions), f32),
        vmem((4, flat), f32),
        vmem((tokens, feats), bf16),
        vmem(args[12].shape, args[12].dtype),
        vmem((1, width), f32),
        vmem((slots, width), bf16),
        vmem((slots, feats), bf16),
        vmem((slots, width), bf16),
        vmem((slots, tokens), bf16),
        vmem((slots, tokens), bf16),
        vmem((positions, flat), f32),
        vmem((positions, flat), f32),
        vmem((positions, flat), f32),
        vmem((positions, flat), f32),
        vmem((4, CHUNKS, flat), f32),
        vmem((2, CHUNKS, flat), f32),
        vmem((4, flat), f32),
        vmem((count_ep, 4, flat), f32),
        vmem((positions, flat), bf16),
        vmem((positions, flat), bf16),
        vmem((positions, channels), bf16),
        vmem((positions, channels * count_tp), bf16),
        vmem((slots, hid), bf16),
        vmem((count_y, slots, feats), f32),
        vmem((count_y, slots, feats), bf16),
        vmem((count_y, slots, feats), bf16),
        vmem((count_y, slots, feats), bf16),
        vmem((count_y, slots, feats), bf16),
        vmem((slots, feats), bf16),
        vmem((slots, feats), bf16),
        dma((len(args),)),
        dma((5,)),
        dma((5,)),
        dma((8,)),
        dma((count_ep,)),
        dma((count_y - 1, groups_y)),
        dma((4,)),
        dma((count_ep,)), dma((count_ep,)),
        dma((count_y - 1, pieces)),
        dma((pieces,)),
        dma((count_y, 4)),
        dma((count_y - 1, groups_y)),
    ]
    return pl.pallas_call(
        functools.partial(kernel, (count_ep, count_tp, groups_y, pieces, state_size)),
        out_shape=[
            vmem((positions, args[8].shape[1]), bf16),
            vmem((tokens, feats), bf16),
        ],
        in_specs=[pl.BlockSpec(memory_space=pltpu.HBM)] * len(args),
        out_specs=[pl.BlockSpec(memory_space=pltpu.VMEM)] * 2,
        scratch_shapes=scratch,
        compiler_params=pltpu.CompilerParams(
            collective_id=0, has_side_effects=True, vmem_limit_bytes=60 * 1024 * 1024
        ),
    )(*args)


def write_out(a_ref, b_ref, a_out, b_out, sems):
    copies = [
        pltpu.make_async_copy(source, target, sems.at[i])
        for i, (source, target) in enumerate(((a_ref, a_out), (b_ref, b_out)))
    ]
    for copy in copies:
        copy.start()
    for copy in copies:
        copy.wait()


def shards(
    mixer_input, mixer_gain, time_step, pole_real, pole_imag, input_real, input_imag,
    read_real, read_imag, out_value, out_gate, expert_input, expert_gain, routes,
    route_weight, expert_gate, expert_up, expert_down,
):
    tokens, top = routes.shape
    capacity = 2 * top * tokens // lax.axis_size("ep")
    def by_channel(table):
        return jnp.swapaxes(table, 1, 2).reshape(-1, table.shape[1])

    args = (
        mixer_input, time_step.T, mixer_gain[None, :], pole_real,
        by_channel(input_real), by_channel(input_imag),
        read_real.reshape(-1, read_real.shape[2]), read_imag.reshape(-1, read_imag.shape[2]),
        out_value, out_gate, expert_input, expert_gain[None, :], routes.T, route_weight.T,
        expert_gate[0], expert_up[0], expert_down[0], pole_imag,
    )
    results = fused(args, pole_real.shape[1], capacity)
    return tuple(
        pl.pallas_call(
            write_out,
            out_shape=[jax.ShapeDtypeStruct(x.shape, x.dtype) for x in results],
            in_specs=[pl.BlockSpec(memory_space=pltpu.VMEM)] * 2,
            out_specs=[pl.BlockSpec(memory_space=pltpu.HBM)] * 2,
            scratch_shapes=[pltpu.SemaphoreType.DMA((2,))],
            compiler_params=pltpu.CompilerParams(vmem_limit_bytes=1024 * 1024),
        )(*results)
    )


def solution(mesh):
    return jax.shard_map(
        shards,
        mesh=mesh,
        in_specs=(
            P("ep", "tp"), P("tp"), P("ep", "tp"), P("tp", None), P("tp", None),
            P("tp", None, None), P("tp", None, None), P("tp", None, None), P("tp", None, None),
            P(None, "tp"), P(None, "tp"), P("ep", "tp"), P("tp"), P("ep", None), P("ep", None),
            P("ep", None, "tp"), P("ep", None, "tp"), P("ep", "tp", None),
        ),
        out_specs=(P("ep", "tp"), P("ep", "tp")),
        check_vma=False,
    )
```
